32 devices in a mesh: sp: 8 (over z, x), tp: 4 (over y, core).
Axes of the slice: x: 2, y: 2, z: 4, core: 2. Of those that a mesh axis runs over, the one named last changes fastest.
Arguments:
- queries: bfloat16 [6144, 2048], P('sp', 'tp'), may hold values from -110 to 110
- key_rows: bfloat16 [6144, 512], P('sp', 'tp'), may hold values from -4.5 to 4.5
- values: bfloat16 [6144, 512], P('sp', 'tp'), may hold values from -6 to 6
- sink_logits: float32 [32], P('tp'), may hold values from 2 to 7
- doc_ids: int32 [6144], P('sp'), may hold values from 0 to 3, as said below
- residual: bfloat16 [6144, 2048], P('sp'), may hold values from -20 to 20
- w_out: bfloat16 [2048, 2048], P('tp'), may hold values from -2.390625 to 2.390625
- norm_gain: float32 [2048], replicated, may hold values from 0.1 to 1.9
- w_value_up: bfloat16 [2048, 5632], P('sp', 'tp'), may hold values from -0.125 to 0.125
- w_gate_up: bfloat16 [2048, 5632], P('sp', 'tp'), may hold values from -0.125 to 0.125
- conv_taps: bfloat16 [3, 5632], P(None, 'tp'), may hold values from -3.5 to 3.5
- w_down_t: bfloat16 [2048, 5632], P('sp', 'tp'), may hold values from -0.078125 to 0.078125
Outputs:
- layer_out: bfloat16 [6144, 2048], P('sp', 'tp')
The draws below stay inside these ranges and needn't reach their ends.
Inputs may be any that keep to these rules, and one draw needn't show every extreme that they name: `doc_ids`: document numbers never fall along the sequence and every one of the 4 documents is present; each document has 2 or more positions.
All inputs are finite; a program needn't handle non-finite values.
Results may differ from the reference program's by a relative error of at most 0.017.
Values may be sent and summed in bfloat16 or wider, within the bound.
A program may use at most 64 MiB of HBM per device.

```python
import jax
import jax.numpy as jnp
from jax import lax

D = 2048
FF = 5632
HEADS = 32
KV_HEADS = 8
HEAD_DIM = 64
WINDOW = 128
TOK_DEV = 768
Q_W = 2048
SEQ = 6144
DOCS = 4
N_TP = 4


def paired_heads(key):
    key_part = jnp.clip(jax.random.normal(jax.random.fold_in(key, 11), (SEQ, KV_HEADS, HEAD_DIM), jnp.float32), -4.0, 4.0)
    query_part = jnp.clip(jax.random.normal(jax.random.fold_in(key, 12), (SEQ, HEADS, HEAD_DIM), jnp.float32), -5.0, 5.0)
    return (query_part.reshape(SEQ, HEADS * HEAD_DIM), key_part.reshape(SEQ, KV_HEADS * HEAD_DIM))


def draw_queries(key, part):
    return paired_heads(key)[0].astype(jnp.bfloat16)


def draw_key_rows(key, part):
    return paired_heads(key)[1].astype(jnp.bfloat16)


def draw_doc_ids(key, part):
    starts_count = DOCS - 1
    centre = 2 * TOK_DEV * (jnp.arange(starts_count, dtype=jnp.int32) + 1)
    offset = jax.random.randint(jax.random.fold_in(key, 31), (starts_count,), 1 - TOK_DEV, TOK_DEV, jnp.int32)
    starts = centre + offset
    position = jnp.arange(SEQ, dtype=jnp.int32)
    return jnp.sum((position[:, None] >= starts[None, :]).astype(jnp.int32), axis=1).astype(jnp.int32)


def draw_residual(key, part):
    column = jnp.arange(D).astype(jnp.float32)
    col_scale = 0.5 * jnp.exp(jnp.log(3.0) * column / (D - 1))
    draws_base = jnp.clip(jax.random.normal(jax.random.fold_in(key, 21), (SEQ, D), jnp.float32), -4.0, 4.0)
    return (draws_base * col_scale[None, :]).astype(jnp.bfloat16)


def level_of(rng, dims, shards, smallest, high):
    loudness, own = 1.0, jax.random.fold_in(rng, 6)
    for dim, blocks in shards:
        draws = jnp.exp(jax.random.uniform(jax.random.fold_in(own, dim), (blocks,), jnp.float32, smallest / len(shards), high / len(shards)))
        loudness = loudness * jnp.repeat(draws, dims[dim] // blocks).reshape([-1 if axis == dim else 1 for axis in range(len(dims))])
    return loudness


def scatter_about(stream_key, extent, deviation, most, split=(), held_as=jnp.bfloat16):
    values = jax.random.normal(stream_key, extent, jnp.float32) * deviation
    if len(split) > 0:
        values = level_of(stream_key, extent, split, -0.22, 0.18) * values
    return jnp.clip(values, min=-most, max=most).astype(held_as)


def setup_inputs(seed: int = 0) -> dict:
    key_of = jax.random.split(jax.random.key(seed), 13)
    return {
        "queries": draw_queries(jax.random.fold_in(key_of[12], 71), 0),
        "key_rows": draw_key_rows(jax.random.fold_in(key_of[12], 71), 0),
        "values": scatter_about(key_of[2], (SEQ, KV_HEADS * HEAD_DIM), 1.0, 6.0, ((0, 8), (1, 4))),
        "sink_logits": jnp.clip(2.0 + 5.0 * jax.random.uniform(key_of[3], (HEADS,), jnp.float32) ** level_of(key_of[3], (HEADS,), ((0, 4),), -0.2, 0.2), 2.0, 7.0),
        "doc_ids": draw_doc_ids(jax.random.fold_in(key_of[12], 71), 0),
        "residual": draw_residual(jax.random.fold_in(key_of[12], 71), 0),
        "w_out": scatter_about(key_of[6], (Q_W, D), 0.4, 2.390625, ((0, 4),)),
        "norm_gain": jnp.clip(1.0 + 0.18 * jax.random.normal(key_of[7], (D,), jnp.float32), 0.1, 1.9),
        "w_value_up": scatter_about(key_of[8], (D, FF), D ** -0.5, 0.125, ((0, 8), (1, 4))),
        "w_gate_up": scatter_about(key_of[9], (D, FF), D ** -0.5, 0.125, ((0, 8), (1, 4))),
        "conv_taps": scatter_about(key_of[10], (3, FF), 3 ** -0.5, 3.5, ((1, 4),)),
        "w_down_t": scatter_about(key_of[11], (D, FF), FF ** -0.5, 0.078125, ((0, 8), (1, 4))),
    }


EPS = 1e-06
NEG = -1e+30

def attend_block(q_block, kv_window, doc_window, doc_query, sink_logits):
    per_kv = HEADS // KV_HEADS
    kv_cols = KV_HEADS * HEAD_DIM
    q_heads = q_block.astype(jnp.float32).reshape(WINDOW, KV_HEADS, per_kv, HEAD_DIM)
    k_heads = kv_window[:, :kv_cols].astype(jnp.float32).reshape(3 * WINDOW, KV_HEADS, HEAD_DIM)
    v_heads = kv_window[:, kv_cols:].astype(jnp.float32).reshape(3 * WINDOW, KV_HEADS, HEAD_DIM)
    score = jnp.einsum('qkgd,jkd->kgqj', q_heads, k_heads) * HEAD_DIM ** (-0.5)
    offsets = jnp.arange(3 * WINDOW)[None, :] - WINDOW - jnp.arange(WINDOW)[:, None]
    allowed = (jnp.abs(offsets) <= WINDOW) & (doc_query[:, None] == doc_window[None, :])
    sink_grid = sink_logits.reshape(KV_HEADS, per_kv)[:, :, None]
    highest = jnp.maximum(lax.optimization_barrier(jnp.max(jnp.where(allowed, score, NEG), axis=-1)), sink_grid)
    raw = jnp.where(allowed, jnp.exp(score - highest[..., None]), 0.0)
    total = lax.optimization_barrier(jnp.sum(raw, axis=-1)) + jnp.exp(sink_grid - highest)
    probs = (raw / total[..., None]).astype(jnp.bfloat16)
    attended = jnp.einsum('kgqj,jkd->qkgd', probs.astype(jnp.float32), v_heads)
    return attended.reshape(WINDOW, HEADS * HEAD_DIM).astype(jnp.bfloat16)

def rounded(term):
    return lax.optimization_barrier(term.astype(jnp.bfloat16)).astype(jnp.float32)

def reference(queries, key_rows, values, sink_logits, doc_ids, residual, w_out, norm_gain, w_value_up, w_gate_up, conv_taps, w_down_t):
    seq_len = queries.shape[0]
    blocks = seq_len // WINDOW
    stacked = jnp.concatenate([key_rows, values], axis=1)
    padded = jnp.pad(stacked, ((WINDOW, WINDOW), (0, 0)))
    labels = doc_ids + 1
    label_pad = jnp.pad(labels, (WINDOW, WINDOW))
    kv_blocks = padded.reshape(blocks + 2, WINDOW, stacked.shape[1])
    kv_window = jnp.concatenate([kv_blocks[:-2], kv_blocks[1:-1], kv_blocks[2:]], axis=1)
    lab_blocks = label_pad.reshape(blocks + 2, WINDOW)
    doc_window = jnp.concatenate([lab_blocks[:-2], lab_blocks[1:-1], lab_blocks[2:]], axis=1)
    q_blocks = queries.reshape(blocks, WINDOW, queries.shape[1])
    doc_query = labels.reshape(blocks, WINDOW)
    attended = lax.map(lambda items: attend_block(items[0], items[1], items[2], items[3], sink_logits), (q_blocks, kv_window, doc_window, doc_query))
    attended = attended.reshape(seq_len, queries.shape[1])
    head_cols = queries.shape[1] // N_TP
    attn_total = jnp.zeros((seq_len, D), jnp.float32)
    for member in range(N_TP):
        cols = attended[:, member * head_cols:(member + 1) * head_cols]
        rows_w = w_out[member * head_cols:(member + 1) * head_cols]
        attn_total = attn_total + rounded(jnp.dot(cols, rows_w, preferred_element_type=jnp.float32))
    mixed = (residual.astype(jnp.float32) + attn_total).astype(jnp.bfloat16)
    mixed_f = mixed.astype(jnp.float32)
    mean_sq = lax.optimization_barrier(jnp.mean(mixed_f * mixed_f, axis=1, keepdims=True))
    normed = (mixed_f * lax.rsqrt(mean_sq + EPS) * norm_gain).astype(jnp.bfloat16)
    up_value = jnp.dot(normed, w_value_up, preferred_element_type=jnp.float32).astype(jnp.bfloat16)
    up_gate = jnp.dot(normed, w_gate_up, preferred_element_type=jnp.float32).astype(jnp.bfloat16)
    value_f = up_value.astype(jnp.float32)
    value_pad = jnp.pad(value_f, ((1, 1), (0, 0)))
    lab_one = jnp.pad(labels, (1, 1))
    prev_same = (lab_one[:-2] == labels)[:, None]
    next_same = (lab_one[2:] == labels)[:, None]
    tap_f = conv_taps.astype(jnp.float32)
    conv = tap_f[0] * jnp.where(prev_same, value_pad[:-2], 0.0) + tap_f[1] * value_f + tap_f[2] * jnp.where(next_same, value_pad[2:], 0.0)
    hidden = (jax.nn.silu(conv) * up_gate.astype(jnp.float32)).astype(jnp.bfloat16)
    ff_cols = FF // N_TP
    ffn_total = jnp.zeros((seq_len, D), jnp.float32)
    for member in range(N_TP):
        cols = hidden[:, member * ff_cols:(member + 1) * ff_cols]
        down_cols = w_down_t[:, member * ff_cols:(member + 1) * ff_cols]
        term = lax.dot_general(cols, down_cols, (((1,), (1,)), ((), ())), preferred_element_type=jnp.float32)
        ffn_total = ffn_total + rounded(term)
    return (mixed.astype(jnp.float32) + ffn_total).astype(jnp.bfloat16)
```

```python
import functools

import jax
import jax.numpy as jnp
from jax import lax
from jax.experimental import pallas as pl
from jax.experimental.pallas import tpu as pltpu
from jax.sharding import PartitionSpec as P

HEAD_DIM = 64
WINDOW = 128
EPS = 1e-06
NEG = -1e30
RIM = 16
LANES = 128
MESH = pl.DeviceIdType.MESH
F32 = jnp.float32
BF16 = jnp.bfloat16


def ring_kernel(
    n, ntp,
    q_ref, k_ref, v_ref, sink_ref, lab_row_ref,
    res_hbm, wout_ref, gain_ref, wv_hbm, wg_hbm, taps_ref, wd_hbm,
    out_ref,
    up, down, kx, vx, lx, lc, part, first, second, mixed, normed, value, gate, rim, pd, box, inbox, res,
    loc_sem, ring_send, ring_recv, halo_send, halo_recv, rim_send, rim_recv,
    core_send, core_recv, y_send, y_recv, back_send, back_recv, pair_send, pair_recv,
    down_send, down_recv, out_send, out_recv,
):
    me = lax.axis_index("sp")
    tp = lax.axis_index("tp")
    core = lax.rem(tp, 2)
    y = tp // 2
    ny = ntp // 2
    partner = y * 2 + 1 - core
    rows = q_ref.shape[0]
    half = rows // 2
    piece = half // ny
    block = wv_hbm.shape[0]
    depth = block // 2
    quarter = block // 4

    def place(p):
        h = p // (n // 2)
        return (1 - h) * (2 * p) + h * (2 * n - 1 - 2 * p)

    odd = lax.rem(me, 2)
    pos = (1 - odd) * (me // 2) + odd * ((2 * n - 1 - me) // 2)
    ahead = place(lax.rem(pos + 1, n))
    behind = place(lax.rem(pos + n - 1, n))
    right = lax.rem(me + 1, n)
    left = lax.rem(me + n - 1, n)

    loads = []
    for i, (src, dst) in enumerate((
        (wv_hbm, up.at[0, pl.ds(me * block, block)]),
        (wg_hbm, up.at[1, pl.ds(me * block, block)]),
        (wd_hbm, down.at[pl.ds(me * block, block)]),
        (res_hbm.at[pl.ds(core * half + y * piece, piece)], res),
    )):
        c = pltpu.make_async_copy(src, dst, loc_sem.at[i])
        c.start()
        loads.append(c)

    barrier = pltpu.get_barrier_semaphore()
    peers = [(ahead, tp), (behind, tp), (right, tp), (left, tp)]
    for j in range(1, ntp):
        peers.append((me, lax.rem(tp + j, ntp)))
    for peer in peers:
        pl.semaphore_signal(barrier, inc=1, device_id=peer, device_id_type=MESH)
    for c in loads:
        c.wait()
    pl.semaphore_wait(barrier, len(peers))

    def spot(stream, way, owner):
        if stream < 2:
            return up.at[stream, pl.ds(owner * block + way * depth, depth)]
        return down.at[pl.ds(owner * block + way * depth + (stream - 2) * quarter, quarter)]

    def ring(stream, way, s, arriving):
        shift = s + 1 if arriving else s
        owner = place(lax.rem(pos + n - shift, n)) if way == 0 else place(lax.rem(pos + shift, n))
        ref = spot(stream, way, owner)
        return pltpu.make_async_remote_copy(
            src_ref=ref, dst_ref=ref,
            send_sem=ring_send.at[stream, way, s], recv_sem=ring_recv.at[stream, way, s],
            device_id=(ahead if way == 0 else behind, tp), device_id_type=MESH,
        )

    def begin(stream):
        for way in range(2):
            ring(stream, way, 0, False).start()

    def forward(stream, s, last=False):
        for way in range(2):
            ring(stream, way, s, True).wait_recv()
            if not last:
                ring(stream, way, s + 1, False).start()

    queue = []
    for s in range(n - 1):
        for stream in (0, 1):
            queue.append((stream, s))
    for s in range(n - 1):
        for stream in (2, 3):
            queue.append((stream, s))
    done = [0]

    def serve(count):
        for _ in range(count):
            if done[0] == len(queue):
                return
            stream, s = queue[done[0]]
            done[0] += 1
            forward(stream, s, last=s == n - 2)
            if stream < 2 and s == n - 2:
                begin(stream + 2)

    halo = []

    def remote(src, dst, send, recv, where):
        c = pltpu.make_async_remote_copy(
            src_ref=src, dst_ref=dst, send_sem=send, recv_sem=recv, device_id=where, device_id_type=MESH
        )
        c.start()
        return c

    ends = pl.ds(rows - WINDOW, WINDOW)
    starts = pl.ds(0, WINDOW)
    low, high = pl.ds(0, WINDOW), pl.ds(rows + WINDOW, WINDOW)
    for i, (src, dst) in enumerate(((k_ref, kx), (v_ref, vx))):
        halo.append(remote(src.at[ends], dst.at[low], halo_send.at[i, 0], halo_recv.at[i, 0], (right, tp)))
        halo.append(remote(src.at[starts], dst.at[high], halo_send.at[i, 1], halo_recv.at[i, 1], (left, tp)))
    halo.append(remote(lab_row_ref.at[:, ends], lx.at[:, low], halo_send.at[2, 0], halo_recv.at[2, 0], (right, tp)))
    halo.append(remote(lab_row_ref.at[:, starts], lx.at[:, high], halo_send.at[2, 1], halo_recv.at[2, 1], (left, tp)))
    begin(0)
    begin(1)
    inner = pl.ds(WINDOW, rows)
    kx[inner, :] = k_ref[...]
    vx[inner, :] = v_ref[...]
    lx[:, inner] = lab_row_ref[...]
    for c in halo:
        c.wait()
    lx[:, low] = jnp.where(me == 0, -1, lx[:, low])
    lx[:, high] = jnp.where(me == n - 1, -1, lx[:, high])
    for i in range(rows // WINDOW + 2):
        chunk = slice(i * WINDOW, (i + 1) * WINDOW)
        square = jnp.broadcast_to(lx[0:1, chunk].astype(F32), (WINDOW, WINDOW))
        lc[chunk, :] = jnp.transpose(square)

    kv_local = k_ref.shape[1] // HEAD_DIM
    per_kv = q_ref.shape[1] // k_ref.shape[1]
    blocks = rows // WINDOW
    model = wout_ref.shape[1]

    def attend(b, carry):
        here = pl.ds(pl.multiple_of(b * WINDOW, WINDOW), WINDOW)
        wide = pl.ds(pl.multiple_of(b * WINDOW, WINDOW), 3 * WINDOW)
        q = q_ref[here, :]
        kw = kx[wide, :]
        vw = vx[wide, :]
        lab_k = lx[0:1, wide].astype(F32)
        lab_q = lc[pl.ds(pl.multiple_of(b * WINDOW + WINDOW, WINDOW), WINDOW), 0:1]
        key = lax.broadcasted_iota(jnp.int32, (WINDOW, 3 * WINDOW), 1) - WINDOW
        query = lax.broadcasted_iota(jnp.int32, (WINDOW, 3 * WINDOW), 0)
        allowed = (jnp.abs(key - query) <= WINDOW) & (lab_q == lab_k)
        results = []
        for g in range(kv_local):
            k = kw[:, g * HEAD_DIM:(g + 1) * HEAD_DIM]
            v = vw[:, g * HEAD_DIM:(g + 1) * HEAD_DIM]
            for j in range(per_kv):
                h = g * per_kv + j
                qh = q[:, h * HEAD_DIM:(h + 1) * HEAD_DIM]
                score = lax.dot_general(
                    qh, k, (((1,), (1,)), ((), ())), preferred_element_type=F32
                ) * HEAD_DIM ** (-0.5)
                score = jnp.where(allowed, score, NEG)
                sink = sink_ref[h]
                highest = jnp.maximum(jnp.max(score, axis=1, keepdims=True), sink)
                raw = jnp.where(allowed, jnp.exp(score - highest), 0.0)
                total = jnp.sum(raw, axis=1, keepdims=True) + jnp.exp(sink - highest)
                probs = (raw / total).astype(BF16)
                results.append(jnp.dot(probs, v, preferred_element_type=F32).astype(BF16))
        attended = jnp.concatenate(results, axis=1)
        part[here, :] = jnp.dot(attended, wout_ref[...], preferred_element_type=F32).astype(BF16)
        return carry

    split = blocks // 3
    for t in range(3):
        lax.fori_loop(t * split, (t + 1) * split if t < 2 else blocks, attend, 0)
        serve(2 if t == 1 else 1)

    tile = 32
    other_half = pl.ds((1 - core) * half, half)
    swap = remote(part.at[other_half], first, core_send, core_recv, (me, partner))
    swap.wait()

    def add_first(i, carry):
        r = pl.ds(pl.multiple_of(i * tile, tile), tile)
        o = pl.ds(pl.multiple_of(core * half + i * tile, tile), tile)
        first[r, :] = (part[o, :].astype(F32) + first[r, :].astype(F32)).astype(BF16)
        return carry

    lax.fori_loop(0, half // tile, add_first, 0)
    copies = []
    for j in range(1, ny):
        to = lax.rem(y + j, ny)
        copies.append(remote(
            first.at[pl.ds(to * piece, piece)], second.at[j - 1], y_send.at[j - 1], y_recv.at[j - 1], (me, to * 2 + core)
        ))
    serve(2)
    for c in copies:
        c.wait()

    def add_second(i, carry):
        r = pl.ds(pl.multiple_of(i * tile, tile), tile)
        s = first[pl.ds(pl.multiple_of(y * piece + i * tile, tile), tile), :].astype(F32)
        for j in range(ny - 1):
            s = s + second[j, r, :].astype(F32)
        o = pl.ds(pl.multiple_of(core * half + y * piece + i * tile, tile), tile)
        mixed[o, :] = (res[r, :].astype(F32) + s).astype(BF16)
        return carry

    lax.fori_loop(0, piece // tile, add_second, 0)
    mine = mixed.at[pl.ds(core * half + y * piece, piece)]
    copies = []
    for j in range(1, ny):
        to = lax.rem(y + j, ny)
        copies.append(remote(mine, mine, back_send.at[j - 1], back_recv.at[j - 1], (me, to * 2 + core)))
    serve(2)
    for j, c in enumerate(copies):
        c.wait_send()
        frm = lax.rem(y + ny - (j + 1), ny)
        theirs = mixed.at[pl.ds(core * half + frm * piece, piece)]
        pltpu.make_async_remote_copy(
            src_ref=theirs, dst_ref=theirs, send_sem=back_send.at[j], recv_sem=back_recv.at[j],
            device_id=(me, partner), device_id_type=MESH,
        ).wait_recv()
    own_half = mixed.at[pl.ds(core * half, half)]
    swap = remote(own_half, own_half, pair_send, pair_recv, (me, partner))
    swap.wait_send()
    their_half = mixed.at[other_half]
    pltpu.make_async_remote_copy(
        src_ref=their_half, dst_ref=their_half, send_sem=pair_send, recv_sem=pair_recv,
        device_id=(me, partner), device_id_type=MESH,
    ).wait_recv()

    def normalise(i, carry):
        r = pl.ds(pl.multiple_of(i * tile, tile), tile)
        m = mixed[r, :].astype(F32)
        mean_sq = jnp.mean(m * m, axis=1, keepdims=True)
        normed[r, :] = (m * lax.rsqrt(mean_sq + EPS) * gain_ref[...]).astype(BF16)
        return carry

    lax.fori_loop(0, rows // tile, normalise, 0)

    serve(2 * (n - 1) - done[0])
    big = rows // 3

    def project(t, which, dst):
        r = slice(t * big, (t + 1) * big)
        dst[r, :] = jnp.dot(normed[r, :], up[which], preferred_element_type=F32).astype(BF16)

    for t in range(3):
        project(t, 0, value)
        serve(1)
    tail = remote(value.at[pl.ds(rows - RIM, RIM)], rim.at[0], rim_send.at[0], rim_recv.at[0], (right, tp))
    head = remote(value.at[pl.ds(0, RIM)], rim.at[1], rim_send.at[1], rim_recv.at[1], (left, tp))
    for t in range(3):
        project(t, 1, gate)
        serve(1)
    tail.wait()
    head.wait()

    taps = taps_ref[...].astype(F32)
    step = 64
    before = rim[0, RIM - 1:RIM, :].astype(F32)

    def label(i, shift):
        return lc[WINDOW + i * step + shift:WINDOW + (i + 1) * step + shift, 0:1]

    for i in range(rows // step):
        r = slice(i * step, (i + 1) * step)
        x = value[r, :].astype(F32)
        after = (value[(i + 1) * step:(i + 1) * step + RIM, :] if (i + 1) * step < rows else rim[1, :, :])[0:1].astype(F32)
        prev = jnp.concatenate([before, x[:-1]], axis=0)
        nxt = jnp.concatenate([x[1:], after], axis=0)
        conv = (
            taps[0:1] * jnp.where(label(i, -1) == label(i, 0), prev, 0.0)
            + taps[1:2] * x
            + taps[2:3] * jnp.where(label(i, 1) == label(i, 0), nxt, 0.0)
        )
        gate[r, :] = (conv * jax.nn.sigmoid(conv) * gate[r, :].astype(F32)).astype(BF16)
        before = x[step - 1:step]
        if i % 3 == 2:
            serve(1)

    per_tp = n // ntp
    mine_rows = pl.ds(core * half, half)
    partner_rows = pl.ds((1 - core) * half, half)
    units = []
    for d in range(n):
        if d in (1, n - 1) and n > 2:
            units.append((2 * (n - 1) + 2 * (n - d), d, 0, 1))
            units.append((2 * (n - 1) + 2 * d, d, 1, 1))
        else:
            units.append((2 * (n - 1) + (2 * max(d, n - d) if d else 0), d, 0, 2))
    units.sort()

    def target(owner):
        to = owner // per_tp
        local = lax.rem(owner, per_tp)
        slot = lax.rem(tp - to + ntp, ntp) - 1
        return to, local, slot

    def lower(u):
        _, d, way, count = units[u]
        owner = place(lax.rem(pos + d, n))
        w = down[pl.ds(pl.multiple_of(owner * block + way * depth, depth), count * depth), :]

        def body(i, carry):
            r = pl.ds(pl.multiple_of(i * big, big), big)
            product = lax.dot_general(
                gate[r, :], w, (((1,), (1,)), ((), ())), preferred_element_type=F32
            ).astype(BF16)
            for j in range(count):
                pd[owner, way + j, r, :] = product[:, j * depth:(j + 1) * depth]
            return carry

        lax.fori_loop(0, 3, body, 0)
        return remote(
            pd.at[owner, pl.ds(way, count), partner_rows], box.at[owner, pl.ds(way, count)],
            down_send.at[u], down_recv.at[u], (me, partner),
        )

    def reduce(u, c):
        _, d, way, count = units[u]
        owner = place(lax.rem(pos + d, n))
        c.wait()

        def merge(i, carry):
            r = pl.ds(pl.multiple_of(i * tile, tile), tile)
            o = pl.ds(pl.multiple_of(core * half + i * tile, tile), tile)
            for j in range(way, way + count):
                pd[owner, j, o, :] = (pd[owner, j, o, :].astype(F32) + box[owner, j, r, :].astype(F32)).astype(BF16)
            return carry

        lax.fori_loop(0, half // tile, merge, 0, unroll=2)
        to, local, slot = target(owner)

        @pl.when(to != tp)
        def _():
            remote(
                pd.at[owner, pl.ds(way, count), mine_rows], inbox.at[local, slot, pl.ds(way, count)],
                out_send.at[u], out_recv.at[local, slot], (me, to),
            )

    waiting = None
    for u in range(len(units)):
        serve(units[u][0] - done[0])
        c = lower(u)
        if waiting is not None:
            reduce(*waiting)
        waiting = (u, c)
    reduce(*waiting)
    serve(len(queue))

    span = per_tp * block
    for local in range(per_tp):
        owner = tp * per_tp + local
        for slot in range(ntp - 1):
            ref = inbox.at[local, slot]
            pltpu.make_async_remote_copy(
                src_ref=ref, dst_ref=ref, send_sem=out_send.at[0], recv_sem=out_recv.at[local, slot],
                device_id=(me, partner), device_id_type=MESH,
            ).wait_recv()
        for same in range(2):
            base = (core if same else 1 - core) * half
            slots = range(1, ntp - 1, 2) if same else range(0, ntp - 1, 2)

            def finish(i, carry):
                r = pl.ds(pl.multiple_of(i * tile, tile), tile)
                o = pl.ds(pl.multiple_of(base + i * tile, tile), tile)
                kept = mixed[o, pl.ds(pl.multiple_of(tp * span, span), span)]
                for j in range(2):
                    s = sum(inbox[local, slot, j, r, :].astype(F32) for slot in slots)
                    if same:
                        s = s + pd[owner, j, o, :].astype(F32)
                    cols = slice(local * block + j * depth, local * block + (j + 1) * depth)
                    out_ref[o, cols] = (kept[:, cols].astype(F32) + s).astype(BF16)
                return carry

            lax.fori_loop(0, half // tile, finish, 0)
    for u, (_, d, way, count) in enumerate(units):
        owner = place(lax.rem(pos + d, n))
        to, local, slot = target(owner)

        @pl.when(to != tp)
        def _():
            ref = pd.at[owner, pl.ds(way, count), mine_rows]
            pltpu.make_async_remote_copy(
                src_ref=ref, dst_ref=ref, send_sem=out_send.at[u], recv_sem=out_recv.at[0, 0],
                device_id=(me, to), device_id_type=MESH,
            ).wait_send()
    for stream in range(4):
        for way in range(2):
            for s in range(n - 1):
                ring(stream, way, s, False).wait_send()


def paired_kernel(
    n, ntp,
    q_ref, k_ref, v_ref, sink_ref, lab_row_ref,
    res_hbm, wout_ref, gain_ref, wv_hbm, wg_hbm, taps_ref, wd_hbm,
    out_ref,
    w3, other, kx, vx, lx, lp, lc, same, part, first, second, mixed, normed, value, gate,
    pd, box, yin1, zin1, zin2, yin2, res,
    loc_sem, halo_send, halo_recv, lab_send, lab_recv, zs, zr, xs, xr,
    core_send, core_recv, y_send, y_recv, ag_send, ag_recv, rim_send, rim_recv,
    box_send, box_recv, yo1_send, yo1_recv, zo1_send, zo1_recv, zo2_send, zo2_recv, yo2_send, yo2_recv,
):
    me = lax.axis_index("sp")
    tp = lax.axis_index("tp")
    core = lax.rem(tp, 2)
    y = tp // 2
    z = me // 2
    x = lax.rem(me, 2)
    zh = z // 2
    own = lax.rem(z, 2)
    pair = 1 - own
    zp = 2 * zh + pair
    far_mid = 2 - zh
    far_end = 3 - 3 * zh
    partner = y * 2 + 1 - core
    across = (1 - y) * 2 + core
    beside = (zp * 2 + x, tp)
    sibling = (z * 2 + 1 - x, tp)
    rows, cols = q_ref.shape
    half = rows // 2
    piece = half // 2
    block, hidden = wv_hbm.shape
    wide = w3.shape[2]
    narrow = hidden - wide
    model = wout_ref.shape[1]
    span = out_ref.shape[1]
    is_mid = (z == 1) | (z == 2)
    is_end = (z == 0) | (z == 3)
    roles = ((is_end, narrow, wide, 0, narrow), (is_mid, wide, narrow, narrow, 0))

    def copy(src, dst, send, recv, where):
        return pltpu.make_async_remote_copy(
            src_ref=src, dst_ref=dst, send_sem=send, recv_sem=recv, device_id=where, device_id_type=MESH
        )

    def arrive(ref, recv):
        copy(ref, ref, core_send.at[0], recv, (me, partner)).wait_recv()

    def left(ref, send):
        copy(ref, ref, send, core_recv.at[0], (me, partner)).wait_send()

    def spot(s, zo, xo, width):
        return w3.at[s, pl.ds(pl.multiple_of((zo * 2 + xo) * block, block), block), pl.ds(0, width)]

    sources = (wv_hbm, wg_hbm, wd_hbm)

    def loads(s):
        for cond, width, rest, at, rest_at in roles:
            def pair_of():
                a = pltpu.make_async_copy(sources[s].at[:, pl.ds(at, width)], spot(s, z, x, width), loc_sem.at[s, 0])
                b = pltpu.make_async_copy(
                    sources[s].at[:, pl.ds(rest_at, rest)], other.at[s, :, pl.ds(0, rest)], loc_sem.at[s, 1]
                )
                return a, b
            yield cond, pair_of

    for s in range(3):
        for cond, pair_of in loads(s):
            @pl.when(cond)
            def _():
                for c in pair_of():
                    c.start()
    my_piece = core * half + y * piece
    res_load = pltpu.make_async_copy(res_hbm.at[pl.ds(pl.multiple_of(my_piece, piece), piece)], res, loc_sem.at[3, 0])
    res_load.start()

    barrier = pltpu.get_barrier_semaphore()
    peers = [(lax.rem(me + j, n), tp) for j in range(1, n)] + [(me, lax.rem(tp + j, ntp)) for j in range(1, ntp)]
    for peer in peers:
        pl.semaphore_signal(barrier, inc=1, device_id=peer, device_id_type=MESH)
    for s in range(3):
        for cond, pair_of in loads(s):
            @pl.when(cond)
            def _():
                for c in pair_of():
                    c.wait()
    res_load.wait()
    pl.semaphore_wait(barrier, len(peers))

    def begin(s):
        @pl.when(is_end)
        def _():
            copy(other.at[s, :, pl.ds(0, wide)], spot(s, z, x, wide), zs.at[s, 0], zr.at[s, 0], beside).start()
            a = spot(s, z, x, narrow)
            copy(a, a, zs.at[s, 1], zr.at[s, 2], ((3 - z) * 2 + x, tp)).start()
            copy(a, a, xs.at[s, 0], xr.at[s, 0], sibling).start()

        @pl.when(is_mid)
        def _():
            a = spot(s, z, x, wide)
            b = other.at[s, :, pl.ds(0, narrow)]
            copy(a, a, zs.at[s, 1], zr.at[s, 1], ((3 - z) * 2 + x, tp)).start()
            copy(b, spot(s, z, x, narrow), zs.at[s, 0], zr.at[s, 0], beside).start()
            copy(b, spot(s, z, x, narrow), zs.at[s, 2], zr.at[s, 1], ((3 - zp) * 2 + x, tp)).start()
            copy(a, a, xs.at[s, 0], xr.at[s, 0], sibling).start()

    owners = (zp, far_mid, far_end)

    def event(s, j):
        for cond, width, _, _, _ in roles:
            @pl.when(cond)
            def _():
                a = spot(s, owners[j], x, width)
                arrive(a, zr.at[s, j])
                copy(a, a, xs.at[s, j + 1], xr.at[s, j + 1], sibling).start()
        if j == 0:
            @pl.when(is_mid)
            def _():
                a = spot(s, zp, x, wide)
                copy(a, a, zs.at[s, 3], zr.at[s, 2], ((3 - z) * 2 + x, tp)).start()

    def xwait(s, j):
        for cond, width, _, _, _ in roles:
            @pl.when(cond)
            def _():
                arrive(spot(s, ((z,) + owners)[j], 1 - x, width), xr.at[s, j])

    def finish_stream(s):
        @pl.when(is_end)
        def _():
            left(spot(s, z, x, wide), zs.at[s, 0])
            left(spot(s, z, x, narrow), zs.at[s, 1])
            for j in range(4):
                left(spot(s, z, x, narrow), xs.at[s, j])

        @pl.when(is_mid)
        def _():
            left(spot(s, z, x, wide), zs.at[s, 1])
            left(spot(s, z, x, narrow), zs.at[s, 0])
            left(spot(s, z, x, narrow), zs.at[s, 2])
            left(spot(s, z, x, wide), zs.at[s, 3])
            for j in range(4):
                left(spot(s, z, x, wide), xs.at[s, j])

    right, before = lax.rem(me + 1, n), lax.rem(me + n - 1, n)
    ends = pl.ds(rows - WINDOW, WINDOW)
    starts = pl.ds(0, WINDOW)
    low, high = pl.ds(0, WINDOW), pl.ds(rows + WINDOW, WINDOW)
    halo = []
    for i, (src, dst) in enumerate(((k_ref, kx), (v_ref, vx))):
        halo.append(copy(src.at[ends], dst.at[low], halo_send.at[i, 0], halo_recv.at[i, 0], (right, tp)))
        halo.append(copy(src.at[starts], dst.at[high], halo_send.at[i, 1], halo_recv.at[i, 1], (before, tp)))
    halo.append(copy(lab_row_ref.at[:, ends], lx.at[:, low], halo_send.at[2, 0], halo_recv.at[2, 0], (right, tp)))
    halo.append(copy(lab_row_ref.at[:, starts], lx.at[:, high], halo_send.at[2, 1], halo_recv.at[2, 1], (before, tp)))
    for c in halo:
        c.start()
    begin(0)

    @pl.when(is_end)
    def _():
        if narrow < wide:
            w3[:, :, narrow:wide] = jnp.zeros((3, n * block, wide - narrow), BF16)

    inner = pl.ds(WINDOW, rows)
    kx[inner, :] = k_ref[...]
    vx[inner, :] = v_ref[...]
    lx[:, inner] = lab_row_ref[...]
    for c in halo:
        c.wait()
    lx[:, low] = jnp.where(me == 0, -1, lx[:, low])
    lx[:, high] = jnp.where(me == n - 1, -1, lx[:, high])
    lab_copy = copy(lx, lp, lab_send, lab_recv, beside)
    lab_copy.start()
    chunks = rows // WINDOW

    def columns(row_ref, slot):
        for i in range(chunks + 2):
            chunk = slice(i * WINDOW, (i + 1) * WINDOW)
            square = jnp.broadcast_to(row_ref[0:1, chunk].astype(F32), (WINDOW, WINDOW))
            lc[chunk, :] = jnp.transpose(square)
        for i in range(chunks):
            here = lc[WINDOW * (i + 1):WINDOW * (i + 2), :]
            for side, shift in ((0, -1), (1, 1)):
                there = lc[WINDOW * (i + 1) + shift:WINDOW * (i + 2) + shift, :]
                same[slot, side, i * WINDOW:(i + 1) * WINDOW, :] = jnp.where(here == there, 1.0, 0.0)

    columns(lx, own)

    kv_local = k_ref.shape[1] // HEAD_DIM
    per_kv = cols // k_ref.shape[1]
    per_half = chunks // 2
    tile = 32

    def attend(i, carry):
        own_half = i // per_half
        j = lax.rem(i, per_half)
        turn = (1 - y) * (per_half - 1 - j) + y * j
        b = ((1 - own_half) * (1 - core) + own_half * core) * per_half + turn
        here = pl.ds(pl.multiple_of(b * WINDOW, WINDOW), WINDOW)
        wide_keys = pl.ds(pl.multiple_of(b * WINDOW, WINDOW), 3 * WINDOW)
        q = q_ref[here, :]
        kw = kx[wide_keys, :]
        vw = vx[wide_keys, :]
        lab_k = lx[0:1, wide_keys].astype(F32)
        lab_q = lc[pl.ds(pl.multiple_of(b * WINDOW + WINDOW, WINDOW), WINDOW), 0:1]
        key = lax.broadcasted_iota(jnp.int32, (WINDOW, 3 * WINDOW), 1) - WINDOW
        query = lax.broadcasted_iota(jnp.int32, (WINDOW, 3 * WINDOW), 0)
        allowed = (jnp.abs(key - query) <= WINDOW) & (lab_q == lab_k)
        results = []
        for g in range(kv_local):
            k = kw[:, g * HEAD_DIM:(g + 1) * HEAD_DIM]
            v = vw[:, g * HEAD_DIM:(g + 1) * HEAD_DIM]
            for u in range(per_kv):
                h = g * per_kv + u
                qh = q[:, h * HEAD_DIM:(h + 1) * HEAD_DIM]
                score = lax.dot_general(
                    qh, k, (((1,), (1,)), ((), ())), preferred_element_type=F32
                ) * HEAD_DIM ** (-0.5)
                score = jnp.where(allowed, score, NEG)
                sink = sink_ref[h]
                highest = jnp.maximum(jnp.max(score, axis=1, keepdims=True), sink)
                raw = jnp.where(allowed, jnp.exp(score - highest), 0.0)
                total = jnp.sum(raw, axis=1, keepdims=True) + jnp.exp(sink - highest)
                probs = (raw / total).astype(BF16)
                results.append(jnp.dot(probs, v, preferred_element_type=F32).astype(BF16))
        attended = jnp.concatenate(results, axis=1)
        part[here, :] = jnp.dot(attended, wout_ref[...], preferred_element_type=F32).astype(BF16)
        mine = first.at[pl.ds(pl.multiple_of(turn * WINDOW, WINDOW), WINDOW)]

        @pl.when(own_half == 0)
        def _():
            copy(part.at[here], mine, core_send.at[j], core_recv.at[j], (me, partner)).start()

        @pl.when(own_half == 1)
        def _():
            arrive(mine, core_recv.at[j])

            def add(t, carry):
                r = pl.ds(pl.multiple_of(turn * WINDOW + t * tile, tile), tile)
                o = pl.ds(pl.multiple_of(b * WINDOW + t * tile, tile), tile)
                first[r, :] = (part[o, :].astype(F32) + first[r, :].astype(F32)).astype(BF16)
                return carry

            lax.fori_loop(0, WINDOW // tile, add, 0)

        @pl.when(i == per_half)
        def _():
            y_copy(0, y).start()

        @pl.when(i == per_half + 1)
        def _():
            y_copy(1, y).start()

        @pl.when(i == 1)
        def _():
            event(0, 0)
            begin(1)

        @pl.when(i == 3)
        def _():
            event(0, 1)

        return carry

    def y_copy(k, yy):
        if k == 0:
            count, src, dst = 2 * piece // 3, (1 - yy) * (half - 2 * piece // 3), (1 - yy) * (piece // 3)
        else:
            count, src, dst = piece // 3, 2 * piece // 3 + (1 - yy) * (piece // 3), yy * (2 * piece // 3)
        return copy(
            first.at[pl.ds(pl.multiple_of(src, 64), count)], second.at[pl.ds(pl.multiple_of(dst, 64), count)],
            y_send.at[k], y_recv.at[k], (me, across),
        )

    lax.fori_loop(0, 2 * per_half, attend, 0)
    event(1, 0)
    event(0, 2)
    lab_copy.wait()
    columns(lp, pair)
    for k in range(2):
        y_copy(k, 1 - y).wait_recv()

    def norm(slot, start, count):
        def body(i, carry):
            r = pl.ds(pl.multiple_of(start + i * tile, tile), tile)
            m = mixed[r, :].astype(F32)
            mean_sq = jnp.mean(m * m, axis=1, keepdims=True)
            normed[slot, r, :] = (m * lax.rsqrt(mean_sq + EPS) * gain_ref[...]).astype(BF16)
            return carry

        lax.fori_loop(0, count // tile, body, 0)

    def add_second(i, carry):
        r = pl.ds(pl.multiple_of(i * tile, tile), tile)
        f = pl.ds(pl.multiple_of(y * piece + i * tile, tile), tile)
        o = pl.ds(pl.multiple_of(my_piece + i * tile, tile), tile)
        s = first[f, :].astype(F32) + second[r, :].astype(F32)
        mixed[o, :] = (res[r, :].astype(F32) + s).astype(BF16)
        return carry

    lax.fori_loop(0, piece // tile, add_second, 0)

    def part_of(c, yy):
        return c * half + yy * piece

    def mixed_at(c, yy):
        return mixed.at[pl.ds(pl.multiple_of(part_of(c, yy), piece), piece)]

    def normed_at(slot, c, yy):
        return normed.at[slot, pl.ds(pl.multiple_of(part_of(c, yy), piece), piece)]

    def share(k, ref, where):
        copy(ref, ref, ag_send.at[k], ag_recv.at[k], where).start()

    share(0, mixed_at(core, y), (me, across))
    share(1, mixed_at(core, y), (me, partner))
    norm(own, my_piece, piece)
    share(2, normed_at(own, core, y), beside)
    begin(2)
    event(1, 1)
    arrive(mixed_at(1 - core, y), ag_recv.at[1])
    norm(own, part_of(1 - core, y), piece)
    arrive(mixed_at(core, 1 - y), ag_recv.at[0])
    share(3, mixed_at(core, 1 - y), (me, partner))
    norm(own, part_of(core, 1 - y), piece)
    arrive(normed_at(pair, core, y), ag_recv.at[2])
    share(4, normed_at(pair, core, y), (me, across))
    share(5, normed_at(pair, core, y), (me, partner))
    arrive(mixed_at(1 - core, 1 - y), ag_recv.at[3])
    norm(own, part_of(1 - core, 1 - y), piece)

    big = rows // 3

    def project(which, slot):
        def body(t, carry):
            r = pl.ds(pl.multiple_of(t * big, big), big)
            product = jnp.dot(normed[slot, r, :], w3[which], preferred_element_type=F32).astype(BF16)
            if which == 0:
                value[slot, pl.ds(pl.multiple_of(RIM + t * big, RIM), big), :] = product
            else:
                gate[slot, r, :] = product
            return carry

        lax.fori_loop(0, 3, body, 0)

    for j in range(4):
        xwait(0, j)
    project(0, own)
    event(1, 2)
    event(2, 0)
    arrive(normed_at(pair, core, 1 - y), ag_recv.at[4])
    share(6, normed_at(pair, core, 1 - y), (me, partner))
    for j in range(4):
        xwait(1, j)
    project(1, own)
    arrive(normed_at(pair, 1 - core, y), ag_recv.at[5])
    arrive(normed_at(pair, 1 - core, 1 - y), ag_recv.at[6])
    project(0, pair)

    inside = pl.ds(RIM, RIM)
    last = pl.ds(rows, RIM)
    fronts, backs = pl.ds(0, RIM), pl.ds(RIM + rows, RIM)
    facing = ((3 - z) * 2 + 1 - x, tp)
    rims = (
        (x == 0, ((0, last, 0, fronts, sibling), (1, inside, 0, backs, sibling),
                  (1, last, 1, fronts, sibling), (0, inside, 1, backs, facing))),
        (x == 1, ((0, inside, 0, backs, sibling), (0, last, 1, fronts, sibling),
                  (1, inside, 1, backs, sibling), (1, last, 0, fronts, facing))),
    )
    for cond, sends in rims:
        @pl.when(cond)
        def _():
            for frm, rs, to, rd, where in sends:
                pad = 2 * to + (0 if rd is fronts else 1)
                copy(value.at[frm, rs], value.at[to, rd], rim_send.at[pad], rim_recv.at[pad], where).start()

    project(1, pair)
    event(2, 1)
    for slot in range(2):
        for side, rd in enumerate((fronts, backs)):
            arrive(value.at[slot, rd], rim_recv.at[2 * slot + side])

    taps_all = taps_ref[...].astype(F32)
    taps = jnp.where(is_mid, taps_all[:, narrow:], taps_all[:, :wide])
    step = 64
    lanes = wide // WINDOW

    for slot in range(2):
        def gated(i, carry):
            base = i * step
            r = pl.ds(pl.multiple_of(base, step), step)
            x_rows = value[slot, pl.ds(pl.multiple_of(RIM + base, RIM), step), :].astype(F32)
            above = value[slot, pl.ds(pl.multiple_of(base, RIM), RIM), :].astype(F32)[RIM - 1:RIM]
            below = value[slot, pl.ds(pl.multiple_of(RIM + base + step, RIM), RIM), :].astype(F32)[0:1]
            prev = jnp.concatenate([above, x_rows[:-1]], axis=0)
            nxt = jnp.concatenate([x_rows[1:], below], axis=0)
            with_prev = jnp.concatenate([same[slot, 0, r, :]] * lanes, axis=1) > 0.5
            with_next = jnp.concatenate([same[slot, 1, r, :]] * lanes, axis=1) > 0.5
            conv = (
                taps[0:1] * jnp.where(with_prev, prev, 0.0)
                + taps[1:2] * x_rows
                + taps[2:3] * jnp.where(with_next, nxt, 0.0)
            )
            gate[slot, r, :] = (conv * jax.nn.sigmoid(conv) * gate[slot, r, :].astype(F32)).astype(BF16)
            return carry

        lax.fori_loop(0, rows // step, gated, 0)

    order = (1 + zh, 3 * zh, far_mid, far_end)
    quarter = rows // 2

    def lower(u):
        t = order[u]
        w = w3[2, pl.ds(pl.multiple_of(t * span, span), span), :]
        for slot in range(2):
            def body(i, carry):
                r = pl.ds(pl.multiple_of(i * big, big), big)
                pd[u, slot, r, :] = lax.dot_general(
                    gate[slot, r, :], w, (((1,), (1,)), ((), ())), preferred_element_type=F32
                ).astype(BF16)
                return carry

            lax.fori_loop(0, 3, body, 0)

        @pl.when(core != lax.rem(t, 2))
        def _():
            copy(pd.at[u], box.at[u // 2], box_send.at[u], box_recv.at[u // 2], (me, partner)).start()

    def rows_of(ref, at):
        return ref.at[pl.ds(at, quarter)]

    def merge(count, body):
        def step_rows(i, carry):
            body(pl.ds(pl.multiple_of(i * tile, tile), tile), pl.ds(pl.multiple_of(quarter + i * tile, tile), tile))
            return carry

        lax.fori_loop(0, count // tile, step_rows, 0)

    upper, under = pl.ds(0, quarter), pl.ds(quarter, quarter)

    def stage_one(u):
        t = order[u]
        target_y = t // 2

        @pl.when(core == lax.rem(t, 2))
        def _():
            arrive(box.at[u // 2], box_recv.at[u // 2])

            def add(slot, lo):
                def body(i, carry):
                    r = pl.ds(pl.multiple_of(lo + i * tile, tile), tile)
                    pd[u, slot, r, :] = (
                        pd[u, slot, r, :].astype(F32) + box[u // 2, slot, r, :].astype(F32)
                    ).astype(BF16)
                    return carry

                lax.fori_loop(0, quarter // tile, body, 0)

            add(pair, quarter)
            copy(pd.at[u, pair, under], zin1.at[u // 2], zo1_send.at[u // 2], zo1_recv.at[u // 2], beside).start()
            add(0, 0)
            add(1, 0)

            @pl.when(y != target_y)
            def _():
                copy(pd.at[u, :, upper], yin1, yo1_send, yo1_recv, (me, across)).start()

            add(own, quarter)

    def stage_two(u):
        t = order[u]
        target_y = t // 2

        @pl.when(core == lax.rem(t, 2))
        def _():
            @pl.when(y == target_y)
            def _():
                arrive(yin1, yo1_recv)

                def body(slot):
                    def inner_body(i, carry):
                        r = pl.ds(pl.multiple_of(i * tile, tile), tile)
                        pd[u, slot, r, :] = (
                            pd[u, slot, r, :].astype(F32) + yin1[slot, r, :].astype(F32)
                        ).astype(BF16)
                        return carry

                    lax.fori_loop(0, quarter // tile, inner_body, 0)

                body(pair)
                copy(pd.at[u, pair, upper], zin2, zo2_send, zo2_recv, beside).start()
                body(own)

            arrive(zin1.at[u // 2], zo1_recv.at[u // 2])

            def add(i, carry):
                r = pl.ds(pl.multiple_of(i * tile, tile), tile)
                o = pl.ds(pl.multiple_of(quarter + i * tile, tile), tile)
                pd[u, own, o, :] = (
                    pd[u, own, o, :].astype(F32) + zin1[u // 2, r, :].astype(F32)
                ).astype(BF16)
                return carry

            lax.fori_loop(0, quarter // tile, add, 0)

            @pl.when(y != target_y)
            def _():
                copy(pd.at[u, own, under], yin2, yo2_send, yo2_recv, (me, across)).start()

    def stage_three(u):
        t = order[u]

        @pl.when(tp == t)
        def _():
            arrive(zin2, zo2_recv)
            arrive(yin2, yo2_recv)
            for at, extra in ((0, zin2), (quarter, yin2)):
                def body(i, carry):
                    r = pl.ds(pl.multiple_of(i * tile, tile), tile)
                    o = pl.ds(pl.multiple_of(at + i * tile, tile), tile)
                    kept = mixed[o, pl.ds(pl.multiple_of(t * span, span), span)].astype(F32)
                    s = pd[u, own, o, :].astype(F32) + extra[r, :].astype(F32)
                    out_ref[o, :] = (kept + s).astype(BF16)
                    return carry

                lax.fori_loop(0, quarter // tile, body, 0)

    def drain(u):
        t = order[u]

        @pl.when(core != lax.rem(t, 2))
        def _():
            left(pd.at[u], box_send.at[u])

        @pl.when(core == lax.rem(t, 2))
        def _():
            left(pd.at[u, pair, under], zo1_send.at[u // 2])

            @pl.when(y != t // 2)
            def _():
                left(pd.at[u, :, upper], yo1_send)
                left(pd.at[u, own, under], yo2_send)

            @pl.when(y == t // 2)
            def _():
                left(pd.at[u, pair, upper], zo2_send)

    xwait(2, 0)
    xwait(2, 1)
    lower(0)
    lower(1)
    stage_one(0)
    stage_one(1)
    event(2, 2)
    xwait(2, 2)
    lower(2)
    stage_two(0)
    stage_two(1)
    stage_one(2)
    xwait(2, 3)
    lower(3)
    stage_one(3)
    stage_three(0)
    stage_three(1)
    stage_two(2)
    stage_two(3)
    stage_three(2)
    stage_three(3)

    for s in range(3):
        finish_stream(s)
    for j in range(per_half):
        left(first.at[pl.ds(0, WINDOW)], core_send.at[j])
    for k in range(2):
        y_copy(k, y).wait_send()
    for k in range(7):
        left(mixed_at(core, y), ag_send.at[k])
    for pad in range(4):
        left(value.at[0, fronts], rim_send.at[pad])
    for u in range(4):
        drain(u)


def solution(mesh):
    n, ntp = mesh.shape["sp"], mesh.shape["tp"]

    def by_ring(q, k, v, sink, doc, res, wout, gain, wv, wg, taps, wd):
        rows, model = res.shape
        hidden = wv.shape[1]
        block = wv.shape[0]
        ny = ntp // 2
        labels = doc + 1
        lab_row = labels[None, :]
        vm = pl.BlockSpec(memory_space=pltpu.VMEM)
        hbm = pl.BlockSpec(memory_space=pl.ANY)
        smem = pl.BlockSpec(memory_space=pltpu.SMEM)
        dma = pltpu.SemaphoreType.DMA
        kvc = k.shape[1]
        span = model // ntp
        scratch = [
            pltpu.VMEM((2, n * block, hidden), BF16),
            pltpu.VMEM((n * block, hidden), BF16),
            pltpu.VMEM((rows + 2 * WINDOW, kvc), BF16),
            pltpu.VMEM((rows + 2 * WINDOW, kvc), BF16),
            pltpu.VMEM((1, rows + 2 * WINDOW), jnp.int32),
            pltpu.VMEM((rows + 2 * WINDOW, WINDOW), F32),
            pltpu.VMEM((rows, model), BF16),
            pltpu.VMEM((rows // 2, model), BF16),
            pltpu.VMEM((max(ny - 1, 1), rows // 2 // ny, model), BF16),
            pltpu.VMEM((rows, model), BF16),
            pltpu.VMEM((rows, model), BF16),
            pltpu.VMEM((rows, hidden), BF16),
            pltpu.VMEM((rows, hidden), BF16),
            pltpu.VMEM((2, RIM, hidden), BF16),
            pltpu.VMEM((n, 2, rows, block // 2), BF16),
            pltpu.VMEM((n, 2, rows // 2, block // 2), BF16),
            pltpu.VMEM((n // ntp, ntp - 1, 2, rows // 2, block // 2), BF16),
            pltpu.VMEM((rows // 2 // ny, model), BF16),
            dma((4,)),
            dma((4, 2, n - 1)), dma((4, 2, n - 1)),
            dma((3, 2)), dma((3, 2)),
            dma((2,)), dma((2,)),
            dma, dma,
            dma((ny,)), dma((ny,)),
            dma((ny,)), dma((ny,)),
            dma, dma,
            dma((n + 2,)), dma((n + 2,)),
            dma((n + 2,)), dma((n // ntp, ntp - 1)),
        ]
        return pl.pallas_call(
            functools.partial(ring_kernel, n, ntp),
            out_shape=jax.ShapeDtypeStruct((rows, span), BF16),
            in_specs=[vm, vm, vm, smem, vm, hbm, vm, vm, hbm, hbm, vm, hbm],
            out_specs=vm,
            scratch_shapes=scratch,
            compiler_params=pltpu.CompilerParams(
                collective_id=0, has_side_effects=True, vmem_limit_bytes=67043328
            ),
            name="layer",
        )(q, k, v, sink, lab_row, res, wout, gain[None, :], wv, wg, taps, wd)


    def by_pairs(q, k, v, sink, doc, res, wout, gain, wv, wg, taps, wd):
        rows, model = res.shape
        block, hidden = wv.shape
        half = rows // 2
        piece = half // 2
        span = model // ntp
        kvc = k.shape[1]
        wide = (hidden // LANES + 1) // 2 * LANES
        lab_row = (doc + 1)[None, :]
        vm = pl.BlockSpec(memory_space=pltpu.VMEM)
        hbm = pl.BlockSpec(memory_space=pl.ANY)
        smem = pl.BlockSpec(memory_space=pltpu.SMEM)
        dma = pltpu.SemaphoreType.DMA
        scratch = [
            pltpu.VMEM((3, n * block, wide), BF16),
            pltpu.VMEM((3, block, wide), BF16),
            pltpu.VMEM((rows + 2 * WINDOW, kvc), BF16),
            pltpu.VMEM((rows + 2 * WINDOW, kvc), BF16),
            pltpu.VMEM((1, rows + 2 * WINDOW), jnp.int32),
            pltpu.VMEM((1, rows + 2 * WINDOW), jnp.int32),
            pltpu.VMEM((rows + 2 * WINDOW, WINDOW), F32),
            pltpu.VMEM((2, 2, rows, WINDOW), F32),
            pltpu.VMEM((rows, model), BF16),
            pltpu.VMEM((half, model), BF16),
            pltpu.VMEM((piece, model), BF16),
            pltpu.VMEM((rows, model), BF16),
            pltpu.VMEM((2, rows, model), BF16),
            pltpu.VMEM((2, rows + 2 * RIM, wide), BF16),
            pltpu.VMEM((2, rows, wide), BF16),
            pltpu.VMEM((4, 2, rows, span), BF16),
            pltpu.VMEM((2, 2, rows, span), BF16),
            pltpu.VMEM((2, half, span), BF16),
            pltpu.VMEM((2, half, span), BF16),
            pltpu.VMEM((half, span), BF16),
            pltpu.VMEM((half, span), BF16),
            pltpu.VMEM((piece, model), BF16),
            dma((4, 2)),
            dma((3, 2)), dma((3, 2)),
            dma, dma,
            dma((3, 4)), dma((3, 3)),
            dma((3, 4)), dma((3, 4)),
            dma((rows // WINDOW // 2,)), dma((rows // WINDOW // 2,)),
            dma((2,)), dma((2,)),
            dma((7,)), dma((7,)),
            dma((4,)), dma((4,)),
            dma((4,)), dma((2,)),
            dma, dma,
            dma((2,)), dma((2,)),
            dma, dma,
            dma, dma,
        ]
        return pl.pallas_call(
            functools.partial(paired_kernel, n, ntp),
            out_shape=jax.ShapeDtypeStruct((rows, span), BF16),
            in_specs=[vm, vm, vm, smem, vm, hbm, vm, vm, hbm, hbm, vm, hbm],
            out_specs=vm,
            scratch_shapes=scratch,
            compiler_params=pltpu.CompilerParams(
                collective_id=0, has_side_effects=True, vmem_limit_bytes=67043328
            ),
            name="layer",
        )(q, k, v, sink, lab_row, res, wout, gain[None, :], wv, wg, taps, wd)

    placed = (
        P("sp", "tp"), P("sp", "tp"), P("sp", "tp"), P("tp"), P("sp"), P("sp", None),
        P("tp", None), P(), P("sp", "tp"), P("sp", "tp"), P(None, "tp"), P("sp", "tp"),
    )
    return jax.shard_map(
        by_pairs if (n, ntp) == (8, 4) else by_ring, mesh=mesh, in_specs=placed, out_specs=P("sp", "tp"), check_vma=False
    )
```

```python
import functools

import jax
import jax.numpy as jnp
from jax import lax
from jax.experimental import pallas as pl
from jax.experimental.pallas import tpu as pltpu
from jax.sharding import PartitionSpec as P

HEAD_DIM = 64
WINDOW = 128
EPS = 1e-06
NEG = -1e30
RIM = 16
LANES = 128
MESH = pl.DeviceIdType.MESH
F32 = jnp.float32
BF16 = jnp.bfloat16


def ring_kernel(
    n, ntp,
    q_ref, k_ref, v_ref, sink_ref, lab_row_ref,
    res_hbm, wout_ref, gain_ref, wv_hbm, wg_hbm, taps_ref, wd_hbm,
    out_ref,
    up, down, kx, vx, lx, lc, part, first, second, mixed, normed, value, gate, rim, pd, box, inbox, res,
    loc_sem, ring_send, ring_recv, halo_send, halo_recv, rim_send, rim_recv,
    core_send, core_recv, y_send, y_recv, back_send, back_recv, pair_send, pair_recv,
    down_send, down_recv, out_send, out_recv,
):
    me = lax.axis_index("sp")
    tp = lax.axis_index("tp")
    core = lax.rem(tp, 2)
    y = tp // 2
    ny = ntp // 2
    partner = y * 2 + 1 - core
    rows = q_ref.shape[0]
    half = rows // 2
    piece = half // ny
    block = wv_hbm.shape[0]
    depth = block // 2
    quarter = block // 4

    def place(p):
        h = p // (n // 2)
        return (1 - h) * (2 * p) + h * (2 * n - 1 - 2 * p)

    odd = lax.rem(me, 2)
    pos = (1 - odd) * (me // 2) + odd * ((2 * n - 1 - me) // 2)
    ahead = place(lax.rem(pos + 1, n))
    behind = place(lax.rem(pos + n - 1, n))
    right = lax.rem(me + 1, n)
    left = lax.rem(me + n - 1, n)

    loads = []
    for i, (src, dst) in enumerate((
        (wv_hbm, up.at[0, pl.ds(me * block, block)]),
        (wg_hbm, up.at[1, pl.ds(me * block, block)]),
        (wd_hbm, down.at[pl.ds(me * block, block)]),
        (res_hbm.at[pl.ds(core * half + y * piece, piece)], res),
    )):
        c = pltpu.make_async_copy(src, dst, loc_sem.at[i])
        c.start()
        loads.append(c)

    barrier = pltpu.get_barrier_semaphore()
    peers = [(ahead, tp), (behind, tp), (right, tp), (left, tp)]
    for j in range(1, ntp):
        peers.append((me, lax.rem(tp + j, ntp)))
    for peer in peers:
        pl.semaphore_signal(barrier, inc=1, device_id=peer, device_id_type=MESH)
    for c in loads:
        c.wait()
    pl.semaphore_wait(barrier, len(peers))

    def spot(stream, way, owner):
        if stream < 2:
            return up.at[stream, pl.ds(owner * block + way * depth, depth)]
        return down.at[pl.ds(owner * block + way * depth + (stream - 2) * quarter, quarter)]

    def ring(stream, way, s, arriving):
        shift = s + 1 if arriving else s
        owner = place(lax.rem(pos + n - shift, n)) if way == 0 else place(lax.rem(pos + shift, n))
        ref = spot(stream, way, owner)
        return pltpu.make_async_remote_copy(
            src_ref=ref, dst_ref=ref,
            send_sem=ring_send.at[stream, way, s], recv_sem=ring_recv.at[stream, way, s],
            device_id=(ahead if way == 0 else behind, tp), device_id_type=MESH,
        )

    def begin(stream):
        for way in range(2):
            ring(stream, way, 0, False).start()

    def forward(stream, s, last=False):
        for way in range(2):
            ring(stream, way, s, True).wait_recv()
            if not last:
                ring(stream, way, s + 1, False).start()

    queue = []
    for s in range(n - 1):
        for stream in (0, 1):
            queue.append((stream, s))
    for s in range(n - 1):
        for stream in (2, 3):
            queue.append((stream, s))
    done = [0]

    def serve(count):
        for _ in range(count):
            if done[0] == len(queue):
                return
            stream, s = queue[done[0]]
            done[0] += 1
            forward(stream, s, last=s == n - 2)
            if stream < 2 and s == n - 2:
                begin(stream + 2)

    halo = []

    def remote(src, dst, send, recv, where):
        c = pltpu.make_async_remote_copy(
            src_ref=src, dst_ref=dst, send_sem=send, recv_sem=recv, device_id=where, device_id_type=MESH
        )
        c.start()
        return c

    ends = pl.ds(rows - WINDOW, WINDOW)
    starts = pl.ds(0, WINDOW)
    low, high = pl.ds(0, WINDOW), pl.ds(rows + WINDOW, WINDOW)
    for i, (src, dst) in enumerate(((k_ref, kx), (v_ref, vx))):
        halo.append(remote(src.at[ends], dst.at[low], halo_send.at[i, 0], halo_recv.at[i, 0], (right, tp)))
        halo.append(remote(src.at[starts], dst.at[high], halo_send.at[i, 1], halo_recv.at[i, 1], (left, tp)))
    halo.append(remote(lab_row_ref.at[:, ends], lx.at[:, low], halo_send.at[2, 0], halo_recv.at[2, 0], (right, tp)))
    halo.append(remote(lab_row_ref.at[:, starts], lx.at[:, high], halo_send.at[2, 1], halo_recv.at[2, 1], (left, tp)))
    begin(0)
    begin(1)
    inner = pl.ds(WINDOW, rows)
    kx[inner, :] = k_ref[...]
    vx[inner, :] = v_ref[...]
    lx[:, inner] = lab_row_ref[...]
    for c in halo:
        c.wait()
    lx[:, low] = jnp.where(me == 0, -1, lx[:, low])
    lx[:, high] = jnp.where(me == n - 1, -1, lx[:, high])
    for i in range(rows // WINDOW + 2):
        chunk = slice(i * WINDOW, (i + 1) * WINDOW)
        square = jnp.broadcast_to(lx[0:1, chunk].astype(F32), (WINDOW, WINDOW))
        lc[chunk, :] = jnp.transpose(square)

    kv_local = k_ref.shape[1] // HEAD_DIM
    per_kv = q_ref.shape[1] // k_ref.shape[1]
    blocks = rows // WINDOW
    model = wout_ref.shape[1]

    def attend(b, carry):
        here = pl.ds(pl.multiple_of(b * WINDOW, WINDOW), WINDOW)
        wide = pl.ds(pl.multiple_of(b * WINDOW, WINDOW), 3 * WINDOW)
        q = q_ref[here, :]
        kw = kx[wide, :]
        vw = vx[wide, :]
        lab_k = lx[0:1, wide].astype(F32)
        lab_q = lc[pl.ds(pl.multiple_of(b * WINDOW + WINDOW, WINDOW), WINDOW), 0:1]
        key = lax.broadcasted_iota(jnp.int32, (WINDOW, 3 * WINDOW), 1) - WINDOW
        query = lax.broadcasted_iota(jnp.int32, (WINDOW, 3 * WINDOW), 0)
        allowed = (jnp.abs(key - query) <= WINDOW) & (lab_q == lab_k)
        results = []
        for g in range(kv_local):
            k = kw[:, g * HEAD_DIM:(g + 1) * HEAD_DIM]
            v = vw[:, g * HEAD_DIM:(g + 1) * HEAD_DIM]
            for j in range(per_kv):
                h = g * per_kv + j
                qh = q[:, h * HEAD_DIM:(h + 1) * HEAD_DIM]
                score = lax.dot_general(
                    qh, k, (((1,), (1,)), ((), ())), preferred_element_type=F32
                ) * HEAD_DIM ** (-0.5)
                score = jnp.where(allowed, score, NEG)
                sink = sink_ref[h]
                highest = jnp.maximum(jnp.max(score, axis=1, keepdims=True), sink)
                raw = jnp.where(allowed, jnp.exp(score - highest), 0.0)
                total = jnp.sum(raw, axis=1, keepdims=True) + jnp.exp(sink - highest)
                probs = (raw / total).astype(BF16)
                results.append(jnp.dot(probs, v, preferred_element_type=F32).astype(BF16))
        attended = jnp.concatenate(results, axis=1)
        part[here, :] = jnp.dot(attended, wout_ref[...], preferred_element_type=F32).astype(BF16)
        return carry

    split = blocks // 3
    for t in range(3):
        lax.fori_loop(t * split, (t + 1) * split if t < 2 else blocks, attend, 0)
        serve(2 if t == 1 else 1)

    tile = 32
    other_half = pl.ds((1 - core) * half, half)
    swap = remote(part.at[other_half], first, core_send, core_recv, (me, partner))
    swap.wait()

    def add_first(i, carry):
        r = pl.ds(pl.multiple_of(i * tile, tile), tile)
        o = pl.ds(pl.multiple_of(core * half + i * tile, tile), tile)
        first[r, :] = (part[o, :].astype(F32) + first[r, :].astype(F32)).astype(BF16)
        return carry

    lax.fori_loop(0, half // tile, add_first, 0)
    copies = []
    for j in range(1, ny):
        to = lax.rem(y + j, ny)
        copies.append(remote(
            first.at[pl.ds(to * piece, piece)], second.at[j - 1], y_send.at[j - 1], y_recv.at[j - 1], (me, to * 2 + core)
        ))
    serve(2)
    for c in copies:
        c.wait()

    def add_second(i, carry):
        r = pl.ds(pl.multiple_of(i * tile, tile), tile)
        s = first[pl.ds(pl.multiple_of(y * piece + i * tile, tile), tile), :].astype(F32)
        for j in range(ny - 1):
            s = s + second[j, r, :].astype(F32)
        o = pl.ds(pl.multiple_of(core * half + y * piece + i * tile, tile), tile)
        mixed[o, :] = (res[r, :].astype(F32) + s).astype(BF16)
        return carry

    lax.fori_loop(0, piece // tile, add_second, 0)
    mine = mixed.at[pl.ds(core * half + y * piece, piece)]
    copies = []
    for j in range(1, ny):
        to = lax.rem(y + j, ny)
        copies.append(remote(mine, mine, back_send.at[j - 1], back_recv.at[j - 1], (me, to * 2 + core)))
    serve(2)
    for j, c in enumerate(copies):
        c.wait_send()
        frm = lax.rem(y + ny - (j + 1), ny)
        theirs = mixed.at[pl.ds(core * half + frm * piece, piece)]
        pltpu.make_async_remote_copy(
            src_ref=theirs, dst_ref=theirs, send_sem=back_send.at[j], recv_sem=back_recv.at[j],
            device_id=(me, partner), device_id_type=MESH,
        ).wait_recv()
    own_half = mixed.at[pl.ds(core * half, half)]
    swap = remote(own_half, own_half, pair_send, pair_recv, (me, partner))
    swap.wait_send()
    their_half = mixed.at[other_half]
    pltpu.make_async_remote_copy(
        src_ref=their_half, dst_ref=their_half, send_sem=pair_send, recv_sem=pair_recv,
        device_id=(me, partner), device_id_type=MESH,
    ).wait_recv()

    def normalise(i, carry):
        r = pl.ds(pl.multiple_of(i * tile, tile), tile)
        m = mixed[r, :].astype(F32)
        mean_sq = jnp.mean(m * m, axis=1, keepdims=True)
        normed[r, :] = (m * lax.rsqrt(mean_sq + EPS) * gain_ref[...]).astype(BF16)
        return carry

    lax.fori_loop(0, rows // tile, normalise, 0)

    serve(2 * (n - 1) - done[0])
    big = rows // 3

    def project(t, which, dst):
        r = slice(t * big, (t + 1) * big)
        dst[r, :] = jnp.dot(normed[r, :], up[which], preferred_element_type=F32).astype(BF16)

    for t in range(3):
        project(t, 0, value)
        serve(1)
    tail = remote(value.at[pl.ds(rows - RIM, RIM)], rim.at[0], rim_send.at[0], rim_recv.at[0], (right, tp))
    head = remote(value.at[pl.ds(0, RIM)], rim.at[1], rim_send.at[1], rim_recv.at[1], (left, tp))
    for t in range(3):
        project(t, 1, gate)
        serve(1)
    tail.wait()
    head.wait()

    taps = taps_ref[...].astype(F32)
    step = 64
    before = rim[0, RIM - 1:RIM, :].astype(F32)

    def label(i, shift):
        return lc[WINDOW + i * step + shift:WINDOW + (i + 1) * step + shift, 0:1]

    for i in range(rows // step):
        r = slice(i * step, (i + 1) * step)
        x = value[r, :].astype(F32)
        after = (value[(i + 1) * step:(i + 1) * step + RIM, :] if (i + 1) * step < rows else rim[1, :, :])[0:1].astype(F32)
        prev = jnp.concatenate([before, x[:-1]], axis=0)
        nxt = jnp.concatenate([x[1:], after], axis=0)
        conv = (
            taps[0:1] * jnp.where(label(i, -1) == label(i, 0), prev, 0.0)
            + taps[1:2] * x
            + taps[2:3] * jnp.where(label(i, 1) == label(i, 0), nxt, 0.0)
        )
        gate[r, :] = (conv * jax.nn.sigmoid(conv) * gate[r, :].astype(F32)).astype(BF16)
        before = x[step - 1:step]
        if i % 3 == 2:
            serve(1)

    per_tp = n // ntp
    mine_rows = pl.ds(core * half, half)
    partner_rows = pl.ds((1 - core) * half, half)
    units = []
    for d in range(n):
        if d in (1, n - 1) and n > 2:
            units.append((2 * (n - 1) + 2 * (n - d), d, 0, 1))
            units.append((2 * (n - 1) + 2 * d, d, 1, 1))
        else:
            units.append((2 * (n - 1) + (2 * max(d, n - d) if d else 0), d, 0, 2))
    units.sort()

    def target(owner):
        to = owner // per_tp
        local = lax.rem(owner, per_tp)
        slot = lax.rem(tp - to + ntp, ntp) - 1
        return to, local, slot

    def lower(u):
        _, d, way, count = units[u]
        owner = place(lax.rem(pos + d, n))
        w = down[pl.ds(pl.multiple_of(owner * block + way * depth, depth), count * depth), :]

        def body(i, carry):
            r = pl.ds(pl.multiple_of(i * big, big), big)
            product = lax.dot_general(
                gate[r, :], w, (((1,), (1,)), ((), ())), preferred_element_type=F32
            ).astype(BF16)
            for j in range(count):
                pd[owner, way + j, r, :] = product[:, j * depth:(j + 1) * depth]
            return carry

        lax.fori_loop(0, 3, body, 0)
        return remote(
            pd.at[owner, pl.ds(way, count), partner_rows], box.at[owner, pl.ds(way, count)],
            down_send.at[u], down_recv.at[u], (me, partner),
        )

    def reduce(u, c):
        _, d, way, count = units[u]
        owner = place(lax.rem(pos + d, n))
        c.wait()

        def merge(i, carry):
            r = pl.ds(pl.multiple_of(i * tile, tile), tile)
            o = pl.ds(pl.multiple_of(core * half + i * tile, tile), tile)
            for j in range(way, way + count):
                pd[owner, j, o, :] = (pd[owner, j, o, :].astype(F32) + box[owner, j, r, :].astype(F32)).astype(BF16)
            return carry

        lax.fori_loop(0, half // tile, merge, 0, unroll=2)
        to, local, slot = target(owner)

        @pl.when(to != tp)
        def _():
            remote(
                pd.at[owner, pl.ds(way, count), mine_rows], inbox.at[local, slot, pl.ds(way, count)],
                out_send.at[u], out_recv.at[local, slot], (me, to),
            )

    waiting = None
    for u in range(len(units)):
        serve(units[u][0] - done[0])
        c = lower(u)
        if waiting is not None:
            reduce(*waiting)
        waiting = (u, c)
    reduce(*waiting)
    serve(len(queue))

    span = per_tp * block
    for local in range(per_tp):
        owner = tp * per_tp + local
        for slot in range(ntp - 1):
            ref = inbox.at[local, slot]
            pltpu.make_async_remote_copy(
                src_ref=ref, dst_ref=ref, send_sem=out_send.at[0], recv_sem=out_recv.at[local, slot],
                device_id=(me, partner), device_id_type=MESH,
            ).wait_recv()
        for same in range(2):
            base = (core if same else 1 - core) * half
            slots = range(1, ntp - 1, 2) if same else range(0, ntp - 1, 2)

            def finish(i, carry):
                r = pl.ds(pl.multiple_of(i * tile, tile), tile)
                o = pl.ds(pl.multiple_of(base + i * tile, tile), tile)
                kept = mixed[o, pl.ds(pl.multiple_of(tp * span, span), span)]
                for j in range(2):
                    s = sum(inbox[local, slot, j, r, :].astype(F32) for slot in slots)
                    if same:
                        s = s + pd[owner, j, o, :].astype(F32)
                    cols = slice(local * block + j * depth, local * block + (j + 1) * depth)
                    out_ref[o, cols] = (kept[:, cols].astype(F32) + s).astype(BF16)
                return carry

            lax.fori_loop(0, half // tile, finish, 0)
    for u, (_, d, way, count) in enumerate(units):
        owner = place(lax.rem(pos + d, n))
        to, local, slot = target(owner)

        @pl.when(to != tp)
        def _():
            ref = pd.at[owner, pl.ds(way, count), mine_rows]
            pltpu.make_async_remote_copy(
                src_ref=ref, dst_ref=ref, send_sem=out_send.at[u], recv_sem=out_recv.at[0, 0],
                device_id=(me, to), device_id_type=MESH,
            ).wait_send()
    for stream in range(4):
        for way in range(2):
            for s in range(n - 1):
                ring(stream, way, s, False).wait_send()


def paired_kernel(
    n, ntp,
    q_hbm, k_ref, v_ref, sink_ref, lab_row_ref,
    res_hbm, wout_hbm, gain_ref, wv_hbm, wg_hbm, taps_ref, wd_hbm,
    out_ref,
    w3, other, kx, vx, lx, lp, lc, same, part, first, second, mixed, normed, value, gate,
    pd, box, yin1, zin1, zin2, yin2, res, q_ref, wout_ref,
    loc_sem, halo_send, halo_recv, lab_send, lab_recv, zs, zr, xs, xr,
    core_send, core_recv, y_send, y_recv, ag_send, ag_recv, rim_send, rim_recv,
    box_send, box_recv, yo1_send, yo1_recv, zo1_send, zo1_recv, zo2_send, zo2_recv, yo2_send, yo2_recv,
):
    me = lax.axis_index("sp")
    tp = lax.axis_index("tp")
    core = lax.rem(tp, 2)
    y = tp // 2
    z = me // 2
    x = lax.rem(me, 2)
    zh = z // 2
    own = lax.rem(z, 2)
    pair = 1 - own
    zp = 2 * zh + pair
    far_mid = 2 - zh
    far_end = 3 - 3 * zh
    partner = y * 2 + 1 - core
    across = (1 - y) * 2 + core
    beside = (zp * 2 + x, tp)
    sibling = (z * 2 + 1 - x, tp)
    rows, cols = q_hbm.shape
    half = rows // 2
    piece = half // 2
    block, hidden = wv_hbm.shape
    wide = w3.shape[2]
    narrow = hidden - wide
    model = wout_hbm.shape[1]
    span = out_ref.shape[1]
    is_mid = (z == 1) | (z == 2)
    is_end = (z == 0) | (z == 3)
    is_wide = is_mid
    is_narrow = is_end
    roles = ((is_narrow, narrow, wide, 0, narrow), (is_wide, wide, narrow, narrow, 0))
    sides = (is_end, is_mid)

    def copy(src, dst, send, recv, where):
        return pltpu.make_async_remote_copy(
            src_ref=src, dst_ref=dst, send_sem=send, recv_sem=recv, device_id=where, device_id_type=MESH
        )

    def arrive(ref, recv):
        copy(ref, ref, core_send.at[0], recv, (me, partner)).wait_recv()

    def left(ref, send):
        copy(ref, ref, send, core_recv.at[0], (me, partner)).wait_send()

    def spot(s, zo, xo, width):
        return w3.at[s, pl.ds(pl.multiple_of((zo * 2 + xo) * block, block), block), pl.ds(0, width)]

    sources = (wv_hbm, wg_hbm, wd_hbm)

    def loads(s):
        for cond, width, rest, at, rest_at in roles:
            def pair_of():
                a = pltpu.make_async_copy(sources[s].at[:, pl.ds(at, width)], spot(s, z, x, width), loc_sem.at[s, 0])
                b = pltpu.make_async_copy(
                    sources[s].at[:, pl.ds(rest_at, rest)], other.at[s, :, pl.ds(0, rest)], loc_sem.at[s, 1]
                )
                return a, b
            yield cond, pair_of

    for s in range(3):
        for cond, pair_of in loads(s):
            @pl.when(cond)
            def _():
                for c in pair_of():
                    c.start()
    my_piece = core * half + y * piece
    res_load = pltpu.make_async_copy(res_hbm.at[pl.ds(pl.multiple_of(my_piece, piece), piece)], res, loc_sem.at[3, 0])
    res_load.start()
    late_loads = (
        pltpu.make_async_copy(q_hbm, q_ref, loc_sem.at[4, 0]),
        pltpu.make_async_copy(wout_hbm, wout_ref, loc_sem.at[4, 1]),
    )
    for c in late_loads:
        c.start()

    barrier = pltpu.get_barrier_semaphore()
    peers = [(lax.rem(me + j, n), tp) for j in range(1, n)] + [(me, lax.rem(tp + j, ntp)) for j in range(1, ntp)]
    for peer in peers:
        pl.semaphore_signal(barrier, inc=1, device_id=peer, device_id_type=MESH)

    def loaded(s):
        for cond, pair_of in loads(s):
            @pl.when(cond)
            def _():
                for c in pair_of():
                    c.wait()

    loaded(0)
    pl.semaphore_wait(barrier, len(peers))

    def begin_end(s):
        for cond, width, rest, _, _ in roles:
            @pl.when(is_end & cond)
            def _():
                b = other.at[s, :, pl.ds(0, rest)]
                copy(b, spot(s, z, x, rest), zs.at[s, 0], zr.at[s, 0], beside).start()

    def begin_far(s):
        for cond, width, rest, _, _ in roles:
            @pl.when(is_end & cond)
            def _():
                a = spot(s, z, x, width)
                copy(a, a, zs.at[s, 1], zr.at[s, 2], ((3 - z) * 2 + x, tp)).start()

            @pl.when(is_mid & cond)
            def _():
                b = other.at[s, :, pl.ds(0, rest)]
                copy(b, spot(s, z, x, rest), zs.at[s, 2], zr.at[s, 1], ((3 - zp) * 2 + x, tp)).start()

    def begin_mid(s):
        for cond, width, rest, _, _ in roles:
            @pl.when(is_mid & cond)
            def _():
                a = spot(s, z, x, width)
                copy(a, a, zs.at[s, 1], zr.at[s, 1], ((3 - z) * 2 + x, tp)).start()

    def begin_out(s):
        for cond, width, rest, _, _ in roles:
            @pl.when(is_mid & cond)
            def _():
                b = other.at[s, :, pl.ds(0, rest)]
                copy(b, spot(s, z, x, rest), zs.at[s, 0], zr.at[s, 0], beside).start()

    def begin_x(s, who=(0, 1)):
        for (cond, width, _, _, _), side in ((r, sides[w]) for r in roles for w in who):
            @pl.when(cond & side)
            def _():
                a = spot(s, z, x, width)
                copy(a, a, xs.at[s, 0], xr.at[s, 0], sibling).start()

    owners = (zp, far_mid, far_end)

    def event(s, j, who=(0, 1)):
        for side in who:
            for cond, width, _, _, _ in roles:
                @pl.when(sides[side] & cond)
                def _():
                    a = spot(s, owners[j], x, width)
                    arrive(a, zr.at[s, j])
                    if side == 1 and j == 0:
                        copy(a, a, zs.at[s, 3], zr.at[s, 2], ((3 - z) * 2 + x, tp)).start()
                    copy(a, a, xs.at[s, j + 1], xr.at[s, j + 1], sibling).start()

    def xwait(s, j):
        for cond, width, _, _, _ in roles:
            @pl.when(cond)
            def _():
                arrive(spot(s, ((z,) + owners)[j], 1 - x, width), xr.at[s, j])

    def finish_stream(s):
        for cond, width, rest, _, _ in roles:
            @pl.when(cond)
            def _():
                left(spot(s, z, x, rest), zs.at[s, 0])
                left(spot(s, z, x, width), zs.at[s, 1])
                for j in range(4):
                    left(spot(s, z, x, width), xs.at[s, j])

            @pl.when(is_mid & cond)
            def _():
                left(spot(s, z, x, rest), zs.at[s, 2])
                left(spot(s, z, x, width), zs.at[s, 3])

    right, before = lax.rem(me + 1, n), lax.rem(me + n - 1, n)
    ends = pl.ds(rows - WINDOW, WINDOW)
    starts = pl.ds(0, WINDOW)
    low, high = pl.ds(0, WINDOW), pl.ds(rows + WINDOW, WINDOW)
    halo = []
    for i, (src, dst) in enumerate(((k_ref, kx), (v_ref, vx))):
        halo.append(copy(src.at[ends], dst.at[low], halo_send.at[i, 0], halo_recv.at[i, 0], (right, tp)))
        halo.append(copy(src.at[starts], dst.at[high], halo_send.at[i, 1], halo_recv.at[i, 1], (before, tp)))
    halo.append(copy(lab_row_ref.at[:, ends], lx.at[:, low], halo_send.at[2, 0], halo_recv.at[2, 0], (right, tp)))
    halo.append(copy(lab_row_ref.at[:, starts], lx.at[:, high], halo_send.at[2, 1], halo_recv.at[2, 1], (before, tp)))
    for c in halo:
        c.start()
    begin_end(0)
    begin_mid(0)
    begin_out(0)
    begin_far(0)
    begin_x(0)
    loaded(1)
    begin_end(1)
    begin_x(1)
    loaded(2)
    begin_x(2, (0,))

    @pl.when(is_narrow)
    def _():
        if narrow < wide:
            w3[:, :, narrow:wide] = jnp.zeros((3, n * block, wide - narrow), BF16)

    inner = pl.ds(WINDOW, rows)
    kx[inner, :] = k_ref[...]
    vx[inner, :] = v_ref[...]
    lx[:, inner] = lab_row_ref[...]
    lab_copy = copy(lx, lp, lab_send, lab_recv, beside)
    chunks = rows // WINDOW

    def columns(row_ref, which):
        for i in which:
            chunk = slice(i * WINDOW, (i + 1) * WINDOW)
            square = jnp.broadcast_to(row_ref[0:1, chunk].astype(F32), (WINDOW, WINDOW))
            lc[chunk, :] = jnp.transpose(square)

    def neighbours(slot):
        for i in range(chunks):
            here = lc[WINDOW * (i + 1):WINDOW * (i + 2), :]
            for side, shift in ((0, -1), (1, 1)):
                there = lc[WINDOW * (i + 1) + shift:WINDOW * (i + 2) + shift, :]
                same[slot, side, i * WINDOW:(i + 1) * WINDOW, :] = jnp.where(here == there, 1.0, 0.0)

    columns(lx, range(1, chunks + 1))

    def edges():
        for c in halo:
            c.wait()
        lx[:, low] = jnp.where(me == 0, -1, lx[:, low])
        lx[:, high] = jnp.where(me == n - 1, -1, lx[:, high])
        lab_copy.start()
        columns(lx, (0, chunks + 1))
        neighbours(own)

    kv_local = k_ref.shape[1] // HEAD_DIM
    per_kv = cols // k_ref.shape[1]
    per_half = chunks // 2
    tile = 32

    def attend(i, carry):
        own_half = i // per_half
        j = lax.rem(i, per_half)
        flip = (1 - own_half) * core + own_half * (1 - y)
        turn = flip * (per_half - 1 - j) + (1 - flip) * j
        b = ((1 - own_half) * (1 - core) + own_half * core) * per_half + turn
        here = pl.ds(pl.multiple_of(b * WINDOW, WINDOW), WINDOW)
        wide_keys = pl.ds(pl.multiple_of(b * WINDOW, WINDOW), 3 * WINDOW)
        q = q_ref[here, :] * jnp.asarray(HEAD_DIM ** (-0.5), BF16)
        kw = kx[wide_keys, :]
        vw = vx[wide_keys, :]
        lab_k = lx[0:1, wide_keys].astype(F32)
        lab_q = lc[pl.ds(pl.multiple_of(b * WINDOW + WINDOW, WINDOW), WINDOW), 0:1]
        key = lax.broadcasted_iota(jnp.int32, (WINDOW, 3 * WINDOW), 1) - WINDOW
        query = lax.broadcasted_iota(jnp.int32, (WINDOW, 3 * WINDOW), 0)
        allowed = (jnp.abs(key - query) <= WINDOW) & (lab_q == lab_k)
        results = []
        for g in range(kv_local):
            k = kw[:, g * HEAD_DIM:(g + 1) * HEAD_DIM]
            v = vw[:, g * HEAD_DIM:(g + 1) * HEAD_DIM]
            heads = range(g * per_kv, (g + 1) * per_kv)
            stacked = jnp.concatenate([q[:, h * HEAD_DIM:(h + 1) * HEAD_DIM] for h in heads], axis=0)
            scores = lax.dot_general(stacked, k, (((1,), (1,)), ((), ())), preferred_element_type=F32)
            raws, scales = [], []
            for u, h in enumerate(heads):
                score = jnp.where(allowed, scores[u * WINDOW:(u + 1) * WINDOW], NEG)
                sink = sink_ref[h]
                highest = jnp.maximum(jnp.max(score, axis=1, keepdims=True), sink)
                raw = jnp.exp(score - highest)
                scales.append(1.0 / (jnp.sum(raw, axis=1, keepdims=True) + jnp.exp(sink - highest)))
                raws.append(raw.astype(BF16))
            summed = jnp.dot(jnp.concatenate(raws, axis=0), v, preferred_element_type=F32)
            for u in range(per_kv):
                results.append((summed[u * WINDOW:(u + 1) * WINDOW] * scales[u]).astype(BF16))
        attended = jnp.concatenate(results, axis=1)
        part[here, :] = jnp.dot(attended, wout_ref[...], preferred_element_type=F32).astype(BF16)
        mine = first.at[pl.ds(pl.multiple_of(turn * WINDOW, WINDOW), WINDOW)]

        @pl.when(own_half == 0)
        def _():
            copy(part.at[here], mine, core_send.at[turn], core_recv.at[turn], (me, partner)).start()

        @pl.when(own_half == 1)
        def _():
            arrive(mine, core_recv.at[turn])

            def add(t, carry):
                r = pl.ds(pl.multiple_of(turn * WINDOW + t * tile, tile), tile)
                o = pl.ds(pl.multiple_of(b * WINDOW + t * tile, tile), tile)
                first[r, :] = (part[o, :].astype(F32) + first[r, :].astype(F32)).astype(BF16)
                return carry

            lax.fori_loop(0, WINDOW // tile, add, 0)

        @pl.when(i == per_half)
        def _():
            y_copy(0, y).start()

        @pl.when(i == per_half + 1)
        def _():
            y_copy(1, y).start()

        @pl.when(i == 1)
        def _():
            edges()

        @pl.when(i == 3)
        def _():
            event(0, 0, (1,))
            begin_mid(1)
            begin_out(1)

        @pl.when(i == 4)
        def _():
            event(0, 1, (1,))

        return carry

    def y_copy(k, yy):
        if k == 0:
            count, src, dst = 2 * piece // 3, (1 - yy) * (half - 2 * piece // 3), (1 - yy) * (piece // 3)
        else:
            count, src, dst = piece // 3, 2 * piece // 3 + (1 - yy) * (piece // 3), yy * (2 * piece // 3)
        return copy(
            first.at[pl.ds(pl.multiple_of(src, 64), count)], second.at[pl.ds(pl.multiple_of(dst, 64), count)],
            y_send.at[k], y_recv.at[k], (me, across),
        )

    res_load.wait()
    for c in late_loads:
        c.wait()
    lax.fori_loop(0, 2 * per_half, attend, 0)
    for k in range(2):
        y_copy(k, 1 - y).wait_recv()

    def norm(slot, start, count):
        def body(i, carry):
            r = pl.ds(pl.multiple_of(start + i * tile, tile), tile)
            m = mixed[r, :].astype(F32)
            mean_sq = jnp.mean(m * m, axis=1, keepdims=True)
            normed[slot, r, :] = (m * lax.rsqrt(mean_sq + EPS) * gain_ref[...]).astype(BF16)
            return carry

        lax.fori_loop(0, count // tile, body, 0)

    def add_second(i, carry):
        r = pl.ds(pl.multiple_of(i * tile, tile), tile)
        f = pl.ds(pl.multiple_of(y * piece + i * tile, tile), tile)
        o = pl.ds(pl.multiple_of(my_piece + i * tile, tile), tile)
        s = first[f, :].astype(F32) + second[r, :].astype(F32)
        mixed[o, :] = (res[r, :].astype(F32) + s).astype(BF16)
        return carry

    lax.fori_loop(0, piece // tile, add_second, 0)

    def part_of(c, yy):
        return c * half + yy * piece

    def mixed_at(c, yy):
        return mixed.at[pl.ds(pl.multiple_of(part_of(c, yy), piece), piece)]

    bit = piece // 2

    def normed_at(slot, c, yy, b):
        return normed.at[slot, pl.ds(pl.multiple_of(part_of(c, yy) + b * bit, bit), bit)]

    def share(k, ref, where):
        copy(ref, ref, ag_send.at[k], ag_recv.at[k], where).start()

    share(0, mixed_at(core, y), (me, across))
    share(1, mixed_at(core, y), (me, partner))
    norm(own, my_piece, piece)
    for b in range(2):
        share(4 + b, normed_at(own, core, y, b), beside)
    event(0, 0, (0,))
    event(1, 0, (1,))
    event(0, 1, (0,))
    arrive(mixed_at(1 - core, y), ag_recv.at[1])
    norm(own, part_of(1 - core, y), piece)
    event(0, 2, (1,))
    arrive(mixed_at(core, 1 - y), ag_recv.at[0])
    share(2, mixed_at(core, 1 - y), (me, partner))
    norm(own, part_of(core, 1 - y), piece)
    event(0, 2, (0,))
    begin_far(1)

    def serve_spread(b):
        arrive(normed_at(pair, core, y, b), ag_recv.at[4 + b])
        share(6 + b, normed_at(pair, core, y, b), (me, across))
        share(8 + b, normed_at(pair, core, y, b), (me, partner))

    serve_spread(0)
    serve_spread(1)
    event(1, 1, (1,))
    event(1, 0, (0,))
    begin_end(2)
    arrive(mixed_at(1 - core, 1 - y), ag_recv.at[2])
    norm(own, part_of(1 - core, 1 - y), piece)

    big = rows // 3

    def project(which, slot):
        def body(t, carry):
            r = pl.ds(pl.multiple_of(t * big, big), big)
            product = jnp.dot(normed[slot, r, :], w3[which], preferred_element_type=F32).astype(BF16)
            if which == 0:
                value[slot, pl.ds(pl.multiple_of(RIM + t * big, RIM), big), :] = product
            else:
                gate[slot, r, :] = product
            return carry

        lax.fori_loop(0, 3, body, 0)

    inside = pl.ds(RIM, RIM)
    last = pl.ds(rows, RIM)
    fronts, backs = pl.ds(0, RIM), pl.ds(RIM + rows, RIM)
    facing = ((3 - z) * 2 + 1 - x, tp)
    near_rims = (
        (x == 0, ((0, last, 0, 0), (1, inside, 0, 1), (1, last, 1, 0))),
        (x == 1, ((0, inside, 0, 1), (0, last, 1, 0), (1, inside, 1, 1))),
    )
    far_rims = (((x == 0) & (zh == 1), (0, inside, 1, 1)), ((x == 1) & (zh == 0), (1, last, 0, 0)))

    def rim_copy(frm, source, to, side, where):
        target = value.at[to, (fronts, backs)[side]]
        pad = 2 * to + side
        copy(value.at[frm, source], target, rim_send.at[pad], rim_recv.at[pad], where).start()

    def send_far_rims(side):
        for cond, spec in far_rims:
            @pl.when(cond & side)
            def _():
                rim_copy(*spec, facing)

    def serve_x(s):
        for j in range(4):
            xwait(s, j)

    serve_x(0)
    project(0, own)
    send_far_rims(is_mid)
    begin_mid(2)
    event(1, 1, (0,))
    event(1, 2)

    def serve_diagonal(b):
        arrive(normed_at(pair, core, 1 - y, b), ag_recv.at[6 + b])
        share(10 + b, normed_at(pair, core, 1 - y, b), (me, partner))

    def serve_rest(b):
        arrive(normed_at(pair, 1 - core, y, b), ag_recv.at[8 + b])
        arrive(normed_at(pair, 1 - core, 1 - y, b), ag_recv.at[10 + b])

    serve_diagonal(0)
    serve_diagonal(1)
    serve_rest(0)
    serve_rest(1)
    project(0, pair)

    send_far_rims(is_end)
    for cond, specs in near_rims:
        @pl.when(cond)
        def _():
            for spec in specs:
                rim_copy(*spec, sibling)

    begin_out(2)
    begin_far(2)
    begin_x(2, (1,))
    event(2, 0, (1,))
    serve_x(1)
    project(1, own)
    project(1, pair)
    event(2, 0, (0,))
    lab_copy.wait()
    columns(lp, range(chunks + 2))
    neighbours(pair)

    def serve_rims(slot):
        for side, rd in enumerate((fronts, backs)):
            if slot == side:
                @pl.when((x != side) | (zh != side))
                def _():
                    arrive(value.at[slot, rd], rim_recv.at[2 * slot + side])

                @pl.when((x == side) & (zh == side))
                def _():
                    value[slot, rd, :] = jnp.zeros((RIM, wide), BF16)
            else:
                arrive(value.at[slot, rd], rim_recv.at[2 * slot + side])

    serve_rims(0)
    serve_rims(1)

    taps_all = taps_ref[...].astype(F32)
    taps = jnp.where(is_wide, taps_all[:, narrow:], taps_all[:, :wide])
    step = 64
    lanes = wide // WINDOW

    for slot in range(2):
        def gated(i, carry):
            base = i * step
            r = pl.ds(pl.multiple_of(base, step), step)
            x_rows = value[slot, pl.ds(pl.multiple_of(RIM + base, RIM), step), :].astype(F32)
            above = value[slot, pl.ds(pl.multiple_of(base, RIM), RIM), :].astype(F32)[RIM - 1:RIM]
            below = value[slot, pl.ds(pl.multiple_of(RIM + base + step, RIM), RIM), :].astype(F32)[0:1]
            prev = jnp.concatenate([above, x_rows[:-1]], axis=0)
            nxt = jnp.concatenate([x_rows[1:], below], axis=0)
            with_prev = jnp.concatenate([same[slot, 0, r, :]] * lanes, axis=1) > 0.5
            with_next = jnp.concatenate([same[slot, 1, r, :]] * lanes, axis=1) > 0.5
            conv = (
                taps[0:1] * jnp.where(with_prev, prev, 0.0)
                + taps[1:2] * x_rows
                + taps[2:3] * jnp.where(with_next, nxt, 0.0)
            )
            gate[slot, r, :] = (conv * jax.nn.sigmoid(conv) * gate[slot, r, :].astype(F32)).astype(BF16)
            return carry

        lax.fori_loop(0, rows // step, gated, 0)

    order = (z, zp, far_mid, far_end)
    quarter = rows // 2

    def lower(u):
        t = order[u]
        w = w3[2, pl.ds(pl.multiple_of(t * span, span), span), :]
        for slot in range(2):
            def body(i, carry):
                r = pl.ds(pl.multiple_of(i * quarter, quarter), quarter)
                pd[u, slot, r, :] = lax.dot_general(
                    gate[slot, r, :], w, (((1,), (1,)), ((), ())), preferred_element_type=F32
                ).astype(BF16)
                return carry

            lax.fori_loop(0, 2, body, 0)

        @pl.when(core != lax.rem(t, 2))
        def _():
            copy(pd.at[u], box.at[u // 2], box_send.at[u], box_recv.at[u // 2], (me, partner)).start()

    cuts = (quarter, quarter, rows // 6, rows // 6)

    def segment(u, g):
        count = (rows - cuts[u]) // 2
        return cuts[u] + g * count, count

    def accumulate(ref, slot, at, count, other_ref, base):
        def body(i, carry):
            r = pl.ds(pl.multiple_of(at + i * tile, tile), tile)
            o = pl.ds(pl.multiple_of(base + i * tile, tile), tile)
            ref[slot, r, :] = (ref[slot, r, :].astype(F32) + other_ref[o, :].astype(F32)).astype(BF16)
            return carry

        lax.fori_loop(0, count // tile, body, 0)

    def z_first(u, g):
        at, count = segment(u, g)
        return copy(
            pd.at[u, pair, pl.ds(at, count)], zin1.at[u // 2, g, pl.ds(0, count)],
            zo1_send.at[u // 2, g], zo1_recv.at[u // 2, g], beside,
        )

    def then_y(u, g):
        at, count = segment(u, g)
        return copy(
            pd.at[u, own, pl.ds(at, count)], yin2.at[g, pl.ds(0, count)], yo2_send.at[g], yo2_recv.at[g], (me, across)
        )

    def y_first(u, slot, k):
        top = pl.ds(0, cuts[u])
        return copy(pd.at[u, slot, top], yin1.at[slot, top], yo1_send.at[k], yo1_recv.at[k], (me, across))

    def then_z(u):
        top = pl.ds(0, cuts[u])
        return copy(pd.at[u, pair, top], zin2.at[top], zo2_send, zo2_recv, beside)

    def stage_one(u):
        t = order[u]

        @pl.when(core == lax.rem(t, 2))
        def _():
            arrive(box.at[u // 2], box_recv.at[u // 2])

            def add(slot, at, count):
                accumulate(pd.at[u], slot, at, count, box.at[u // 2, slot], at)

            def tops():
                add(pair, 0, cuts[u])

                @pl.when(y != t // 2)
                def _():
                    y_first(u, pair, 0).start()

                add(own, 0, cuts[u])

                @pl.when(y != t // 2)
                def _():
                    y_first(u, own, 1).start()

            def rest():
                for g in range(2):
                    add(pair, *segment(u, g))
                    z_first(u, g).start()

            if u < 2:
                tops()
                rest()
            else:
                rest()
                tops()
            for g in range(2):
                add(own, *segment(u, g))

    def stage_y(u):
        t = order[u]

        @pl.when(tp == t)
        def _():
            top = pl.ds(0, cuts[u])
            arrive(yin1.at[pair, top], yo1_recv.at[0])
            accumulate(pd.at[u], pair, 0, cuts[u], yin1.at[pair], 0)
            then_z(u).start()
            arrive(yin1.at[own, top], yo1_recv.at[1])
            accumulate(pd.at[u], own, 0, cuts[u], yin1.at[own], 0)

    def stage_z(u):
        t = order[u]

        @pl.when(core == lax.rem(t, 2))
        def _():
            for g in range(2):
                at, count = segment(u, g)
                arrive(zin1.at[u // 2, g, pl.ds(0, count)], zo1_recv.at[u // 2, g])
                accumulate(pd.at[u], own, at, count, zin1.at[u // 2, g], 0)

                @pl.when(y != t // 2)
                def _():
                    then_y(u, g).start()

    def stage_three(u):
        t = order[u]

        @pl.when(tp == t)
        def _():
            def close(at, count, extra):
                def body(i, carry):
                    r = pl.ds(pl.multiple_of(i * tile, tile), tile)
                    o = pl.ds(pl.multiple_of(at + i * tile, tile), tile)
                    kept = mixed[o, pl.ds(pl.multiple_of(t * span, span), span)].astype(F32)
                    s = pd[u, own, o, :].astype(F32) + extra[r, :].astype(F32)
                    out_ref[o, :] = (kept + s).astype(BF16)
                    return carry

                lax.fori_loop(0, count // tile, body, 0)

            arrive(zin2.at[pl.ds(0, cuts[u])], zo2_recv)
            close(0, cuts[u], zin2)
            for g in range(2):
                at, count = segment(u, g)
                arrive(yin2.at[g, pl.ds(0, count)], yo2_recv.at[g])
                close(at, count, yin2.at[g])

    def drain(u):
        t = order[u]

        @pl.when(core != lax.rem(t, 2))
        def _():
            left(pd.at[u], box_send.at[u])

        @pl.when(core == lax.rem(t, 2))
        def _():
            for g in range(2):
                z_first(u, g).wait_send()

            @pl.when(y != t // 2)
            def _():
                for k, slot in enumerate((pair, own)):
                    y_first(u, slot, k).wait_send()
                for g in range(2):
                    then_y(u, g).wait_send()

            @pl.when(y == t // 2)
            def _():
                then_z(u).wait_send()

    xwait(2, 0)
    lower(0)
    event(2, 1)
    xwait(2, 1)
    lower(1)
    stage_one(0)
    stage_one(1)
    event(2, 2)
    xwait(2, 2)
    lower(2)
    stage_one(2)
    xwait(2, 3)
    lower(3)
    stage_one(3)
    stage_z(0)
    stage_z(1)
    stage_y(0)
    stage_y(1)
    stage_z(2)
    stage_z(3)
    stage_y(2)
    stage_y(3)
    stage_three(0)
    stage_three(1)
    stage_three(2)
    stage_three(3)

    for s in range(3):
        finish_stream(s)
    for j in range(per_half):
        left(first.at[pl.ds(0, WINDOW)], core_send.at[j])
    for k in range(2):
        y_copy(k, y).wait_send()
    for k in range(3):
        left(mixed_at(core, y), ag_send.at[k])
    for k in range(4, 12):
        left(normed_at(own, core, y, 0), ag_send.at[k])
    for pad in range(4):
        sends = (x == pad // 3) | (zh == pad // 3) if pad in (0, 3) else x >= 0

        @pl.when(sends)
        def _():
            left(value.at[0, fronts], rim_send.at[pad])
    for u in range(4):
        drain(u)


def solution(mesh):
    n, ntp = mesh.shape["sp"], mesh.shape["tp"]

    def by_ring(q, k, v, sink, doc, res, wout, gain, wv, wg, taps, wd):
        rows, model = res.shape
        hidden = wv.shape[1]
        block = wv.shape[0]
        ny = ntp // 2
        labels = doc + 1
        lab_row = labels[None, :]
        vm = pl.BlockSpec(memory_space=pltpu.VMEM)
        hbm = pl.BlockSpec(memory_space=pl.ANY)
        smem = pl.BlockSpec(memory_space=pltpu.SMEM)
        dma = pltpu.SemaphoreType.DMA
        kvc = k.shape[1]
        span = model // ntp
        scratch = [
            pltpu.VMEM((2, n * block, hidden), BF16),
            pltpu.VMEM((n * block, hidden), BF16),
            pltpu.VMEM((rows + 2 * WINDOW, kvc), BF16),
            pltpu.VMEM((rows + 2 * WINDOW, kvc), BF16),
            pltpu.VMEM((1, rows + 2 * WINDOW), jnp.int32),
            pltpu.VMEM((rows + 2 * WINDOW, WINDOW), F32),
            pltpu.VMEM((rows, model), BF16),
            pltpu.VMEM((rows // 2, model), BF16),
            pltpu.VMEM((max(ny - 1, 1), rows // 2 // ny, model), BF16),
            pltpu.VMEM((rows, model), BF16),
            pltpu.VMEM((rows, model), BF16),
            pltpu.VMEM((rows, hidden), BF16),
            pltpu.VMEM((rows, hidden), BF16),
            pltpu.VMEM((2, RIM, hidden), BF16),
            pltpu.VMEM((n, 2, rows, block // 2), BF16),
            pltpu.VMEM((n, 2, rows // 2, block // 2), BF16),
            pltpu.VMEM((n // ntp, ntp - 1, 2, rows // 2, block // 2), BF16),
            pltpu.VMEM((rows // 2 // ny, model), BF16),
            dma((4,)),
            dma((4, 2, n - 1)), dma((4, 2, n - 1)),
            dma((3, 2)), dma((3, 2)),
            dma((2,)), dma((2,)),
            dma, dma,
            dma((ny,)), dma((ny,)),
            dma((ny,)), dma((ny,)),
            dma, dma,
            dma((n + 2,)), dma((n + 2,)),
            dma((n + 2,)), dma((n // ntp, ntp - 1)),
        ]
        return pl.pallas_call(
            functools.partial(ring_kernel, n, ntp),
            out_shape=jax.ShapeDtypeStruct((rows, span), BF16),
            in_specs=[vm, vm, vm, smem, vm, hbm, vm, vm, hbm, hbm, vm, hbm],
            out_specs=vm,
            scratch_shapes=scratch,
            compiler_params=pltpu.CompilerParams(
                collective_id=0, has_side_effects=True, vmem_limit_bytes=67043328
            ),
            name="layer",
        )(q, k, v, sink, lab_row, res, wout, gain[None, :], wv, wg, taps, wd)


    def by_pairs(q, k, v, sink, doc, res, wout, gain, wv, wg, taps, wd):
        rows, model = res.shape
        block, hidden = wv.shape
        half = rows // 2
        piece = half // 2
        span = model // ntp
        kvc = k.shape[1]
        third = rows // 12 * 5
        wide = (hidden // LANES + 1) // 2 * LANES
        lab_row = doc[None, :]
        vm = pl.BlockSpec(memory_space=pltpu.VMEM)
        hbm = pl.BlockSpec(memory_space=pl.ANY)
        smem = pl.BlockSpec(memory_space=pltpu.SMEM)
        dma = pltpu.SemaphoreType.DMA
        scratch = [
            pltpu.VMEM((3, n * block, wide), BF16),
            pltpu.VMEM((3, block, wide), BF16),
            pltpu.VMEM((rows + 2 * WINDOW, kvc), BF16),
            pltpu.VMEM((rows + 2 * WINDOW, kvc), BF16),
            pltpu.VMEM((1, rows + 2 * WINDOW), jnp.int32),
            pltpu.VMEM((1, rows + 2 * WINDOW), jnp.int32),
            pltpu.VMEM((rows + 2 * WINDOW, WINDOW), F32),
            pltpu.VMEM((2, 2, rows, WINDOW), F32),
            pltpu.VMEM((rows, model), BF16),
            pltpu.VMEM((half, model), BF16),
            pltpu.VMEM((piece, model), BF16),
            pltpu.VMEM((rows, model), BF16),
            pltpu.VMEM((2, rows, model), BF16),
            pltpu.VMEM((2, rows + 2 * RIM, wide), BF16),
            pltpu.VMEM((2, rows, wide), BF16),
            pltpu.VMEM((4, 2, rows, span), BF16),
            pltpu.VMEM((2, 2, rows, span), BF16),
            pltpu.VMEM((2, half, span), BF16),
            pltpu.VMEM((2, 2, third, span), BF16),
            pltpu.VMEM((half, span), BF16),
            pltpu.VMEM((2, third, span), BF16),
            pltpu.VMEM((piece, model), BF16),
            pltpu.VMEM(q.shape, BF16),
            pltpu.VMEM(wout.shape, BF16),
            dma((5, 2)),
            dma((3, 2)), dma((3, 2)),
            dma, dma,
            dma((3, 4)), dma((3, 3)),
            dma((3, 4)), dma((3, 4)),
            dma((rows // WINDOW // 2,)), dma((rows // WINDOW // 2,)),
            dma((2,)), dma((2,)),
            dma((12,)), dma((12,)),
            dma((4,)), dma((4,)),
            dma((4,)), dma((2,)),
            dma((2,)), dma((2,)),
            dma((2, 2)), dma((2, 2)),
            dma, dma,
            dma((2,)), dma((2,)),
        ]
        return pl.pallas_call(
            functools.partial(paired_kernel, n, ntp),
            out_shape=jax.ShapeDtypeStruct((rows, span), BF16),
            in_specs=[hbm, vm, vm, smem, vm, hbm, hbm, vm, hbm, hbm, vm, hbm],
            out_specs=vm,
            scratch_shapes=scratch,
            compiler_params=pltpu.CompilerParams(
                collective_id=0, has_side_effects=True, vmem_limit_bytes=67043328
            ),
            name="layer",
        )(q, k, v, sink, lab_row, res, wout, gain[None, :], wv, wg, taps, wd)

    placed = (
        P("sp", "tp"), P("sp", "tp"), P("sp", "tp"), P("tp"), P("sp"), P("sp", None),
        P("tp", None), P(), P("sp", "tp"), P("sp", "tp"), P(None, "tp"), P("sp", "tp"),
    )
    return jax.shard_map(
        by_pairs if (n, ntp) == (8, 4) else by_ring, mesh=mesh, in_specs=placed, out_specs=P("sp", "tp"), check_vma=False
    )
```

```python
import functools

import jax
import jax.numpy as jnp
from jax import lax
from jax.experimental import pallas as pl
from jax.experimental.pallas import tpu as pltpu
from jax.sharding import PartitionSpec as P

HEAD_DIM = 64
WINDOW = 128
EPS = 1e-06
NEG = -1e30
RIM = 16
LANES = 128
MESH = pl.DeviceIdType.MESH
F32 = jnp.float32
BF16 = jnp.bfloat16


def ring_kernel(
    n, ntp,
    q_ref, k_ref, v_ref, sink_ref, lab_row_ref,
    res_hbm, wout_ref, gain_ref, wv_hbm, wg_hbm, taps_ref, wd_hbm,
    out_ref,
    up, down, kx, vx, lx, lc, part, first, second, mixed, normed, value, gate, rim, pd, box, inbox, res,
    loc_sem, ring_send, ring_recv, halo_send, halo_recv, rim_send, rim_recv,
    core_send, core_recv, y_send, y_recv, back_send, back_recv, pair_send, pair_recv,
    down_send, down_recv, out_send, out_recv,
):
    me = lax.axis_index("sp")
    tp = lax.axis_index("tp")
    core = lax.rem(tp, 2)
    y = tp // 2
    ny = ntp // 2
    partner = y * 2 + 1 - core
    rows = q_ref.shape[0]
    half = rows // 2
    piece = half // ny
    block = wv_hbm.shape[0]
    depth = block // 2
    quarter = block // 4

    def place(p):
        h = p // (n // 2)
        return (1 - h) * (2 * p) + h * (2 * n - 1 - 2 * p)

    odd = lax.rem(me, 2)
    pos = (1 - odd) * (me // 2) + odd * ((2 * n - 1 - me) // 2)
    ahead = place(lax.rem(pos + 1, n))
    behind = place(lax.rem(pos + n - 1, n))
    right = lax.rem(me + 1, n)
    left = lax.rem(me + n - 1, n)

    loads = []
    for i, (src, dst) in enumerate((
        (wv_hbm, up.at[0, pl.ds(me * block, block)]),
        (wg_hbm, up.at[1, pl.ds(me * block, block)]),
        (wd_hbm, down.at[pl.ds(me * block, block)]),
        (res_hbm.at[pl.ds(core * half + y * piece, piece)], res),
    )):
        c = pltpu.make_async_copy(src, dst, loc_sem.at[i])
        c.start()
        loads.append(c)

    barrier = pltpu.get_barrier_semaphore()
    peers = [(ahead, tp), (behind, tp), (right, tp), (left, tp)]
    for j in range(1, ntp):
        peers.append((me, lax.rem(tp + j, ntp)))
    for peer in peers:
        pl.semaphore_signal(barrier, inc=1, device_id=peer, device_id_type=MESH)
    for c in loads:
        c.wait()
    pl.semaphore_wait(barrier, len(peers))

    def spot(stream, way, owner):
        if stream < 2:
            return up.at[stream, pl.ds(owner * block + way * depth, depth)]
        return down.at[pl.ds(owner * block + way * depth + (stream - 2) * quarter, quarter)]

    def ring(stream, way, s, arriving):
        shift = s + 1 if arriving else s
        owner = place(lax.rem(pos + n - shift, n)) if way == 0 else place(lax.rem(pos + shift, n))
        ref = spot(stream, way, owner)
        return pltpu.make_async_remote_copy(
            src_ref=ref, dst_ref=ref,
            send_sem=ring_send.at[stream, way, s], recv_sem=ring_recv.at[stream, way, s],
            device_id=(ahead if way == 0 else behind, tp), device_id_type=MESH,
        )

    def begin(stream):
        for way in range(2):
            ring(stream, way, 0, False).start()

    def forward(stream, s, last=False):
        for way in range(2):
            ring(stream, way, s, True).wait_recv()
            if not last:
                ring(stream, way, s + 1, False).start()

    queue = []
    for s in range(n - 1):
        for stream in (0, 1):
            queue.append((stream, s))
    for s in range(n - 1):
        for stream in (2, 3):
            queue.append((stream, s))
    done = [0]

    def serve(count):
        for _ in range(count):
            if done[0] == len(queue):
                return
            stream, s = queue[done[0]]
            done[0] += 1
            forward(stream, s, last=s == n - 2)
            if stream < 2 and s == n - 2:
                begin(stream + 2)

    halo = []

    def remote(src, dst, send, recv, where):
        c = pltpu.make_async_remote_copy(
            src_ref=src, dst_ref=dst, send_sem=send, recv_sem=recv, device_id=where, device_id_type=MESH
        )
        c.start()
        return c

    ends = pl.ds(rows - WINDOW, WINDOW)
    starts = pl.ds(0, WINDOW)
    low, high = pl.ds(0, WINDOW), pl.ds(rows + WINDOW, WINDOW)
    for i, (src, dst) in enumerate(((k_ref, kx), (v_ref, vx))):
        halo.append(remote(src.at[ends], dst.at[low], halo_send.at[i, 0], halo_recv.at[i, 0], (right, tp)))
        halo.append(remote(src.at[starts], dst.at[high], halo_send.at[i, 1], halo_recv.at[i, 1], (left, tp)))
    halo.append(remote(lab_row_ref.at[:, ends], lx.at[:, low], halo_send.at[2, 0], halo_recv.at[2, 0], (right, tp)))
    halo.append(remote(lab_row_ref.at[:, starts], lx.at[:, high], halo_send.at[2, 1], halo_recv.at[2, 1], (left, tp)))
    begin(0)
    begin(1)
    inner = pl.ds(WINDOW, rows)
    kx[inner, :] = k_ref[...]
    vx[inner, :] = v_ref[...]
    lx[:, inner] = lab_row_ref[...]
    for c in halo:
        c.wait()
    lx[:, low] = jnp.where(me == 0, -1, lx[:, low])
    lx[:, high] = jnp.where(me == n - 1, -1, lx[:, high])
    for i in range(rows // WINDOW + 2):
        chunk = slice(i * WINDOW, (i + 1) * WINDOW)
        square = jnp.broadcast_to(lx[0:1, chunk].astype(F32), (WINDOW, WINDOW))
        lc[chunk, :] = jnp.transpose(square)

    kv_local = k_ref.shape[1] // HEAD_DIM
    per_kv = q_ref.shape[1] // k_ref.shape[1]
    blocks = rows // WINDOW
    model = wout_ref.shape[1]

    def attend(b, carry):
        here = pl.ds(pl.multiple_of(b * WINDOW, WINDOW), WINDOW)
        wide = pl.ds(pl.multiple_of(b * WINDOW, WINDOW), 3 * WINDOW)
        q = q_ref[here, :]
        kw = kx[wide, :]
        vw = vx[wide, :]
        lab_k = lx[0:1, wide].astype(F32)
        lab_q = lc[pl.ds(pl.multiple_of(b * WINDOW + WINDOW, WINDOW), WINDOW), 0:1]
        key = lax.broadcasted_iota(jnp.int32, (WINDOW, 3 * WINDOW), 1) - WINDOW
        query = lax.broadcasted_iota(jnp.int32, (WINDOW, 3 * WINDOW), 0)
        allowed = (jnp.abs(key - query) <= WINDOW) & (lab_q == lab_k)
        results = []
        for g in range(kv_local):
            k = kw[:, g * HEAD_DIM:(g + 1) * HEAD_DIM]
            v = vw[:, g * HEAD_DIM:(g + 1) * HEAD_DIM]
            for j in range(per_kv):
                h = g * per_kv + j
                qh = q[:, h * HEAD_DIM:(h + 1) * HEAD_DIM]
                score = lax.dot_general(
                    qh, k, (((1,), (1,)), ((), ())), preferred_element_type=F32
                ) * HEAD_DIM ** (-0.5)
                score = jnp.where(allowed, score, NEG)
                sink = sink_ref[h]
                highest = jnp.maximum(jnp.max(score, axis=1, keepdims=True), sink)
                raw = jnp.where(allowed, jnp.exp(score - highest), 0.0)
                total = jnp.sum(raw, axis=1, keepdims=True) + jnp.exp(sink - highest)
                probs = (raw / total).astype(BF16)
                results.append(jnp.dot(probs, v, preferred_element_type=F32).astype(BF16))
        attended = jnp.concatenate(results, axis=1)
        part[here, :] = jnp.dot(attended, wout_ref[...], preferred_element_type=F32).astype(BF16)
        return carry

    split = blocks // 3
    for t in range(3):
        lax.fori_loop(t * split, (t + 1) * split if t < 2 else blocks, attend, 0)
        serve(2 if t == 1 else 1)

    tile = 32
    other_half = pl.ds((1 - core) * half, half)
    swap = remote(part.at[other_half], first, core_send, core_recv, (me, partner))
    swap.wait()

    def add_first(i, carry):
        r = pl.ds(pl.multiple_of(i * tile, tile), tile)
        o = pl.ds(pl.multiple_of(core * half + i * tile, tile), tile)
        first[r, :] = (part[o, :].astype(F32) + first[r, :].astype(F32)).astype(BF16)
        return carry

    lax.fori_loop(0, half // tile, add_first, 0)
    copies = []
    for j in range(1, ny):
        to = lax.rem(y + j, ny)
        copies.append(remote(
            first.at[pl.ds(to * piece, piece)], second.at[j - 1], y_send.at[j - 1], y_recv.at[j - 1], (me, to * 2 + core)
        ))
    serve(2)
    for c in copies:
        c.wait()

    def add_second(i, carry):
        r = pl.ds(pl.multiple_of(i * tile, tile), tile)
        s = first[pl.ds(pl.multiple_of(y * piece + i * tile, tile), tile), :].astype(F32)
        for j in range(ny - 1):
            s = s + second[j, r, :].astype(F32)
        o = pl.ds(pl.multiple_of(core * half + y * piece + i * tile, tile), tile)
        mixed[o, :] = (res[r, :].astype(F32) + s).astype(BF16)
        return carry

    lax.fori_loop(0, piece // tile, add_second, 0)
    mine = mixed.at[pl.ds(core * half + y * piece, piece)]
    copies = []
    for j in range(1, ny):
        to = lax.rem(y + j, ny)
        copies.append(remote(mine, mine, back_send.at[j - 1], back_recv.at[j - 1], (me, to * 2 + core)))
    serve(2)
    for j, c in enumerate(copies):
        c.wait_send()
        frm = lax.rem(y + ny - (j + 1), ny)
        theirs = mixed.at[pl.ds(core * half + frm * piece, piece)]
        pltpu.make_async_remote_copy(
            src_ref=theirs, dst_ref=theirs, send_sem=back_send.at[j], recv_sem=back_recv.at[j],
            device_id=(me, partner), device_id_type=MESH,
        ).wait_recv()
    own_half = mixed.at[pl.ds(core * half, half)]
    swap = remote(own_half, own_half, pair_send, pair_recv, (me, partner))
    swap.wait_send()
    their_half = mixed.at[other_half]
    pltpu.make_async_remote_copy(
        src_ref=their_half, dst_ref=their_half, send_sem=pair_send, recv_sem=pair_recv,
        device_id=(me, partner), device_id_type=MESH,
    ).wait_recv()

    def normalise(i, carry):
        r = pl.ds(pl.multiple_of(i * tile, tile), tile)
        m = mixed[r, :].astype(F32)
        mean_sq = jnp.mean(m * m, axis=1, keepdims=True)
        normed[r, :] = (m * lax.rsqrt(mean_sq + EPS) * gain_ref[...]).astype(BF16)
        return carry

    lax.fori_loop(0, rows // tile, normalise, 0)

    serve(2 * (n - 1) - done[0])
    big = rows // 3

    def project(t, which, dst):
        r = slice(t * big, (t + 1) * big)
        dst[r, :] = jnp.dot(normed[r, :], up[which], preferred_element_type=F32).astype(BF16)

    for t in range(3):
        project(t, 0, value)
        serve(1)
    tail = remote(value.at[pl.ds(rows - RIM, RIM)], rim.at[0], rim_send.at[0], rim_recv.at[0], (right, tp))
    head = remote(value.at[pl.ds(0, RIM)], rim.at[1], rim_send.at[1], rim_recv.at[1], (left, tp))
    for t in range(3):
        project(t, 1, gate)
        serve(1)
    tail.wait()
    head.wait()

    taps = taps_ref[...].astype(F32)
    step = 64
    before = rim[0, RIM - 1:RIM, :].astype(F32)

    def label(i, shift):
        return lc[WINDOW + i * step + shift:WINDOW + (i + 1) * step + shift, 0:1]

    for i in range(rows // step):
        r = slice(i * step, (i + 1) * step)
        x = value[r, :].astype(F32)
        after = (value[(i + 1) * step:(i + 1) * step + RIM, :] if (i + 1) * step < rows else rim[1, :, :])[0:1].astype(F32)
        prev = jnp.concatenate([before, x[:-1]], axis=0)
        nxt = jnp.concatenate([x[1:], after], axis=0)
        conv = (
            taps[0:1] * jnp.where(label(i, -1) == label(i, 0), prev, 0.0)
            + taps[1:2] * x
            + taps[2:3] * jnp.where(label(i, 1) == label(i, 0), nxt, 0.0)
        )
        gate[r, :] = (conv * jax.nn.sigmoid(conv) * gate[r, :].astype(F32)).astype(BF16)
        before = x[step - 1:step]
        if i % 3 == 2:
            serve(1)

    per_tp = n // ntp
    mine_rows = pl.ds(core * half, half)
    partner_rows = pl.ds((1 - core) * half, half)
    units = []
    for d in range(n):
        if d in (1, n - 1) and n > 2:
            units.append((2 * (n - 1) + 2 * (n - d), d, 0, 1))
            units.append((2 * (n - 1) + 2 * d, d, 1, 1))
        else:
            units.append((2 * (n - 1) + (2 * max(d, n - d) if d else 0), d, 0, 2))
    units.sort()

    def target(owner):
        to = owner // per_tp
        local = lax.rem(owner, per_tp)
        slot = lax.rem(tp - to + ntp, ntp) - 1
        return to, local, slot

    def lower(u):
        _, d, way, count = units[u]
        owner = place(lax.rem(pos + d, n))
        w = down[pl.ds(pl.multiple_of(owner * block + way * depth, depth), count * depth), :]

        def body(i, carry):
            r = pl.ds(pl.multiple_of(i * big, big), big)
            product = lax.dot_general(
                gate[r, :], w, (((1,), (1,)), ((), ())), preferred_element_type=F32
            ).astype(BF16)
            for j in range(count):
                pd[owner, way + j, r, :] = product[:, j * depth:(j + 1) * depth]
            return carry

        lax.fori_loop(0, 3, body, 0)
        return remote(
            pd.at[owner, pl.ds(way, count), partner_rows], box.at[owner, pl.ds(way, count)],
            down_send.at[u], down_recv.at[u], (me, partner),
        )

    def reduce(u, c):
        _, d, way, count = units[u]
        owner = place(lax.rem(pos + d, n))
        c.wait()

        def merge(i, carry):
            r = pl.ds(pl.multiple_of(i * tile, tile), tile)
            o = pl.ds(pl.multiple_of(core * half + i * tile, tile), tile)
            for j in range(way, way + count):
                pd[owner, j, o, :] = (pd[owner, j, o, :].astype(F32) + box[owner, j, r, :].astype(F32)).astype(BF16)
            return carry

        lax.fori_loop(0, half // tile, merge, 0, unroll=2)
        to, local, slot = target(owner)

        @pl.when(to != tp)
        def _():
            remote(
                pd.at[owner, pl.ds(way, count), mine_rows], inbox.at[local, slot, pl.ds(way, count)],
                out_send.at[u], out_recv.at[local, slot], (me, to),
            )

    waiting = None
    for u in range(len(units)):
        serve(units[u][0] - done[0])
        c = lower(u)
        if waiting is not None:
            reduce(*waiting)
        waiting = (u, c)
    reduce(*waiting)
    serve(len(queue))

    span = per_tp * block
    for local in range(per_tp):
        owner = tp * per_tp + local
        for slot in range(ntp - 1):
            ref = inbox.at[local, slot]
            pltpu.make_async_remote_copy(
                src_ref=ref, dst_ref=ref, send_sem=out_send.at[0], recv_sem=out_recv.at[local, slot],
                device_id=(me, partner), device_id_type=MESH,
            ).wait_recv()
        for same in range(2):
            base = (core if same else 1 - core) * half
            slots = range(1, ntp - 1, 2) if same else range(0, ntp - 1, 2)

            def finish(i, carry):
                r = pl.ds(pl.multiple_of(i * tile, tile), tile)
                o = pl.ds(pl.multiple_of(base + i * tile, tile), tile)
                kept = mixed[o, pl.ds(pl.multiple_of(tp * span, span), span)]
                for j in range(2):
                    s = sum(inbox[local, slot, j, r, :].astype(F32) for slot in slots)
                    if same:
                        s = s + pd[owner, j, o, :].astype(F32)
                    cols = slice(local * block + j * depth, local * block + (j + 1) * depth)
                    out_ref[o, cols] = (kept[:, cols].astype(F32) + s).astype(BF16)
                return carry

            lax.fori_loop(0, half // tile, finish, 0)
    for u, (_, d, way, count) in enumerate(units):
        owner = place(lax.rem(pos + d, n))
        to, local, slot = target(owner)

        @pl.when(to != tp)
        def _():
            ref = pd.at[owner, pl.ds(way, count), mine_rows]
            pltpu.make_async_remote_copy(
                src_ref=ref, dst_ref=ref, send_sem=out_send.at[u], recv_sem=out_recv.at[0, 0],
                device_id=(me, to), device_id_type=MESH,
            ).wait_send()
    for stream in range(4):
        for way in range(2):
            for s in range(n - 1):
                ring(stream, way, s, False).wait_send()


def paired_kernel(
    n, ntp,
    q_hbm, k_ref, v_ref, sink_ref, lab_row_ref,
    res_hbm, wout_hbm, gain_ref, wv_hbm, wg_hbm, taps_ref, wd_hbm,
    out_hbm,
    w3, other, kx, vx, lx, lp, lc, same, part, first, second, mixed, normed, value, gate,
    pd, box, yin1, zin1, zin2, yin2, res, q_ref, wout_ref, kept, result,
    loc_sem, halo_send, halo_recv, lab_send, lab_recv, zs, zr, xs, xr,
    core_send, core_recv, y_send, y_recv, ag_send, ag_recv, rim_send, rim_recv,
    box_send, box_recv, yo1_send, yo1_recv, zo1_send, zo1_recv, zo2_send, zo2_recv, yo2_send, yo2_recv, out_sem,
):
    me = lax.axis_index("sp")
    tp = lax.axis_index("tp")
    core = lax.rem(tp, 2)
    y = tp // 2
    z = me // 2
    x = lax.rem(me, 2)
    zh = z // 2
    own = lax.rem(z, 2)
    pair = 1 - own
    zp = 2 * zh + pair
    far_mid = 2 - zh
    far_end = 3 - 3 * zh
    partner = y * 2 + 1 - core
    across = (1 - y) * 2 + core
    beside = (zp * 2 + x, tp)
    sibling = (z * 2 + 1 - x, tp)
    rows, cols = q_hbm.shape
    half = rows // 2
    piece = half // 2
    block, hidden = wv_hbm.shape
    wide = w3.shape[2]
    narrow = hidden - wide
    model = wout_hbm.shape[1]
    span = out_hbm.shape[1]
    is_mid = (z == 1) | (z == 2)
    is_end = (z == 0) | (z == 3)
    is_wide = is_mid
    is_narrow = is_end
    roles = ((is_narrow, narrow, wide, 0, narrow), (is_wide, wide, narrow, narrow, 0))
    sides = (is_end, is_mid)

    def copy(src, dst, send, recv, where):
        return pltpu.make_async_remote_copy(
            src_ref=src, dst_ref=dst, send_sem=send, recv_sem=recv, device_id=where, device_id_type=MESH
        )

    def arrive(ref, recv):
        copy(ref, ref, core_send.at[0], recv, (me, partner)).wait_recv()

    def left(ref, send):
        copy(ref, ref, send, core_recv.at[0], (me, partner)).wait_send()

    def spot(s, zo, xo, width):
        return w3.at[s, pl.ds(pl.multiple_of((zo * 2 + xo) * block, block), block), pl.ds(0, width)]

    sources = (wv_hbm, wg_hbm, wd_hbm)

    def loads(s):
        for cond, width, rest, at, rest_at in roles:
            def pair_of():
                a = pltpu.make_async_copy(sources[s].at[:, pl.ds(at, width)], spot(s, z, x, width), loc_sem.at[s, 0])
                b = pltpu.make_async_copy(
                    sources[s].at[:, pl.ds(rest_at, rest)], other.at[s, :, pl.ds(0, rest)], loc_sem.at[s, 1]
                )
                return a, b
            yield cond, pair_of

    for s in range(3):
        for cond, pair_of in loads(s):
            @pl.when(cond)
            def _():
                for c in pair_of():
                    c.start()
    my_piece = core * half + y * piece
    res_load = pltpu.make_async_copy(res_hbm.at[pl.ds(pl.multiple_of(my_piece, piece), piece)], res, loc_sem.at[3, 0])
    res_load.start()
    late_loads = (
        pltpu.make_async_copy(q_hbm, q_ref, loc_sem.at[4, 0]),
        pltpu.make_async_copy(wout_hbm, wout_ref, loc_sem.at[4, 1]),
    )
    for c in late_loads:
        c.start()

    barrier = pltpu.get_barrier_semaphore()
    peers = [(lax.rem(me + j, n), tp) for j in range(1, n)] + [(me, lax.rem(tp + j, ntp)) for j in range(1, ntp)]
    for peer in peers:
        pl.semaphore_signal(barrier, inc=1, device_id=peer, device_id_type=MESH)

    def loaded(s):
        for cond, pair_of in loads(s):
            @pl.when(cond)
            def _():
                for c in pair_of():
                    c.wait()

    loaded(0)
    pl.semaphore_wait(barrier, len(peers))

    def begin_end(s):
        for cond, width, rest, _, _ in roles:
            @pl.when(is_end & cond)
            def _():
                b = other.at[s, :, pl.ds(0, rest)]
                copy(b, spot(s, z, x, rest), zs.at[s, 0], zr.at[s, 0], beside).start()

    def far_end_sends(s):
        for cond, width, rest, _, _ in roles:
            @pl.when(is_end & cond)
            def _():
                a = spot(s, z, x, width)
                copy(a, a, zs.at[s, 1], zr.at[s, 2], ((3 - z) * 2 + x, tp)).start()

    def far_mid_sends(s):
        for cond, width, rest, _, _ in roles:
            @pl.when(is_mid & cond)
            def _():
                b = other.at[s, :, pl.ds(0, rest)]
                copy(b, spot(s, z, x, rest), zs.at[s, 2], zr.at[s, 1], ((3 - zp) * 2 + x, tp)).start()

    def begin_mid(s):
        for cond, width, rest, _, _ in roles:
            @pl.when(is_mid & cond)
            def _():
                a = spot(s, z, x, width)
                copy(a, a, zs.at[s, 1], zr.at[s, 1], ((3 - z) * 2 + x, tp)).start()

    def begin_out(s):
        for cond, width, rest, _, _ in roles:
            @pl.when(is_mid & cond)
            def _():
                b = other.at[s, :, pl.ds(0, rest)]
                copy(b, spot(s, z, x, rest), zs.at[s, 0], zr.at[s, 0], beside).start()

    def begin_x(s, who=(0, 1)):
        for (cond, width, _, _, _), side in ((r, sides[w]) for r in roles for w in who):
            @pl.when(cond & side)
            def _():
                a = spot(s, z, x, width)
                copy(a, a, xs.at[s, 0], xr.at[s, 0], sibling).start()

    owners = (zp, far_mid, far_end)

    def event(s, j, who=(0, 1)):
        for side in who:
            for cond, width, _, _, _ in roles:
                @pl.when(sides[side] & cond)
                def _():
                    a = spot(s, owners[j], x, width)
                    arrive(a, zr.at[s, j])
                    if side == 1 and j == 0:
                        copy(a, a, zs.at[s, 3], zr.at[s, 2], ((3 - z) * 2 + x, tp)).start()
                    copy(a, a, xs.at[s, j + 1], xr.at[s, j + 1], sibling).start()

    def xwait(s, j):
        for cond, width, _, _, _ in roles:
            @pl.when(cond)
            def _():
                arrive(spot(s, ((z,) + owners)[j], 1 - x, width), xr.at[s, j])

    def finish_stream(s):
        for cond, width, rest, _, _ in roles:
            @pl.when(cond)
            def _():
                left(spot(s, z, x, rest), zs.at[s, 0])
                left(spot(s, z, x, width), zs.at[s, 1])
                for j in range(4):
                    left(spot(s, z, x, width), xs.at[s, j])

            @pl.when(is_mid & cond)
            def _():
                left(spot(s, z, x, rest), zs.at[s, 2])
                left(spot(s, z, x, width), zs.at[s, 3])

    right, before = lax.rem(me + 1, n), lax.rem(me + n - 1, n)
    ends = pl.ds(rows - WINDOW, WINDOW)
    starts = pl.ds(0, WINDOW)
    low, high = pl.ds(0, WINDOW), pl.ds(rows + WINDOW, WINDOW)
    halo = []
    for i, (src, dst) in enumerate(((k_ref, kx), (v_ref, vx))):
        halo.append(copy(src.at[ends], dst.at[low], halo_send.at[i, 0], halo_recv.at[i, 0], (right, tp)))
        halo.append(copy(src.at[starts], dst.at[high], halo_send.at[i, 1], halo_recv.at[i, 1], (before, tp)))
    halo.append(copy(lab_row_ref.at[:, ends], lx.at[:, low], halo_send.at[2, 0], halo_recv.at[2, 0], (right, tp)))
    halo.append(copy(lab_row_ref.at[:, starts], lx.at[:, high], halo_send.at[2, 1], halo_recv.at[2, 1], (before, tp)))
    for c in halo:
        c.start()
    begin_end(0)
    begin_mid(0)
    begin_out(0)
    far_end_sends(0)
    far_mid_sends(0)
    begin_x(0)
    loaded(1)
    begin_end(1)
    begin_x(1)
    loaded(2)
    begin_x(2, (0,))

    @pl.when(is_narrow)
    def _():
        if narrow < wide:
            w3[:, :, narrow:wide] = jnp.zeros((3, n * block, wide - narrow), BF16)

    inner = pl.ds(WINDOW, rows)
    kx[inner, :] = k_ref[...]
    vx[inner, :] = v_ref[...]
    lx[:, inner] = lab_row_ref[...]
    lab_copy = copy(lx, lp, lab_send, lab_recv, beside)
    chunks = rows // WINDOW

    def columns(row_ref, which):
        for i in which:
            chunk = slice(i * WINDOW, (i + 1) * WINDOW)
            square = jnp.broadcast_to(row_ref[0:1, chunk].astype(F32), (WINDOW, WINDOW))
            lc[chunk, :] = jnp.transpose(square)

    def neighbours(slot):
        for i in range(chunks):
            here = lc[WINDOW * (i + 1):WINDOW * (i + 2), :]
            for side, shift in ((0, -1), (1, 1)):
                there = lc[WINDOW * (i + 1) + shift:WINDOW * (i + 2) + shift, :]
                same[slot, side, i * WINDOW:(i + 1) * WINDOW, :] = jnp.where(here == there, 1.0, 0.0)

    columns(lx, range(1, chunks + 1))

    def edges():
        for c in halo:
            c.wait()
        lx[:, low] = jnp.where(me == 0, -1, lx[:, low])
        lx[:, high] = jnp.where(me == n - 1, -1, lx[:, high])
        lab_copy.start()
        columns(lx, (0, chunks + 1))
        neighbours(own)

    kv_local = k_ref.shape[1] // HEAD_DIM
    per_kv = cols // k_ref.shape[1]
    per_half = chunks // 2
    tile = 32

    def attend(i, carry):
        own_half = i // per_half
        j = lax.rem(i, per_half)
        flip = (1 - own_half) * core + own_half * (1 - y)
        turn = flip * (per_half - 1 - j) + (1 - flip) * j
        b = ((1 - own_half) * (1 - core) + own_half * core) * per_half + turn
        here = pl.ds(pl.multiple_of(b * WINDOW, WINDOW), WINDOW)
        wide_keys = pl.ds(pl.multiple_of(b * WINDOW, WINDOW), 3 * WINDOW)
        q = q_ref[here, :] * jnp.asarray(HEAD_DIM ** (-0.5), BF16)
        kw = kx[wide_keys, :]
        vw = vx[wide_keys, :]
        lab_k = lx[0:1, wide_keys].astype(F32)
        lab_q = lc[pl.ds(pl.multiple_of(b * WINDOW + WINDOW, WINDOW), WINDOW), 0:1]
        key = lax.broadcasted_iota(jnp.int32, (WINDOW, 3 * WINDOW), 1) - WINDOW
        query = lax.broadcasted_iota(jnp.int32, (WINDOW, 3 * WINDOW), 0)
        allowed = (jnp.abs(key - query) <= WINDOW) & (lab_q == lab_k)
        results = []
        for g in range(kv_local):
            k = kw[:, g * HEAD_DIM:(g + 1) * HEAD_DIM]
            v = vw[:, g * HEAD_DIM:(g + 1) * HEAD_DIM]
            heads = range(g * per_kv, (g + 1) * per_kv)
            stacked = jnp.concatenate([q[:, h * HEAD_DIM:(h + 1) * HEAD_DIM] for h in heads], axis=0)
            scores = lax.dot_general(stacked, k, (((1,), (1,)), ((), ())), preferred_element_type=F32)
            raws, scales = [], []
            for u, h in enumerate(heads):
                score = jnp.where(allowed, scores[u * WINDOW:(u + 1) * WINDOW], NEG)
                sink = sink_ref[h]
                highest = jnp.maximum(jnp.max(score, axis=1, keepdims=True), sink)
                raw = jnp.exp(score - highest)
                scales.append(1.0 / (jnp.sum(raw, axis=1, keepdims=True) + jnp.exp(sink - highest)))
                raws.append(raw.astype(BF16))
            summed = jnp.dot(jnp.concatenate(raws, axis=0), v, preferred_element_type=F32)
            for u in range(per_kv):
                results.append((summed[u * WINDOW:(u + 1) * WINDOW] * scales[u]).astype(BF16))
        attended = jnp.concatenate(results, axis=1)
        part[here, :] = jnp.dot(attended, wout_ref[...], preferred_element_type=F32).astype(BF16)
        mine = first.at[pl.ds(pl.multiple_of(turn * WINDOW, WINDOW), WINDOW)]

        @pl.when(own_half == 0)
        def _():
            copy(part.at[here], mine, core_send.at[turn], core_recv.at[turn], (me, partner)).start()

        @pl.when(own_half == 1)
        def _():
            arrive(mine, core_recv.at[turn])

            def add(t, carry):
                r = pl.ds(pl.multiple_of(turn * WINDOW + t * tile, tile), tile)
                o = pl.ds(pl.multiple_of(b * WINDOW + t * tile, tile), tile)
                first[r, :] = (part[o, :].astype(F32) + first[r, :].astype(F32)).astype(BF16)
                return carry

            lax.fori_loop(0, WINDOW // tile, add, 0)

        @pl.when(i == per_half)
        def _():
            y_copy(0, y).start()

        @pl.when(i == per_half + 1)
        def _():
            y_copy(1, y).start()

        @pl.when(i == 1)
        def _():
            edges()

        @pl.when(i == 3)
        def _():
            event(0, 0, (1,))
            begin_mid(1)
            begin_out(1)
            far_mid_sends(1)

        @pl.when(i == 4)
        def _():
            event(0, 1, (1,))

        return carry

    def y_copy(k, yy):
        if k == 0:
            count, src, dst = 2 * piece // 3, (1 - yy) * (half - 2 * piece // 3), (1 - yy) * (piece // 3)
        else:
            count, src, dst = piece // 3, 2 * piece // 3 + (1 - yy) * (piece // 3), yy * (2 * piece // 3)
        return copy(
            first.at[pl.ds(pl.multiple_of(src, 64), count)], second.at[pl.ds(pl.multiple_of(dst, 64), count)],
            y_send.at[k], y_recv.at[k], (me, across),
        )

    res_load.wait()
    for c in late_loads:
        c.wait()
    lax.fori_loop(0, 2 * per_half, attend, 0)
    for k in range(2):
        y_copy(k, 1 - y).wait_recv()

    def norm(slot, start, count):
        def body(i, carry):
            r = pl.ds(pl.multiple_of(start + i * tile, tile), tile)
            m = mixed[r, :].astype(F32)
            mean_sq = jnp.mean(m * m, axis=1, keepdims=True)
            normed[slot, r, :] = (m * lax.rsqrt(mean_sq + EPS) * gain_ref[...]).astype(BF16)
            return carry

        lax.fori_loop(0, count // tile, body, 0)

    def add_second(i, carry):
        r = pl.ds(pl.multiple_of(i * tile, tile), tile)
        f = pl.ds(pl.multiple_of(y * piece + i * tile, tile), tile)
        o = pl.ds(pl.multiple_of(my_piece + i * tile, tile), tile)
        s = first[f, :].astype(F32) + second[r, :].astype(F32)
        mixed[o, :] = (res[r, :].astype(F32) + s).astype(BF16)
        return carry

    lax.fori_loop(0, piece // tile, add_second, 0)

    def part_of(c, yy):
        return c * half + yy * piece

    def mixed_at(c, yy):
        return mixed.at[pl.ds(pl.multiple_of(part_of(c, yy), piece), piece)]

    bit = piece // 2

    def normed_at(slot, c, yy, b):
        return normed.at[slot, pl.ds(pl.multiple_of(part_of(c, yy) + b * bit, bit), bit)]

    def share(k, ref, where):
        copy(ref, ref, ag_send.at[k], ag_recv.at[k], where).start()

    share(0, mixed_at(core, y), (me, across))
    share(1, mixed_at(core, y), (me, partner))
    norm(own, my_piece, piece)
    for b in range(2):
        share(4 + b, normed_at(own, core, y, b), beside)
    event(0, 0, (0,))
    event(1, 0, (1,))
    event(0, 1, (0,))
    arrive(mixed_at(1 - core, y), ag_recv.at[1])
    norm(own, part_of(1 - core, y), piece)
    event(0, 2, (1,))
    arrive(mixed_at(core, 1 - y), ag_recv.at[0])
    share(2, mixed_at(core, 1 - y), (me, partner))
    norm(own, part_of(core, 1 - y), piece)
    event(0, 2, (0,))

    def serve_spread(b):
        arrive(normed_at(pair, core, y, b), ag_recv.at[4 + b])
        share(6 + b, normed_at(pair, core, y, b), (me, across))
        share(8 + b, normed_at(pair, core, y, b), (me, partner))

    event(1, 0, (0,))
    far_end_sends(1)
    event(1, 1, (0,))
    serve_spread(0)
    serve_spread(1)
    event(1, 1, (1,))
    begin_end(2)
    arrive(mixed_at(1 - core, 1 - y), ag_recv.at[2])
    norm(own, part_of(1 - core, 1 - y), piece)

    big = rows // 3

    def project(which, slot):
        def body(t, carry):
            r = pl.ds(pl.multiple_of(t * big, big), big)
            product = jnp.dot(normed[slot, r, :], w3[which], preferred_element_type=F32).astype(BF16)
            if which == 0:
                value[slot, pl.ds(pl.multiple_of(RIM + t * big, RIM), big), :] = product
            else:
                gate[slot, r, :] = product
            return carry

        lax.fori_loop(0, 3, body, 0)

    inside = pl.ds(RIM, RIM)
    last = pl.ds(rows, RIM)
    fronts, backs = pl.ds(0, RIM), pl.ds(RIM + rows, RIM)
    facing = ((3 - z) * 2 + 1 - x, tp)
    near_rims = (
        (x == 0, ((0, last, 0, 0), (1, inside, 0, 1), (1, last, 1, 0))),
        (x == 1, ((0, inside, 0, 1), (0, last, 1, 0), (1, inside, 1, 1))),
    )
    far_rims = (((x == 0) & (zh == 1), (0, inside, 1, 1)), ((x == 1) & (zh == 0), (1, last, 0, 0)))

    def rim_copy(frm, source, to, side, where):
        target = value.at[to, (fronts, backs)[side]]
        pad = 2 * to + side
        copy(value.at[frm, source], target, rim_send.at[pad], rim_recv.at[pad], where).start()

    def send_far_rims(side):
        for cond, spec in far_rims:
            @pl.when(cond & side)
            def _():
                rim_copy(*spec, facing)

    mine = mixed.at[:, pl.ds(pl.multiple_of(tp * span, span), span)]
    kept_copy = pltpu.make_async_copy(mine, kept, loc_sem.at[3, 1])
    kept_copy.start()

    def serve_x(s):
        for j in range(4):
            xwait(s, j)

    serve_x(0)
    project(0, own)
    send_far_rims(is_mid)
    begin_mid(2)
    begin_out(2)
    far_mid_sends(2)
    event(1, 2)

    def serve_diagonal(b):
        arrive(normed_at(pair, core, 1 - y, b), ag_recv.at[6 + b])
        share(10 + b, normed_at(pair, core, 1 - y, b), (me, partner))

    def serve_rest(b):
        arrive(normed_at(pair, 1 - core, y, b), ag_recv.at[8 + b])
        arrive(normed_at(pair, 1 - core, 1 - y, b), ag_recv.at[10 + b])

    serve_diagonal(0)
    serve_diagonal(1)
    serve_rest(0)
    serve_rest(1)
    project(0, pair)

    send_far_rims(is_end)
    for cond, specs in near_rims:
        @pl.when(cond)
        def _():
            for spec in specs:
                rim_copy(*spec, sibling)

    far_end_sends(2)
    begin_x(2, (1,))
    event(2, 0, (0,))
    serve_x(1)
    project(1, own)
    event(2, 0, (1,))
    project(1, pair)
    event(2, 1, (1,))
    lab_copy.wait()
    columns(lp, range(chunks + 2))
    neighbours(pair)

    def serve_rims(slot):
        for side, rd in enumerate((fronts, backs)):
            if slot == side:
                @pl.when((x != side) | (zh != side))
                def _():
                    arrive(value.at[slot, rd], rim_recv.at[2 * slot + side])

                @pl.when((x == side) & (zh == side))
                def _():
                    value[slot, rd, :] = jnp.zeros((RIM, wide), BF16)
            else:
                arrive(value.at[slot, rd], rim_recv.at[2 * slot + side])

    serve_rims(0)
    serve_rims(1)

    taps_all = taps_ref[...].astype(F32)
    taps = jnp.where(is_wide, taps_all[:, narrow:], taps_all[:, :wide])
    step = 64
    lanes = wide // WINDOW

    for slot in range(2):
        def gated(i, carry):
            base = i * step
            r = pl.ds(pl.multiple_of(base, step), step)
            x_rows = value[slot, pl.ds(pl.multiple_of(RIM + base, RIM), step), :].astype(F32)
            above = value[slot, pl.ds(pl.multiple_of(base, RIM), RIM), :].astype(F32)[RIM - 1:RIM]
            below = value[slot, pl.ds(pl.multiple_of(RIM + base + step, RIM), RIM), :].astype(F32)[0:1]
            prev = jnp.concatenate([above, x_rows[:-1]], axis=0)
            nxt = jnp.concatenate([x_rows[1:], below], axis=0)
            with_prev = jnp.concatenate([same[slot, 0, r, :]] * lanes, axis=1) > 0.5
            with_next = jnp.concatenate([same[slot, 1, r, :]] * lanes, axis=1) > 0.5
            conv = (
                taps[0:1] * jnp.where(with_prev, prev, 0.0)
                + taps[1:2] * x_rows
                + taps[2:3] * jnp.where(with_next, nxt, 0.0)
            )
            gate[slot, r, :] = (conv * jax.nn.sigmoid(conv) * gate[slot, r, :].astype(F32)).astype(BF16)
            return carry

        lax.fori_loop(0, rows // step, gated, 0)

    order = (z, zp, far_mid, far_end)
    quarter = rows // 2

    def boxed(u, k):
        slot = (pair, own)[k]
        return copy(pd.at[u, slot], box.at[u // 2, slot], box_send.at[u, k], box_recv.at[u // 2, k], (me, partner))

    def lower(u):
        t = order[u]
        w = w3[2, pl.ds(pl.multiple_of(t * span, span), span), :]
        for k, slot in enumerate((pair, own)):
            def body(i, carry):
                r = pl.ds(pl.multiple_of(i * quarter, quarter), quarter)
                pd[u, slot, r, :] = lax.dot_general(
                    gate[slot, r, :], w, (((1,), (1,)), ((), ())), preferred_element_type=F32
                ).astype(BF16)
                return carry

            lax.fori_loop(0, 2, body, 0)

            @pl.when(core != lax.rem(t, 2))
            def _():
                boxed(u, k).start()

    cuts = (rows // 6 * 3, rows // 6 * 3, rows // 6 * 3, rows // 6 * 2)

    def segment(u, g):
        count = (rows - cuts[u]) // 2
        return cuts[u] + g * count, count

    slab = rows // 12

    def accumulate(ref, slot, at, count, other_ref, base):
        def body(i, carry):
            r = pl.ds(pl.multiple_of(at + i * slab, slab), slab)
            o = pl.ds(pl.multiple_of(base + i * slab, slab), slab)
            ref[slot, r, :] = (ref[slot, r, :].astype(F32) + other_ref[o, :].astype(F32)).astype(BF16)
            return carry

        lax.fori_loop(0, count // slab, body, 0)

    def z_first(u, g):
        at, count = segment(u, g)
        return copy(
            pd.at[u, pair, pl.ds(at, count)], zin1.at[u // 2, g, pl.ds(0, count)],
            zo1_send.at[u // 2, g], zo1_recv.at[u // 2, g], beside,
        )

    def then_y(u, g):
        at, count = segment(u, g)
        return copy(
            pd.at[u, own, pl.ds(at, count)], yin2.at[g, pl.ds(0, count)], yo2_send.at[g], yo2_recv.at[g], (me, across)
        )

    def y_first(u, slot, k):
        top = pl.ds(0, cuts[u])
        return copy(pd.at[u, slot, top], yin1.at[slot, top], yo1_send.at[k], yo1_recv.at[k], (me, across))

    def then_z(u):
        top = pl.ds(0, cuts[u])
        return copy(pd.at[u, pair, top], zin2.at[top], zo2_send, zo2_recv, beside)

    def stage_one(u):
        t = order[u]

        @pl.when(core == lax.rem(t, 2))
        def _():

            def add(slot, at, count):
                accumulate(pd.at[u], slot, at, count, box.at[u // 2, slot], at)

            arrive(box.at[u // 2, pair], box_recv.at[u // 2, 0])
            if u < 3:
                add(pair, 0, cuts[u])

                @pl.when(y != t // 2)
                def _():
                    y_first(u, pair, 0).start()

            for g in range(2):
                add(pair, *segment(u, g))
                z_first(u, g).start()
            if u == 3:
                add(pair, 0, cuts[u])

                @pl.when(y != t // 2)
                def _():
                    y_first(u, pair, 0).start()

            arrive(box.at[u // 2, own], box_recv.at[u // 2, 1])
            add(own, 0, cuts[u])

            @pl.when(y != t // 2)
            def _():
                y_first(u, own, 1).start()

            for g in range(2):
                add(own, *segment(u, g))

    def stage_y(u):
        t = order[u]

        @pl.when(tp == t)
        def _():
            top = pl.ds(0, cuts[u])
            arrive(yin1.at[pair, top], yo1_recv.at[0])
            accumulate(pd.at[u], pair, 0, cuts[u], yin1.at[pair], 0)
            then_z(u).start()
            arrive(yin1.at[own, top], yo1_recv.at[1])
            accumulate(pd.at[u], own, 0, cuts[u], yin1.at[own], 0)

    def stage_z(u):
        t = order[u]

        @pl.when(core == lax.rem(t, 2))
        def _():
            for g in range(2):
                at, count = segment(u, g)
                arrive(zin1.at[u // 2, g, pl.ds(0, count)], zo1_recv.at[u // 2, g])
                accumulate(pd.at[u], own, at, count, zin1.at[u // 2, g], 0)

                @pl.when(y != t // 2)
                def _():
                    then_y(u, g).start()

    def put(at, count, k):
        r = pl.ds(at, count)
        return pltpu.make_async_copy(result.at[r], out_hbm.at[r], out_sem.at[k])

    def stage_three(u):
        t = order[u]

        @pl.when(tp == t)
        def _():
            def close(at, count, extra, k):
                def body(i, carry):
                    r = pl.ds(pl.multiple_of(i * slab, slab), slab)
                    o = pl.ds(pl.multiple_of(at + i * slab, slab), slab)
                    s = pd[u, own, o, :].astype(F32) + extra[r, :].astype(F32)
                    result[o, :] = (kept[o, :].astype(F32) + s).astype(BF16)
                    return carry

                lax.fori_loop(0, count // slab, body, 0)
                put(at, count, k).start()

            arrive(zin2.at[pl.ds(0, cuts[u])], zo2_recv)
            close(0, cuts[u], zin2, 0)
            for g in range(2):
                at, count = segment(u, g)
                arrive(yin2.at[g, pl.ds(0, count)], yo2_recv.at[g])
                close(at, count, yin2.at[g], 1 + g)
            put(0, cuts[u], 0).wait()
            for g in range(2):
                put(*segment(u, g), 1 + g).wait()

    def drain(u):
        t = order[u]

        @pl.when(core != lax.rem(t, 2))
        def _():
            for k in range(2):
                boxed(u, k).wait_send()

        @pl.when(core == lax.rem(t, 2))
        def _():
            for g in range(2):
                z_first(u, g).wait_send()

            @pl.when(y != t // 2)
            def _():
                for k, slot in enumerate((pair, own)):
                    y_first(u, slot, k).wait_send()
                for g in range(2):
                    then_y(u, g).wait_send()

            @pl.when(y == t // 2)
            def _():
                then_z(u).wait_send()

    xwait(2, 0)
    lower(0)
    event(2, 1, (0,))
    stage_one(0)
    xwait(2, 1)
    lower(1)
    stage_one(1)
    event(2, 2)
    xwait(2, 2)
    lower(2)
    stage_one(2)
    xwait(2, 3)
    lower(3)
    stage_one(3)
    stage_z(0)
    stage_z(1)
    stage_y(0)
    stage_y(1)
    stage_z(2)
    stage_z(3)
    stage_y(2)
    stage_y(3)
    kept_copy.wait()
    stage_three(0)
    stage_three(1)
    stage_three(2)
    stage_three(3)

    for s in range(3):
        finish_stream(s)
    for j in range(per_half):
        left(first.at[pl.ds(0, WINDOW)], core_send.at[j])
    for k in range(2):
        y_copy(k, y).wait_send()
    for k in range(3):
        left(mixed_at(core, y), ag_send.at[k])
    for k in range(4, 12):
        left(normed_at(own, core, y, 0), ag_send.at[k])
    for pad in range(4):
        sends = (x == pad // 3) | (zh == pad // 3) if pad in (0, 3) else x >= 0

        @pl.when(sends)
        def _():
            left(value.at[0, fronts], rim_send.at[pad])
    for u in range(4):
        drain(u)


def solution(mesh):
    n, ntp = mesh.shape["sp"], mesh.shape["tp"]

    def by_ring(q, k, v, sink, doc, res, wout, gain, wv, wg, taps, wd):
        rows, model = res.shape
        hidden = wv.shape[1]
        block = wv.shape[0]
        ny = ntp // 2
        labels = doc + 1
        lab_row = labels[None, :]
        vm = pl.BlockSpec(memory_space=pltpu.VMEM)
        hbm = pl.BlockSpec(memory_space=pl.ANY)
        smem = pl.BlockSpec(memory_space=pltpu.SMEM)
        dma = pltpu.SemaphoreType.DMA
        kvc = k.shape[1]
        span = model // ntp
        scratch = [
            pltpu.VMEM((2, n * block, hidden), BF16),
            pltpu.VMEM((n * block, hidden), BF16),
            pltpu.VMEM((rows + 2 * WINDOW, kvc), BF16),
            pltpu.VMEM((rows + 2 * WINDOW, kvc), BF16),
            pltpu.VMEM((1, rows + 2 * WINDOW), jnp.int32),
            pltpu.VMEM((rows + 2 * WINDOW, WINDOW), F32),
            pltpu.VMEM((rows, model), BF16),
            pltpu.VMEM((rows // 2, model), BF16),
            pltpu.VMEM((max(ny - 1, 1), rows // 2 // ny, model), BF16),
            pltpu.VMEM((rows, model), BF16),
            pltpu.VMEM((rows, model), BF16),
            pltpu.VMEM((rows, hidden), BF16),
            pltpu.VMEM((rows, hidden), BF16),
            pltpu.VMEM((2, RIM, hidden), BF16),
            pltpu.VMEM((n, 2, rows, block // 2), BF16),
            pltpu.VMEM((n, 2, rows // 2, block // 2), BF16),
            pltpu.VMEM((n // ntp, ntp - 1, 2, rows // 2, block // 2), BF16),
            pltpu.VMEM((rows // 2 // ny, model), BF16),
            dma((4,)),
            dma((4, 2, n - 1)), dma((4, 2, n - 1)),
            dma((3, 2)), dma((3, 2)),
            dma((2,)), dma((2,)),
            dma, dma,
            dma((ny,)), dma((ny,)),
            dma((ny,)), dma((ny,)),
            dma, dma,
            dma((n + 2,)), dma((n + 2,)),
            dma((n + 2,)), dma((n // ntp, ntp - 1)),
        ]
        return pl.pallas_call(
            functools.partial(ring_kernel, n, ntp),
            out_shape=jax.ShapeDtypeStruct((rows, span), BF16),
            in_specs=[vm, vm, vm, smem, vm, hbm, vm, vm, hbm, hbm, vm, hbm],
            out_specs=vm,
            scratch_shapes=scratch,
            compiler_params=pltpu.CompilerParams(
                collective_id=0, has_side_effects=True, vmem_limit_bytes=67043328
            ),
            name="layer",
        )(q, k, v, sink, lab_row, res, wout, gain[None, :], wv, wg, taps, wd)


    def by_pairs(q, k, v, sink, doc, res, wout, gain, wv, wg, taps, wd):
        rows, model = res.shape
        block, hidden = wv.shape
        half = rows // 2
        piece = half // 2
        span = model // ntp
        kvc = k.shape[1]
        third = rows // 12 * 5
        wide = (hidden // LANES + 1) // 2 * LANES
        lab_row = doc[None, :]
        vm = pl.BlockSpec(memory_space=pltpu.VMEM)
        hbm = pl.BlockSpec(memory_space=pl.ANY)
        smem = pl.BlockSpec(memory_space=pltpu.SMEM)
        dma = pltpu.SemaphoreType.DMA
        scratch = [
            pltpu.VMEM((3, n * block, wide), BF16),
            pltpu.VMEM((3, block, wide), BF16),
            pltpu.VMEM((rows + 2 * WINDOW, kvc), BF16),
            pltpu.VMEM((rows + 2 * WINDOW, kvc), BF16),
            pltpu.VMEM((1, rows + 2 * WINDOW), jnp.int32),
            pltpu.VMEM((1, rows + 2 * WINDOW), jnp.int32),
            pltpu.VMEM((rows + 2 * WINDOW, WINDOW), F32),
            pltpu.VMEM((2, 2, rows, WINDOW), F32),
            pltpu.VMEM((rows, model), BF16),
            pltpu.VMEM((half, model), BF16),
            pltpu.VMEM((piece, model), BF16),
            pltpu.VMEM((rows, model), BF16),
            pltpu.VMEM((2, rows, model), BF16),
            pltpu.VMEM((2, rows + 2 * RIM, wide), BF16),
            pltpu.VMEM((2, rows, wide), BF16),
            pltpu.VMEM((4, 2, rows, span), BF16),
            pltpu.VMEM((2, 2, rows, span), BF16),
            pltpu.VMEM((2, half, span), BF16),
            pltpu.VMEM((2, 2, third, span), BF16),
            pltpu.VMEM((half, span), BF16),
            pltpu.VMEM((2, third, span), BF16),
            pltpu.VMEM((piece, model), BF16),
            pltpu.VMEM(q.shape, BF16),
            pltpu.VMEM(wout.shape, BF16),
            pltpu.VMEM((rows, span), BF16),
            pltpu.VMEM((rows, span), BF16),
            dma((5, 2)),
            dma((3, 2)), dma((3, 2)),
            dma, dma,
            dma((3, 4)), dma((3, 3)),
            dma((3, 4)), dma((3, 4)),
            dma((rows // WINDOW // 2,)), dma((rows // WINDOW // 2,)),
            dma((2,)), dma((2,)),
            dma((12,)), dma((12,)),
            dma((4,)), dma((4,)),
            dma((4, 2)), dma((2, 2)),
            dma((2,)), dma((2,)),
            dma((2, 2)), dma((2, 2)),
            dma, dma,
            dma((2,)), dma((2,)),
            dma((3,)),
        ]
        return pl.pallas_call(
            functools.partial(paired_kernel, n, ntp),
            out_shape=jax.ShapeDtypeStruct((rows, span), BF16),
            in_specs=[hbm, vm, vm, smem, vm, hbm, hbm, vm, hbm, hbm, vm, hbm],
            out_specs=hbm,
            scratch_shapes=scratch,
            compiler_params=pltpu.CompilerParams(
                collective_id=0, has_side_effects=True, vmem_limit_bytes=67043328
            ),
            name="layer",
        )(q, k, v, sink, lab_row, res, wout, gain[None, :], wv, wg, taps, wd)

    placed = (
        P("sp", "tp"), P("sp", "tp"), P("sp", "tp"), P("tp"), P("sp"), P("sp", None),
        P("tp", None), P(), P("sp", "tp"), P("sp", "tp"), P(None, "tp"), P("sp", "tp"),
    )
    return jax.shard_map(
        by_pairs if (n, ntp) == (8, 4) else by_ring, mesh=mesh, in_specs=placed, out_specs=P("sp", "tp"), check_vma=False
    )
```

```python
import functools

import jax
import jax.numpy as jnp
from jax import lax
from jax.experimental import pallas as pl
from jax.experimental.pallas import tpu as pltpu
from jax.sharding import PartitionSpec as P

HEAD_DIM = 64
WINDOW = 128
EPS = 1e-06
NEG = -1e30
RIM = 16
LANES = 128
MESH = pl.DeviceIdType.MESH
F32 = jnp.float32
BF16 = jnp.bfloat16


def ring_kernel(
    n, ntp,
    q_ref, k_ref, v_ref, sink_ref, lab_row_ref,
    res_hbm, wout_ref, gain_ref, wv_hbm, wg_hbm, taps_ref, wd_hbm,
    out_ref,
    up, down, kx, vx, lx, lc, part, first, second, mixed, normed, value, gate, rim, pd, box, inbox, res,
    loc_sem, ring_send, ring_recv, halo_send, halo_recv, rim_send, rim_recv,
    core_send, core_recv, y_send, y_recv, back_send, back_recv, pair_send, pair_recv,
    down_send, down_recv, out_send, out_recv,
):
    me = lax.axis_index("sp")
    tp = lax.axis_index("tp")
    core = lax.rem(tp, 2)
    y = tp // 2
    ny = ntp // 2
    partner = y * 2 + 1 - core
    rows = q_ref.shape[0]
    half = rows // 2
    piece = half // ny
    block = wv_hbm.shape[0]
    depth = block // 2
    quarter = block // 4

    def place(p):
        h = p // (n // 2)
        return (1 - h) * (2 * p) + h * (2 * n - 1 - 2 * p)

    odd = lax.rem(me, 2)
    pos = (1 - odd) * (me // 2) + odd * ((2 * n - 1 - me) // 2)
    ahead = place(lax.rem(pos + 1, n))
    behind = place(lax.rem(pos + n - 1, n))
    right = lax.rem(me + 1, n)
    left = lax.rem(me + n - 1, n)

    loads = []
    for i, (src, dst) in enumerate((
        (wv_hbm, up.at[0, pl.ds(me * block, block)]),
        (wg_hbm, up.at[1, pl.ds(me * block, block)]),
        (wd_hbm, down.at[pl.ds(me * block, block)]),
        (res_hbm.at[pl.ds(core * half + y * piece, piece)], res),
    )):
        c = pltpu.make_async_copy(src, dst, loc_sem.at[i])
        c.start()
        loads.append(c)

    barrier = pltpu.get_barrier_semaphore()
    peers = [(ahead, tp), (behind, tp), (right, tp), (left, tp)]
    for j in range(1, ntp):
        peers.append((me, lax.rem(tp + j, ntp)))
    for peer in peers:
        pl.semaphore_signal(barrier, inc=1, device_id=peer, device_id_type=MESH)
    for c in loads:
        c.wait()
    pl.semaphore_wait(barrier, len(peers))

    def spot(stream, way, owner):
        if stream < 2:
            return up.at[stream, pl.ds(owner * block + way * depth, depth)]
        return down.at[pl.ds(owner * block + way * depth + (stream - 2) * quarter, quarter)]

    def ring(stream, way, s, arriving):
        shift = s + 1 if arriving else s
        owner = place(lax.rem(pos + n - shift, n)) if way == 0 else place(lax.rem(pos + shift, n))
        ref = spot(stream, way, owner)
        return pltpu.make_async_remote_copy(
            src_ref=ref, dst_ref=ref,
            send_sem=ring_send.at[stream, way, s], recv_sem=ring_recv.at[stream, way, s],
            device_id=(ahead if way == 0 else behind, tp), device_id_type=MESH,
        )

    def begin(stream):
        for way in range(2):
            ring(stream, way, 0, False).start()

    def forward(stream, s, last=False):
        for way in range(2):
            ring(stream, way, s, True).wait_recv()
            if not last:
                ring(stream, way, s + 1, False).start()

    queue = []
    for s in range(n - 1):
        for stream in (0, 1):
            queue.append((stream, s))
    for s in range(n - 1):
        for stream in (2, 3):
            queue.append((stream, s))
    done = [0]

    def serve(count):
        for _ in range(count):
            if done[0] == len(queue):
                return
            stream, s = queue[done[0]]
            done[0] += 1
            forward(stream, s, last=s == n - 2)
            if stream < 2 and s == n - 2:
                begin(stream + 2)

    halo = []

    def remote(src, dst, send, recv, where):
        c = pltpu.make_async_remote_copy(
            src_ref=src, dst_ref=dst, send_sem=send, recv_sem=recv, device_id=where, device_id_type=MESH
        )
        c.start()
        return c

    ends = pl.ds(rows - WINDOW, WINDOW)
    starts = pl.ds(0, WINDOW)
    low, high = pl.ds(0, WINDOW), pl.ds(rows + WINDOW, WINDOW)
    for i, (src, dst) in enumerate(((k_ref, kx), (v_ref, vx))):
        halo.append(remote(src.at[ends], dst.at[low], halo_send.at[i, 0], halo_recv.at[i, 0], (right, tp)))
        halo.append(remote(src.at[starts], dst.at[high], halo_send.at[i, 1], halo_recv.at[i, 1], (left, tp)))
    halo.append(remote(lab_row_ref.at[:, ends], lx.at[:, low], halo_send.at[2, 0], halo_recv.at[2, 0], (right, tp)))
    halo.append(remote(lab_row_ref.at[:, starts], lx.at[:, high], halo_send.at[2, 1], halo_recv.at[2, 1], (left, tp)))
    begin(0)
    begin(1)
    inner = pl.ds(WINDOW, rows)
    kx[inner, :] = k_ref[...]
    vx[inner, :] = v_ref[...]
    lx[:, inner] = lab_row_ref[...]
    for c in halo:
        c.wait()
    lx[:, low] = jnp.where(me == 0, -1, lx[:, low])
    lx[:, high] = jnp.where(me == n - 1, -1, lx[:, high])
    for i in range(rows // WINDOW + 2):
        chunk = slice(i * WINDOW, (i + 1) * WINDOW)
        square = jnp.broadcast_to(lx[0:1, chunk].astype(F32), (WINDOW, WINDOW))
        lc[chunk, :] = jnp.transpose(square)

    kv_local = k_ref.shape[1] // HEAD_DIM
    per_kv = q_ref.shape[1] // k_ref.shape[1]
    blocks = rows // WINDOW
    model = wout_ref.shape[1]

    def attend(b, carry):
        here = pl.ds(pl.multiple_of(b * WINDOW, WINDOW), WINDOW)
        wide = pl.ds(pl.multiple_of(b * WINDOW, WINDOW), 3 * WINDOW)
        q = q_ref[here, :]
        kw = kx[wide, :]
        vw = vx[wide, :]
        lab_k = lx[0:1, wide].astype(F32)
        lab_q = lc[pl.ds(pl.multiple_of(b * WINDOW + WINDOW, WINDOW), WINDOW), 0:1]
        key = lax.broadcasted_iota(jnp.int32, (WINDOW, 3 * WINDOW), 1) - WINDOW
        query = lax.broadcasted_iota(jnp.int32, (WINDOW, 3 * WINDOW), 0)
        allowed = (jnp.abs(key - query) <= WINDOW) & (lab_q == lab_k)
        results = []
        for g in range(kv_local):
            k = kw[:, g * HEAD_DIM:(g + 1) * HEAD_DIM]
            v = vw[:, g * HEAD_DIM:(g + 1) * HEAD_DIM]
            for j in range(per_kv):
                h = g * per_kv + j
                qh = q[:, h * HEAD_DIM:(h + 1) * HEAD_DIM]
                score = lax.dot_general(
                    qh, k, (((1,), (1,)), ((), ())), preferred_element_type=F32
                ) * HEAD_DIM ** (-0.5)
                score = jnp.where(allowed, score, NEG)
                sink = sink_ref[h]
                highest = jnp.maximum(jnp.max(score, axis=1, keepdims=True), sink)
                raw = jnp.where(allowed, jnp.exp(score - highest), 0.0)
                total = jnp.sum(raw, axis=1, keepdims=True) + jnp.exp(sink - highest)
                probs = (raw / total).astype(BF16)
                results.append(jnp.dot(probs, v, preferred_element_type=F32).astype(BF16))
        attended = jnp.concatenate(results, axis=1)
        part[here, :] = jnp.dot(attended, wout_ref[...], preferred_element_type=F32).astype(BF16)
        return carry

    split = blocks // 3
    for t in range(3):
        lax.fori_loop(t * split, (t + 1) * split if t < 2 else blocks, attend, 0)
        serve(2 if t == 1 else 1)

    tile = 32
    other_half = pl.ds((1 - core) * half, half)
    swap = remote(part.at[other_half], first, core_send, core_recv, (me, partner))
    swap.wait()

    def add_first(i, carry):
        r = pl.ds(pl.multiple_of(i * tile, tile), tile)
        o = pl.ds(pl.multiple_of(core * half + i * tile, tile), tile)
        first[r, :] = (part[o, :].astype(F32) + first[r, :].astype(F32)).astype(BF16)
        return carry

    lax.fori_loop(0, half // tile, add_first, 0)
    copies = []
    for j in range(1, ny):
        to = lax.rem(y + j, ny)
        copies.append(remote(
            first.at[pl.ds(to * piece, piece)], second.at[j - 1], y_send.at[j - 1], y_recv.at[j - 1], (me, to * 2 + core)
        ))
    serve(2)
    for c in copies:
        c.wait()

    def add_second(i, carry):
        r = pl.ds(pl.multiple_of(i * tile, tile), tile)
        s = first[pl.ds(pl.multiple_of(y * piece + i * tile, tile), tile), :].astype(F32)
        for j in range(ny - 1):
            s = s + second[j, r, :].astype(F32)
        o = pl.ds(pl.multiple_of(core * half + y * piece + i * tile, tile), tile)
        mixed[o, :] = (res[r, :].astype(F32) + s).astype(BF16)
        return carry

    lax.fori_loop(0, piece // tile, add_second, 0)
    mine = mixed.at[pl.ds(core * half + y * piece, piece)]
    copies = []
    for j in range(1, ny):
        to = lax.rem(y + j, ny)
        copies.append(remote(mine, mine, back_send.at[j - 1], back_recv.at[j - 1], (me, to * 2 + core)))
    serve(2)
    for j, c in enumerate(copies):
        c.wait_send()
        frm = lax.rem(y + ny - (j + 1), ny)
        theirs = mixed.at[pl.ds(core * half + frm * piece, piece)]
        pltpu.make_async_remote_copy(
            src_ref=theirs, dst_ref=theirs, send_sem=back_send.at[j], recv_sem=back_recv.at[j],
            device_id=(me, partner), device_id_type=MESH,
        ).wait_recv()
    own_half = mixed.at[pl.ds(core * half, half)]
    swap = remote(own_half, own_half, pair_send, pair_recv, (me, partner))
    swap.wait_send()
    their_half = mixed.at[other_half]
    pltpu.make_async_remote_copy(
        src_ref=their_half, dst_ref=their_half, send_sem=pair_send, recv_sem=pair_recv,
        device_id=(me, partner), device_id_type=MESH,
    ).wait_recv()

    def normalise(i, carry):
        r = pl.ds(pl.multiple_of(i * tile, tile), tile)
        m = mixed[r, :].astype(F32)
        mean_sq = jnp.mean(m * m, axis=1, keepdims=True)
        normed[r, :] = (m * lax.rsqrt(mean_sq + EPS) * gain_ref[...]).astype(BF16)
        return carry

    lax.fori_loop(0, rows // tile, normalise, 0)

    serve(2 * (n - 1) - done[0])
    big = rows // 3

    def project(t, which, dst):
        r = slice(t * big, (t + 1) * big)
        dst[r, :] = jnp.dot(normed[r, :], up[which], preferred_element_type=F32).astype(BF16)

    for t in range(3):
        project(t, 0, value)
        serve(1)
    tail = remote(value.at[pl.ds(rows - RIM, RIM)], rim.at[0], rim_send.at[0], rim_recv.at[0], (right, tp))
    head = remote(value.at[pl.ds(0, RIM)], rim.at[1], rim_send.at[1], rim_recv.at[1], (left, tp))
    for t in range(3):
        project(t, 1, gate)
        serve(1)
    tail.wait()
    head.wait()

    taps = taps_ref[...].astype(F32)
    step = 64
    before = rim[0, RIM - 1:RIM, :].astype(F32)

    def label(i, shift):
        return lc[WINDOW + i * step + shift:WINDOW + (i + 1) * step + shift, 0:1]

    for i in range(rows // step):
        r = slice(i * step, (i + 1) * step)
        x = value[r, :].astype(F32)
        after = (value[(i + 1) * step:(i + 1) * step + RIM, :] if (i + 1) * step < rows else rim[1, :, :])[0:1].astype(F32)
        prev = jnp.concatenate([before, x[:-1]], axis=0)
        nxt = jnp.concatenate([x[1:], after], axis=0)
        conv = (
            taps[0:1] * jnp.where(label(i, -1) == label(i, 0), prev, 0.0)
            + taps[1:2] * x
            + taps[2:3] * jnp.where(label(i, 1) == label(i, 0), nxt, 0.0)
        )
        gate[r, :] = (conv * jax.nn.sigmoid(conv) * gate[r, :].astype(F32)).astype(BF16)
        before = x[step - 1:step]
        if i % 3 == 2:
            serve(1)

    per_tp = n // ntp
    mine_rows = pl.ds(core * half, half)
    partner_rows = pl.ds((1 - core) * half, half)
    units = []
    for d in range(n):
        if d in (1, n - 1) and n > 2:
            units.append((2 * (n - 1) + 2 * (n - d), d, 0, 1))
            units.append((2 * (n - 1) + 2 * d, d, 1, 1))
        else:
            units.append((2 * (n - 1) + (2 * max(d, n - d) if d else 0), d, 0, 2))
    units.sort()

    def target(owner):
        to = owner // per_tp
        local = lax.rem(owner, per_tp)
        slot = lax.rem(tp - to + ntp, ntp) - 1
        return to, local, slot

    def lower(u):
        _, d, way, count = units[u]
        owner = place(lax.rem(pos + d, n))
        w = down[pl.ds(pl.multiple_of(owner * block + way * depth, depth), count * depth), :]

        def body(i, carry):
            r = pl.ds(pl.multiple_of(i * big, big), big)
            product = lax.dot_general(
                gate[r, :], w, (((1,), (1,)), ((), ())), preferred_element_type=F32
            ).astype(BF16)
            for j in range(count):
                pd[owner, way + j, r, :] = product[:, j * depth:(j + 1) * depth]
            return carry

        lax.fori_loop(0, 3, body, 0)
        return remote(
            pd.at[owner, pl.ds(way, count), partner_rows], box.at[owner, pl.ds(way, count)],
            down_send.at[u], down_recv.at[u], (me, partner),
        )

    def reduce(u, c):
        _, d, way, count = units[u]
        owner = place(lax.rem(pos + d, n))
        c.wait()

        def merge(i, carry):
            r = pl.ds(pl.multiple_of(i * tile, tile), tile)
            o = pl.ds(pl.multiple_of(core * half + i * tile, tile), tile)
            for j in range(way, way + count):
                pd[owner, j, o, :] = (pd[owner, j, o, :].astype(F32) + box[owner, j, r, :].astype(F32)).astype(BF16)
            return carry

        lax.fori_loop(0, half // tile, merge, 0, unroll=2)
        to, local, slot = target(owner)

        @pl.when(to != tp)
        def _():
            remote(
                pd.at[owner, pl.ds(way, count), mine_rows], inbox.at[local, slot, pl.ds(way, count)],
                out_send.at[u], out_recv.at[local, slot], (me, to),
            )

    waiting = None
    for u in range(len(units)):
        serve(units[u][0] - done[0])
        c = lower(u)
        if waiting is not None:
            reduce(*waiting)
        waiting = (u, c)
    reduce(*waiting)
    serve(len(queue))

    span = per_tp * block
    for local in range(per_tp):
        owner = tp * per_tp + local
        for slot in range(ntp - 1):
            ref = inbox.at[local, slot]
            pltpu.make_async_remote_copy(
                src_ref=ref, dst_ref=ref, send_sem=out_send.at[0], recv_sem=out_recv.at[local, slot],
                device_id=(me, partner), device_id_type=MESH,
            ).wait_recv()
        for same in range(2):
            base = (core if same else 1 - core) * half
            slots = range(1, ntp - 1, 2) if same else range(0, ntp - 1, 2)

            def finish(i, carry):
                r = pl.ds(pl.multiple_of(i * tile, tile), tile)
                o = pl.ds(pl.multiple_of(base + i * tile, tile), tile)
                kept = mixed[o, pl.ds(pl.multiple_of(tp * span, span), span)]
                for j in range(2):
                    s = sum(inbox[local, slot, j, r, :].astype(F32) for slot in slots)
                    if same:
                        s = s + pd[owner, j, o, :].astype(F32)
                    cols = slice(local * block + j * depth, local * block + (j + 1) * depth)
                    out_ref[o, cols] = (kept[:, cols].astype(F32) + s).astype(BF16)
                return carry

            lax.fori_loop(0, half // tile, finish, 0)
    for u, (_, d, way, count) in enumerate(units):
        owner = place(lax.rem(pos + d, n))
        to, local, slot = target(owner)

        @pl.when(to != tp)
        def _():
            ref = pd.at[owner, pl.ds(way, count), mine_rows]
            pltpu.make_async_remote_copy(
                src_ref=ref, dst_ref=ref, send_sem=out_send.at[u], recv_sem=out_recv.at[0, 0],
                device_id=(me, to), device_id_type=MESH,
            ).wait_send()
    for stream in range(4):
        for way in range(2):
            for s in range(n - 1):
                ring(stream, way, s, False).wait_send()


def paired_kernel(
    n, ntp,
    q_hbm, k_ref, v_ref, sink_ref, lab_row_ref,
    res_hbm, wout_hbm, gain_ref, wv_hbm, wg_hbm, taps_ref, wd_hbm,
    out_hbm,
    w3, other, passing, kx, vx, lx, lp, lc, same, part, first, second, mixed, normed, value, gate,
    pd, box, yin1, zin1, zin2, yin2, res, q_ref, wout_ref, kept, result,
    loc_sem, halo_send, halo_recv, lab_send, lab_recv, zs, zr, xs, xr,
    core_send, core_recv, y_send, y_recv, ag_send, ag_recv, rim_send, rim_recv,
    box_send, box_recv, yo1_send, yo1_recv, zo1_send, zo1_recv, zo2_send, zo2_recv, yo2_send, yo2_recv, out_sem,
):
    me = lax.axis_index("sp")
    tp = lax.axis_index("tp")
    core = lax.rem(tp, 2)
    y = tp // 2
    z = me // 2
    x = lax.rem(me, 2)
    zh = z // 2
    own = lax.rem(z, 2)
    pair = 1 - own
    zp = 2 * zh + pair
    far_mid = 2 - zh
    far_end = 3 - 3 * zh
    partner = y * 2 + 1 - core
    across = (1 - y) * 2 + core
    beside = (zp * 2 + x, tp)
    sibling = (z * 2 + 1 - x, tp)
    rows, cols = q_hbm.shape
    half = rows // 2
    piece = half // 2
    block, hidden = wv_hbm.shape
    wide = w3.shape[2]
    narrow = hidden - wide
    model = wout_hbm.shape[1]
    span = out_hbm.shape[1]
    is_mid = (z == 1) | (z == 2)
    is_end = (z == 0) | (z == 3)
    is_wide = is_mid
    is_narrow = is_end
    roles = ((is_narrow, narrow, wide, 0, narrow), (is_wide, wide, narrow, narrow, 0))
    sides = (is_end, is_mid)

    def copy(src, dst, send, recv, where):
        return pltpu.make_async_remote_copy(
            src_ref=src, dst_ref=dst, send_sem=send, recv_sem=recv, device_id=where, device_id_type=MESH
        )

    def arrive(ref, recv):
        copy(ref, ref, core_send.at[0], recv, (me, partner)).wait_recv()

    def left(ref, send):
        copy(ref, ref, send, core_recv.at[0], (me, partner)).wait_send()

    def spot(s, zo, xo, width):
        return w3.at[s, pl.ds(pl.multiple_of((zo * 2 + xo) * block, block), block), pl.ds(0, width)]

    sources = (wv_hbm, wg_hbm, wd_hbm)

    def loads(s):
        for cond, width, rest, at, rest_at in roles:
            def pair_of():
                a = pltpu.make_async_copy(sources[s].at[:, pl.ds(at, width)], spot(s, z, x, width), loc_sem.at[s, 0])
                b = pltpu.make_async_copy(
                    sources[s].at[:, pl.ds(rest_at, rest)], other.at[s, :, pl.ds(0, rest)], loc_sem.at[s, 1]
                )
                return a, b
            yield cond, pair_of

    for s in range(3):
        for cond, pair_of in loads(s):
            @pl.when(cond)
            def _():
                for c in pair_of():
                    c.start()
    my_piece = core * half + y * piece
    res_load = pltpu.make_async_copy(res_hbm.at[pl.ds(pl.multiple_of(my_piece, piece), piece)], res, loc_sem.at[3, 0])
    res_load.start()
    late_loads = (
        pltpu.make_async_copy(q_hbm, q_ref, loc_sem.at[4, 0]),
        pltpu.make_async_copy(wout_hbm, wout_ref, loc_sem.at[4, 1]),
    )
    for c in late_loads:
        c.start()

    barrier = pltpu.get_barrier_semaphore()
    peers = [(lax.rem(me + j, n), tp) for j in range(1, n)] + [(me, lax.rem(tp + j, ntp)) for j in range(1, ntp)]
    for peer in peers:
        pl.semaphore_signal(barrier, inc=1, device_id=peer, device_id_type=MESH)

    def loaded(s):
        for cond, pair_of in loads(s):
            @pl.when(cond)
            def _():
                for c in pair_of():
                    c.wait()

    loaded(0)
    pl.semaphore_wait(barrier, len(peers))

    def begin_end(s):
        for cond, width, rest, _, _ in roles:
            @pl.when(is_end & cond)
            def _():
                b = other.at[s, :, pl.ds(0, rest)]
                copy(b, spot(s, z, x, rest), zs.at[s, 0], zr.at[s, 0], beside).start()

    def far_end_sends(s):
        for cond, width, rest, _, _ in roles:
            @pl.when(is_end & cond)
            def _():
                a = spot(s, z, x, width)
                copy(a, a, zs.at[s, 1], zr.at[s, 2], ((3 - z) * 2 + x, tp)).start()

    def far_mid_sends(s):
        for cond, width, rest, _, _ in roles:
            @pl.when(is_mid & cond)
            def _():
                b = other.at[s, :, pl.ds(0, rest)]
                copy(b, spot(s, z, x, rest), zs.at[s, 2], zr.at[s, 1], ((3 - zp) * 2 + x, tp)).start()

    def begin_mid(s):
        for cond, width, rest, _, _ in roles:
            @pl.when(is_mid & cond)
            def _():
                a = spot(s, z, x, width)
                copy(a, a, zs.at[s, 1], zr.at[s, 1], ((3 - z) * 2 + x, tp)).start()

    def begin_out(s):
        for cond, width, rest, _, _ in roles:
            @pl.when(is_mid & cond)
            def _():
                b = other.at[s, :, pl.ds(0, rest)]
                copy(b, spot(s, z, x, rest), zs.at[s, 0], zr.at[s, 0], beside).start()

    def begin_x(s, who=(0, 1)):
        for (cond, width, _, _, _), side in ((r, sides[w]) for r in roles for w in who):
            @pl.when(cond & side)
            def _():
                a = spot(s, z, x, width)
                copy(a, a, xs.at[s, 0], xr.at[s, 0], sibling).start()

    def pass_on(first):
        for cond, width, rest, _, _ in roles:
            @pl.when(is_end & cond)
            def _():
                b = other.at[2, :, pl.ds(0, rest)]
                held = passing.at[:, pl.ds(0, rest)]
                if first:
                    copy(b, held, xs.at[2, 4], xr.at[2, 4], sibling).start()
                else:
                    arrive(held, xr.at[2, 4])
                    copy(held, spot(2, z, 1 - x, rest), zs.at[2, 4], zr.at[2, 3], beside).start()

    owners = (zp, far_mid, far_end)

    def event(s, j, who=(0, 1)):
        for side in who:
            for cond, width, _, _, _ in roles:
                @pl.when(sides[side] & cond)
                def _():
                    a = spot(s, owners[j], x, width)
                    arrive(a, zr.at[s, j])
                    if side == 1 and j == 0:
                        copy(a, a, zs.at[s, 3], zr.at[s, 2], ((3 - z) * 2 + x, tp)).start()
                    if (s, j, side) != (2, 0, 1):
                        copy(a, a, xs.at[s, j + 1], xr.at[s, j + 1], sibling).start()

    def xwait(s, j):
        for side in range(2):
            for cond, width, _, _, _ in roles:
                @pl.when(sides[side] & cond)
                def _():
                    where = spot(s, ((z,) + owners)[j], 1 - x, width)
                    arrive(where, zr.at[2, 3] if (s, j, side) == (2, 1, 1) else xr.at[s, j])

    def finish_stream(s):
        for cond, width, rest, _, _ in roles:
            @pl.when(cond)
            def _():
                left(spot(s, z, x, rest), zs.at[s, 0])
                left(spot(s, z, x, width), zs.at[s, 1])
                for j in range(4):
                    if (s, j) != (2, 1):
                        left(spot(s, z, x, width), xs.at[s, j])

            if s == 2:
                @pl.when(is_end & cond)
                def _():
                    left(spot(s, z, x, width), xs.at[2, 1])
                    left(spot(s, z, x, rest), xs.at[2, 4])
                    left(spot(s, z, x, rest), zs.at[2, 4])

            @pl.when(is_mid & cond)
            def _():
                left(spot(s, z, x, rest), zs.at[s, 2])
                left(spot(s, z, x, width), zs.at[s, 3])

    right, before = lax.rem(me + 1, n), lax.rem(me + n - 1, n)
    ends = pl.ds(rows - WINDOW, WINDOW)
    starts = pl.ds(0, WINDOW)
    low, high = pl.ds(0, WINDOW), pl.ds(rows + WINDOW, WINDOW)
    halo = []
    for i, (src, dst) in enumerate(((k_ref, kx), (v_ref, vx))):
        halo.append(copy(src.at[ends], dst.at[low], halo_send.at[i, 0], halo_recv.at[i, 0], (right, tp)))
        halo.append(copy(src.at[starts], dst.at[high], halo_send.at[i, 1], halo_recv.at[i, 1], (before, tp)))
    halo.append(copy(lab_row_ref.at[:, ends], lx.at[:, low], halo_send.at[2, 0], halo_recv.at[2, 0], (right, tp)))
    halo.append(copy(lab_row_ref.at[:, starts], lx.at[:, high], halo_send.at[2, 1], halo_recv.at[2, 1], (before, tp)))
    for c in halo:
        c.start()
    begin_end(0)
    begin_mid(0)
    begin_out(0)
    far_end_sends(0)
    far_mid_sends(0)
    begin_x(0)
    loaded(1)
    begin_end(1)
    begin_x(1)
    loaded(2)
    begin_x(2, (0,))
    pass_on(True)

    @pl.when(is_narrow)
    def _():
        if narrow < wide:
            w3[:, :, narrow:wide] = jnp.zeros((3, n * block, wide - narrow), BF16)

    inner = pl.ds(WINDOW, rows)
    kx[inner, :] = k_ref[...]
    vx[inner, :] = v_ref[...]
    lx[:, inner] = lab_row_ref[...]
    lab_copy = copy(lx, lp, lab_send, lab_recv, beside)
    chunks = rows // WINDOW

    def columns(row_ref, which):
        for i in which:
            chunk = slice(i * WINDOW, (i + 1) * WINDOW)
            square = jnp.broadcast_to(row_ref[0:1, chunk].astype(F32), (WINDOW, WINDOW))
            lc[chunk, :] = jnp.transpose(square)

    def neighbours(slot):
        for i in range(chunks):
            here = lc[WINDOW * (i + 1):WINDOW * (i + 2), :]
            for side, shift in ((0, -1), (1, 1)):
                there = lc[WINDOW * (i + 1) + shift:WINDOW * (i + 2) + shift, :]
                same[slot, side, i * WINDOW:(i + 1) * WINDOW, :] = jnp.where(here == there, 1.0, 0.0)

    columns(lx, range(1, chunks + 1))

    def edges():
        for c in halo:
            c.wait()
        lx[:, low] = jnp.where(me == 0, -1, lx[:, low])
        lx[:, high] = jnp.where(me == n - 1, -1, lx[:, high])
        lab_copy.start()
        columns(lx, (0, chunks + 1))
        neighbours(own)

    kv_local = k_ref.shape[1] // HEAD_DIM
    per_kv = cols // k_ref.shape[1]
    per_half = chunks // 2
    tile = 32

    def attend(i, carry):
        own_half = i // per_half
        j = lax.rem(i, per_half)
        flip = (1 - own_half) * core + own_half * (1 - y)
        turn = flip * (per_half - 1 - j) + (1 - flip) * j
        b = ((1 - own_half) * (1 - core) + own_half * core) * per_half + turn
        here = pl.ds(pl.multiple_of(b * WINDOW, WINDOW), WINDOW)
        wide_keys = pl.ds(pl.multiple_of(b * WINDOW, WINDOW), 3 * WINDOW)
        q = q_ref[here, :] * jnp.asarray(HEAD_DIM ** (-0.5), BF16)
        kw = kx[wide_keys, :]
        vw = vx[wide_keys, :]
        lab_k = lx[0:1, wide_keys].astype(F32)
        lab_q = lc[pl.ds(pl.multiple_of(b * WINDOW + WINDOW, WINDOW), WINDOW), 0:1]
        key = lax.broadcasted_iota(jnp.int32, (WINDOW, 3 * WINDOW), 1) - WINDOW
        query = lax.broadcasted_iota(jnp.int32, (WINDOW, 3 * WINDOW), 0)
        allowed = (jnp.abs(key - query) <= WINDOW) & (lab_q == lab_k)
        results = []
        for g in range(kv_local):
            k = kw[:, g * HEAD_DIM:(g + 1) * HEAD_DIM]
            v = vw[:, g * HEAD_DIM:(g + 1) * HEAD_DIM]
            heads = range(g * per_kv, (g + 1) * per_kv)
            stacked = jnp.concatenate([q[:, h * HEAD_DIM:(h + 1) * HEAD_DIM] for h in heads], axis=0)
            scores = lax.dot_general(stacked, k, (((1,), (1,)), ((), ())), preferred_element_type=F32)
            raws, scales = [], []
            for u, h in enumerate(heads):
                score = jnp.where(allowed, scores[u * WINDOW:(u + 1) * WINDOW], NEG)
                sink = sink_ref[h]
                highest = jnp.maximum(jnp.max(score, axis=1, keepdims=True), sink)
                raw = jnp.exp(score - highest)
                scales.append(1.0 / (jnp.sum(raw, axis=1, keepdims=True) + jnp.exp(sink - highest)))
                raws.append(raw.astype(BF16))
            summed = jnp.dot(jnp.concatenate(raws, axis=0), v, preferred_element_type=F32)
            for u in range(per_kv):
                results.append((summed[u * WINDOW:(u + 1) * WINDOW] * scales[u]).astype(BF16))
        attended = jnp.concatenate(results, axis=1)
        part[here, :] = jnp.dot(attended, wout_ref[...], preferred_element_type=F32).astype(BF16)
        mine = first.at[pl.ds(pl.multiple_of(turn * WINDOW, WINDOW), WINDOW)]

        @pl.when(own_half == 0)
        def _():
            copy(part.at[here], mine, core_send.at[turn], core_recv.at[turn], (me, partner)).start()

        @pl.when(own_half == 1)
        def _():
            arrive(mine, core_recv.at[turn])

            def add(t, carry):
                r = pl.ds(pl.multiple_of(turn * WINDOW + t * tile, tile), tile)
                o = pl.ds(pl.multiple_of(b * WINDOW + t * tile, tile), tile)
                first[r, :] = (part[o, :].astype(F32) + first[r, :].astype(F32)).astype(BF16)
                return carry

            lax.fori_loop(0, WINDOW // tile, add, 0)

        @pl.when(i == per_half)
        def _():
            y_copy(0, y).start()

        @pl.when(i == per_half + 1)
        def _():
            y_copy(1, y).start()

        @pl.when(i == 1)
        def _():
            edges()

        @pl.when(i == 3)
        def _():
            event(0, 0, (1,))
            begin_mid(1)
            begin_out(1)
            far_mid_sends(1)

        @pl.when(i == 4)
        def _():
            event(0, 1, (1,))

        return carry

    def y_copy(k, yy):
        if k == 0:
            count, src, dst = 2 * piece // 3, (1 - yy) * (half - 2 * piece // 3), (1 - yy) * (piece // 3)
        else:
            count, src, dst = piece // 3, 2 * piece // 3 + (1 - yy) * (piece // 3), yy * (2 * piece // 3)
        return copy(
            first.at[pl.ds(pl.multiple_of(src, 64), count)], second.at[pl.ds(pl.multiple_of(dst, 64), count)],
            y_send.at[k], y_recv.at[k], (me, across),
        )

    res_load.wait()
    for c in late_loads:
        c.wait()
    lax.fori_loop(0, 2 * per_half, attend, 0)
    for k in range(2):
        y_copy(k, 1 - y).wait_recv()

    def norm(slot, start, count):
        def body(i, carry):
            r = pl.ds(pl.multiple_of(start + i * tile, tile), tile)
            m = mixed[r, :].astype(F32)
            mean_sq = jnp.mean(m * m, axis=1, keepdims=True)
            normed[slot, r, :] = (m * lax.rsqrt(mean_sq + EPS) * gain_ref[...]).astype(BF16)
            return carry

        lax.fori_loop(0, count // tile, body, 0)

    def add_second(i, carry):
        r = pl.ds(pl.multiple_of(i * tile, tile), tile)
        f = pl.ds(pl.multiple_of(y * piece + i * tile, tile), tile)
        o = pl.ds(pl.multiple_of(my_piece + i * tile, tile), tile)
        s = first[f, :].astype(F32) + second[r, :].astype(F32)
        mixed[o, :] = (res[r, :].astype(F32) + s).astype(BF16)
        return carry

    lax.fori_loop(0, piece // tile, add_second, 0)

    def part_of(c, yy):
        return c * half + yy * piece

    def mixed_at(c, yy):
        return mixed.at[pl.ds(pl.multiple_of(part_of(c, yy), piece), piece)]

    bit = piece // 2

    def normed_at(slot, c, yy, b):
        return normed.at[slot, pl.ds(pl.multiple_of(part_of(c, yy) + b * bit, bit), bit)]

    def share(k, ref, where):
        copy(ref, ref, ag_send.at[k], ag_recv.at[k], where).start()

    share(0, mixed_at(core, y), (me, across))
    share(1, mixed_at(core, y), (me, partner))
    norm(own, my_piece, piece)
    for b in range(2):
        share(4 + b, normed_at(own, core, y, b), beside)
    event(0, 0, (0,))
    event(1, 0, (1,))
    event(0, 1, (0,))
    arrive(mixed_at(1 - core, y), ag_recv.at[1])
    norm(own, part_of(1 - core, y), piece)
    event(0, 2, (1,))
    arrive(mixed_at(core, 1 - y), ag_recv.at[0])
    share(2, mixed_at(core, 1 - y), (me, partner))
    norm(own, part_of(core, 1 - y), piece)
    event(0, 2, (0,))

    def serve_spread(b):
        arrive(normed_at(pair, core, y, b), ag_recv.at[4 + b])
        share(6 + b, normed_at(pair, core, y, b), (me, across))
        share(8 + b, normed_at(pair, core, y, b), (me, partner))

    event(1, 0, (0,))
    event(1, 1, (0,))
    serve_spread(0)
    far_end_sends(1)
    serve_spread(1)
    event(1, 1, (1,))
    begin_end(2)
    pass_on(False)
    arrive(mixed_at(1 - core, 1 - y), ag_recv.at[2])
    norm(own, part_of(1 - core, 1 - y), piece)

    big = rows // 2

    def project(which, slot):
        def body(t, carry):
            r = pl.ds(pl.multiple_of(t * big, big), big)
            product = jnp.dot(normed[slot, r, :], w3[which], preferred_element_type=F32).astype(BF16)
            if which == 0:
                value[slot, pl.ds(pl.multiple_of(RIM + t * big, RIM), big), :] = product
            else:
                gate[slot, r, :] = product
            return carry

        lax.fori_loop(0, 2, body, 0)

    inside = pl.ds(RIM, RIM)
    last = pl.ds(rows, RIM)
    fronts, backs = pl.ds(0, RIM), pl.ds(RIM + rows, RIM)
    facing = ((3 - z) * 2 + 1 - x, tp)
    near_rims = (
        (x == 0, ((0, last, 0, 0), (1, inside, 0, 1), (1, last, 1, 0))),
        (x == 1, ((0, inside, 0, 1), (0, last, 1, 0), (1, inside, 1, 1))),
    )
    far_rims = (((x == 0) & (zh == 1), (0, inside, 1, 1)), ((x == 1) & (zh == 0), (1, last, 0, 0)))

    def rim_copy(frm, source, to, side, where):
        target = value.at[to, (fronts, backs)[side]]
        pad = 2 * to + side
        copy(value.at[frm, source], target, rim_send.at[pad], rim_recv.at[pad], where).start()

    def send_far_rims(side):
        for cond, spec in far_rims:
            @pl.when(cond & side)
            def _():
                rim_copy(*spec, facing)

    mine = mixed.at[:, pl.ds(pl.multiple_of(tp * span, span), span)]
    kept_copy = pltpu.make_async_copy(mine, kept, loc_sem.at[3, 1])
    kept_copy.start()

    def serve_x(s):
        for j in range(4):
            xwait(s, j)

    serve_x(0)
    project(0, own)
    send_far_rims(is_mid)
    begin_mid(2)
    begin_out(2)
    far_mid_sends(2)
    event(1, 2)

    def serve_diagonal(b):
        arrive(normed_at(pair, core, 1 - y, b), ag_recv.at[6 + b])
        share(10 + b, normed_at(pair, core, 1 - y, b), (me, partner))

    def serve_rest(b):
        arrive(normed_at(pair, 1 - core, y, b), ag_recv.at[8 + b])
        arrive(normed_at(pair, 1 - core, 1 - y, b), ag_recv.at[10 + b])

    serve_diagonal(0)
    serve_diagonal(1)
    serve_rest(0)
    serve_rest(1)
    project(0, pair)

    send_far_rims(is_end)
    for cond, specs in near_rims:
        @pl.when(cond)
        def _():
            for spec in specs:
                rim_copy(*spec, sibling)

    far_end_sends(2)
    begin_x(2, (1,))
    event(2, 0, (0,))
    serve_x(1)
    project(1, own)
    event(2, 0, (1,))
    project(1, pair)
    event(2, 1, (1,))
    lab_copy.wait()
    columns(lp, range(chunks + 2))
    neighbours(pair)

    def serve_rims(slot):
        for side, rd in enumerate((fronts, backs)):
            if slot == side:
                @pl.when((x != side) | (zh != side))
                def _():
                    arrive(value.at[slot, rd], rim_recv.at[2 * slot + side])

                @pl.when((x == side) & (zh == side))
                def _():
                    value[slot, rd, :] = jnp.zeros((RIM, wide), BF16)
            else:
                arrive(value.at[slot, rd], rim_recv.at[2 * slot + side])

    serve_rims(0)
    serve_rims(1)

    taps_all = taps_ref[...].astype(F32)
    taps = jnp.where(is_wide, taps_all[:, narrow:], taps_all[:, :wide])
    step = 64
    lanes = wide // WINDOW

    for slot in range(2):
        def gated(i, carry):
            base = i * step
            r = pl.ds(pl.multiple_of(base, step), step)
            x_rows = value[slot, pl.ds(pl.multiple_of(RIM + base, RIM), step), :].astype(F32)
            above = value[slot, pl.ds(pl.multiple_of(base, RIM), RIM), :].astype(F32)[RIM - 1:RIM]
            below = value[slot, pl.ds(pl.multiple_of(RIM + base + step, RIM), RIM), :].astype(F32)[0:1]
            prev = jnp.concatenate([above, x_rows[:-1]], axis=0)
            nxt = jnp.concatenate([x_rows[1:], below], axis=0)
            with_prev = jnp.concatenate([same[slot, 0, r, :]] * lanes, axis=1) > 0.5
            with_next = jnp.concatenate([same[slot, 1, r, :]] * lanes, axis=1) > 0.5
            conv = (
                taps[0:1] * jnp.where(with_prev, prev, 0.0)
                + taps[1:2] * x_rows
                + taps[2:3] * jnp.where(with_next, nxt, 0.0)
            )
            gate[slot, r, :] = (conv * jax.nn.sigmoid(conv) * gate[slot, r, :].astype(F32)).astype(BF16)
            return carry

        lax.fori_loop(0, rows // step, gated, 0)

    order = (z, zp, far_mid, far_end)
    quarter = rows // 2

    def boxed(u, k):
        slot = (pair, own)[k]
        return copy(pd.at[u, slot], box.at[u // 2, slot], box_send.at[u, k], box_recv.at[u // 2, k], (me, partner))

    def lower(u):
        t = order[u]
        w = w3[2, pl.ds(pl.multiple_of(t * span, span), span), :]
        for k, slot in enumerate((pair, own)):
            def body(i, carry):
                r = pl.ds(pl.multiple_of(i * rows, rows), rows)
                pd[u, slot, r, :] = lax.dot_general(
                    gate[slot, r, :], w, (((1,), (1,)), ((), ())), preferred_element_type=F32
                ).astype(BF16)
                return carry

            lax.fori_loop(0, 1, body, 0)

            @pl.when(core != lax.rem(t, 2))
            def _():
                boxed(u, k).start()

    cuts = (rows // 6 * 3, rows // 6 * 3, rows // 6 * 3, rows // 6 * 2)

    def segment(u, g):
        count = (rows - cuts[u]) // 2
        return cuts[u] + g * count, count

    slab = rows // 12

    def accumulate(ref, slot, at, count, other_ref, base):
        def body(i, carry):
            r = pl.ds(pl.multiple_of(at + i * slab, slab), slab)
            o = pl.ds(pl.multiple_of(base + i * slab, slab), slab)
            ref[slot, r, :] = (ref[slot, r, :].astype(F32) + other_ref[o, :].astype(F32)).astype(BF16)
            return carry

        lax.fori_loop(0, count // slab, body, 0)

    def z_first(u, g):
        at, count = segment(u, g)
        return copy(
            pd.at[u, pair, pl.ds(at, count)], zin1.at[u // 2, g, pl.ds(0, count)],
            zo1_send.at[u // 2, g], zo1_recv.at[u // 2, g], beside,
        )

    def then_y(u, g):
        at, count = segment(u, g)
        return copy(
            pd.at[u, own, pl.ds(at, count)], yin2.at[g, pl.ds(0, count)], yo2_send.at[g], yo2_recv.at[g], (me, across)
        )

    def y_first(u, slot, k):
        top = pl.ds(0, cuts[u])
        return copy(pd.at[u, slot, top], yin1.at[slot, top], yo1_send.at[k], yo1_recv.at[k], (me, across))

    def then_z(u):
        top = pl.ds(0, cuts[u])
        return copy(pd.at[u, pair, top], zin2.at[top], zo2_send, zo2_recv, beside)

    def stage_one(u):
        t = order[u]

        @pl.when(core == lax.rem(t, 2))
        def _():

            def add(slot, at, count):
                accumulate(pd.at[u], slot, at, count, box.at[u // 2, slot], at)

            arrive(box.at[u // 2, pair], box_recv.at[u // 2, 0])
            if u < 3:
                add(pair, 0, cuts[u])

                @pl.when(y != t // 2)
                def _():
                    y_first(u, pair, 0).start()

            for g in range(2):
                add(pair, *segment(u, g))
                z_first(u, g).start()
            if u == 3:
                add(pair, 0, cuts[u])

                @pl.when(y != t // 2)
                def _():
                    y_first(u, pair, 0).start()

            arrive(box.at[u // 2, own], box_recv.at[u // 2, 1])
            add(own, 0, cuts[u])

            @pl.when(y != t // 2)
            def _():
                y_first(u, own, 1).start()

            for g in range(2):
                add(own, *segment(u, g))

    def stage_y(u):
        t = order[u]

        @pl.when(tp == t)
        def _():
            top = pl.ds(0, cuts[u])
            arrive(yin1.at[pair, top], yo1_recv.at[0])
            accumulate(pd.at[u], pair, 0, cuts[u], yin1.at[pair], 0)
            then_z(u).start()
            arrive(yin1.at[own, top], yo1_recv.at[1])
            accumulate(pd.at[u], own, 0, cuts[u], yin1.at[own], 0)

    def stage_z(u):
        t = order[u]

        @pl.when(core == lax.rem(t, 2))
        def _():
            for g in range(2):
                at, count = segment(u, g)
                arrive(zin1.at[u // 2, g, pl.ds(0, count)], zo1_recv.at[u // 2, g])
                accumulate(pd.at[u], own, at, count, zin1.at[u // 2, g], 0)

                @pl.when(y != t // 2)
                def _():
                    then_y(u, g).start()

    def put(at, count, k):
        r = pl.ds(at, count)
        return pltpu.make_async_copy(result.at[r], out_hbm.at[r], out_sem.at[k])

    def stage_three(u):
        t = order[u]

        @pl.when(tp == t)
        def _():
            def close(at, count, extra, k):
                def body(i, carry):
                    r = pl.ds(pl.multiple_of(i * slab, slab), slab)
                    o = pl.ds(pl.multiple_of(at + i * slab, slab), slab)
                    s = pd[u, own, o, :].astype(F32) + extra[r, :].astype(F32)
                    result[o, :] = (kept[o, :].astype(F32) + s).astype(BF16)
                    return carry

                lax.fori_loop(0, count // slab, body, 0)
                put(at, count, k).start()

            arrive(zin2.at[pl.ds(0, cuts[u])], zo2_recv)
            close(0, cuts[u], zin2, 0)
            for g in range(2):
                at, count = segment(u, g)
                arrive(yin2.at[g, pl.ds(0, count)], yo2_recv.at[g])
                close(at, count, yin2.at[g], 1 + g)
            put(0, cuts[u], 0).wait()
            for g in range(2):
                put(*segment(u, g), 1 + g).wait()

    def drain(u):
        t = order[u]

        @pl.when(core != lax.rem(t, 2))
        def _():
            for k in range(2):
                boxed(u, k).wait_send()

        @pl.when(core == lax.rem(t, 2))
        def _():
            for g in range(2):
                z_first(u, g).wait_send()

            @pl.when(y != t // 2)
            def _():
                for k, slot in enumerate((pair, own)):
                    y_first(u, slot, k).wait_send()
                for g in range(2):
                    then_y(u, g).wait_send()

            @pl.when(y == t // 2)
            def _():
                then_z(u).wait_send()

    xwait(2, 0)
    lower(0)
    event(2, 1, (0,))
    stage_one(0)
    xwait(2, 1)
    lower(1)
    stage_one(1)
    event(2, 2)
    xwait(2, 2)
    lower(2)
    stage_one(2)
    xwait(2, 3)
    lower(3)
    stage_one(3)
    stage_z(0)
    stage_z(1)
    stage_y(0)
    stage_y(1)
    stage_z(2)
    stage_z(3)
    stage_y(2)
    stage_y(3)
    kept_copy.wait()
    stage_three(0)
    stage_three(1)
    stage_three(2)
    stage_three(3)

    for s in range(3):
        finish_stream(s)
    for j in range(per_half):
        left(first.at[pl.ds(0, WINDOW)], core_send.at[j])
    for k in range(2):
        y_copy(k, y).wait_send()
    for k in range(3):
        left(mixed_at(core, y), ag_send.at[k])
    for k in range(4, 12):
        left(normed_at(own, core, y, 0), ag_send.at[k])
    for pad in range(4):
        sends = (x == pad // 3) | (zh == pad // 3) if pad in (0, 3) else x >= 0

        @pl.when(sends)
        def _():
            left(value.at[0, fronts], rim_send.at[pad])
    for u in range(4):
        drain(u)


def solution(mesh):
    n, ntp = mesh.shape["sp"], mesh.shape["tp"]

    def by_ring(q, k, v, sink, doc, res, wout, gain, wv, wg, taps, wd):
        rows, model = res.shape
        hidden = wv.shape[1]
        block = wv.shape[0]
        ny = ntp // 2
        labels = doc + 1
        lab_row = labels[None, :]
        vm = pl.BlockSpec(memory_space=pltpu.VMEM)
        hbm = pl.BlockSpec(memory_space=pl.ANY)
        smem = pl.BlockSpec(memory_space=pltpu.SMEM)
        dma = pltpu.SemaphoreType.DMA
        kvc = k.shape[1]
        span = model // ntp
        scratch = [
            pltpu.VMEM((2, n * block, hidden), BF16),
            pltpu.VMEM((n * block, hidden), BF16),
            pltpu.VMEM((rows + 2 * WINDOW, kvc), BF16),
            pltpu.VMEM((rows + 2 * WINDOW, kvc), BF16),
            pltpu.VMEM((1, rows + 2 * WINDOW), jnp.int32),
            pltpu.VMEM((rows + 2 * WINDOW, WINDOW), F32),
            pltpu.VMEM((rows, model), BF16),
            pltpu.VMEM((rows // 2, model), BF16),
            pltpu.VMEM((max(ny - 1, 1), rows // 2 // ny, model), BF16),
            pltpu.VMEM((rows, model), BF16),
            pltpu.VMEM((rows, model), BF16),
            pltpu.VMEM((rows, hidden), BF16),
            pltpu.VMEM((rows, hidden), BF16),
            pltpu.VMEM((2, RIM, hidden), BF16),
            pltpu.VMEM((n, 2, rows, block // 2), BF16),
            pltpu.VMEM((n, 2, rows // 2, block // 2), BF16),
            pltpu.VMEM((n // ntp, ntp - 1, 2, rows // 2, block // 2), BF16),
            pltpu.VMEM((rows // 2 // ny, model), BF16),
            dma((4,)),
            dma((4, 2, n - 1)), dma((4, 2, n - 1)),
            dma((3, 2)), dma((3, 2)),
            dma((2,)), dma((2,)),
            dma, dma,
            dma((ny,)), dma((ny,)),
            dma((ny,)), dma((ny,)),
            dma, dma,
            dma((n + 2,)), dma((n + 2,)),
            dma((n + 2,)), dma((n // ntp, ntp - 1)),
        ]
        return pl.pallas_call(
            functools.partial(ring_kernel, n, ntp),
            out_shape=jax.ShapeDtypeStruct((rows, span), BF16),
            in_specs=[vm, vm, vm, smem, vm, hbm, vm, vm, hbm, hbm, vm, hbm],
            out_specs=vm,
            scratch_shapes=scratch,
            compiler_params=pltpu.CompilerParams(
                collective_id=0, has_side_effects=True, vmem_limit_bytes=67043328
            ),
            name="layer",
        )(q, k, v, sink, lab_row, res, wout, gain[None, :], wv, wg, taps, wd)


    def by_pairs(q, k, v, sink, doc, res, wout, gain, wv, wg, taps, wd):
        rows, model = res.shape
        block, hidden = wv.shape
        half = rows // 2
        piece = half // 2
        span = model // ntp
        kvc = k.shape[1]
        third = rows // 12 * 5
        wide = (hidden // LANES + 1) // 2 * LANES
        lab_row = doc[None, :]
        vm = pl.BlockSpec(memory_space=pltpu.VMEM)
        hbm = pl.BlockSpec(memory_space=pl.ANY)
        smem = pl.BlockSpec(memory_space=pltpu.SMEM)
        dma = pltpu.SemaphoreType.DMA
        scratch = [
            pltpu.VMEM((3, n * block, wide), BF16),
            pltpu.VMEM((3, block, wide), BF16),
            pltpu.VMEM((block, wide), BF16),
            pltpu.VMEM((rows + 2 * WINDOW, kvc), BF16),
            pltpu.VMEM((rows + 2 * WINDOW, kvc), BF16),
            pltpu.VMEM((1, rows + 2 * WINDOW), jnp.int32),
            pltpu.VMEM((1, rows + 2 * WINDOW), jnp.int32),
            pltpu.VMEM((rows + 2 * WINDOW, WINDOW), F32),
            pltpu.VMEM((2, 2, rows, WINDOW), F32),
            pltpu.VMEM((rows, model), BF16),
            pltpu.VMEM((half, model), BF16),
            pltpu.VMEM((piece, model), BF16),
            pltpu.VMEM((rows, model), BF16),
            pltpu.VMEM((2, rows, model), BF16),
            pltpu.VMEM((2, rows + 2 * RIM, wide), BF16),
            pltpu.VMEM((2, rows, wide), BF16),
            pltpu.VMEM((4, 2, rows, span), BF16),
            pltpu.VMEM((2, 2, rows, span), BF16),
            pltpu.VMEM((2, half, span), BF16),
            pltpu.VMEM((2, 2, third, span), BF16),
            pltpu.VMEM((half, span), BF16),
            pltpu.VMEM((2, third, span), BF16),
            pltpu.VMEM((piece, model), BF16),
            pltpu.VMEM(q.shape, BF16),
            pltpu.VMEM(wout.shape, BF16),
            pltpu.VMEM((rows, span), BF16),
            pltpu.VMEM((rows, span), BF16),
            dma((5, 2)),
            dma((3, 2)), dma((3, 2)),
            dma, dma,
            dma((3, 5)), dma((3, 4)),
            dma((3, 5)), dma((3, 5)),
            dma((rows // WINDOW // 2,)), dma((rows // WINDOW // 2,)),
            dma((2,)), dma((2,)),
            dma((12,)), dma((12,)),
            dma((4,)), dma((4,)),
            dma((4, 2)), dma((2, 2)),
            dma((2,)), dma((2,)),
            dma((2, 2)), dma((2, 2)),
            dma, dma,
            dma((2,)), dma((2,)),
            dma((3,)),
        ]
        return pl.pallas_call(
            functools.partial(paired_kernel, n, ntp),
            out_shape=jax.ShapeDtypeStruct((rows, span), BF16),
            in_specs=[hbm, vm, vm, smem, vm, hbm, hbm, vm, hbm, hbm, vm, hbm],
            out_specs=hbm,
            scratch_shapes=scratch,
            compiler_params=pltpu.CompilerParams(
                collective_id=0, has_side_effects=True, vmem_limit_bytes=67043328
            ),
            name="layer",
        )(q, k, v, sink, lab_row, res, wout, gain[None, :], wv, wg, taps, wd)

    placed = (
        P("sp", "tp"), P("sp", "tp"), P("sp", "tp"), P("tp"), P("sp"), P("sp", None),
        P("tp", None), P(), P("sp", "tp"), P("sp", "tp"), P(None, "tp"), P("sp", "tp"),
    )
    return jax.shard_map(
        by_pairs if (n, ntp) == (8, 4) else by_ring, mesh=mesh, in_specs=placed, out_specs=P("sp", "tp"), check_vma=False
    )
```

```python
import functools

import jax
import jax.numpy as jnp
from jax import lax
from jax.experimental import pallas as pl
from jax.experimental.pallas import tpu as pltpu
from jax.sharding import PartitionSpec as P

HEAD_DIM = 64
WINDOW = 128
EPS = 1e-06
NEG = -1e30
RIM = 16
LANES = 128
MESH = pl.DeviceIdType.MESH
F32 = jnp.float32
BF16 = jnp.bfloat16


def ring_kernel(
    n, ntp,
    q_ref, k_ref, v_ref, sink_ref, lab_row_ref,
    res_hbm, wout_ref, gain_ref, wv_hbm, wg_hbm, taps_ref, wd_hbm,
    out_ref,
    up, down, kx, vx, lx, lc, part, first, second, mixed, normed, value, gate, rim, pd, box, inbox, res,
    loc_sem, ring_send, ring_recv, halo_send, halo_recv, rim_send, rim_recv,
    core_send, core_recv, y_send, y_recv, back_send, back_recv, pair_send, pair_recv,
    down_send, down_recv, out_send, out_recv,
):
    me = lax.axis_index("sp")
    tp = lax.axis_index("tp")
    core = lax.rem(tp, 2)
    y = tp // 2
    ny = ntp // 2
    partner = y * 2 + 1 - core
    rows = q_ref.shape[0]
    half = rows // 2
    piece = half // ny
    block = wv_hbm.shape[0]
    depth = block // 2
    quarter = block // 4

    def place(p):
        h = p // (n // 2)
        return (1 - h) * (2 * p) + h * (2 * n - 1 - 2 * p)

    odd = lax.rem(me, 2)
    pos = (1 - odd) * (me // 2) + odd * ((2 * n - 1 - me) // 2)
    ahead = place(lax.rem(pos + 1, n))
    behind = place(lax.rem(pos + n - 1, n))
    right = lax.rem(me + 1, n)
    left = lax.rem(me + n - 1, n)

    loads = []
    for i, (src, dst) in enumerate((
        (wv_hbm, up.at[0, pl.ds(me * block, block)]),
        (wg_hbm, up.at[1, pl.ds(me * block, block)]),
        (wd_hbm, down.at[pl.ds(me * block, block)]),
        (res_hbm.at[pl.ds(core * half + y * piece, piece)], res),
    )):
        c = pltpu.make_async_copy(src, dst, loc_sem.at[i])
        c.start()
        loads.append(c)

    barrier = pltpu.get_barrier_semaphore()
    peers = [(ahead, tp), (behind, tp), (right, tp), (left, tp)]
    for j in range(1, ntp):
        peers.append((me, lax.rem(tp + j, ntp)))
    for peer in peers:
        pl.semaphore_signal(barrier, inc=1, device_id=peer, device_id_type=MESH)
    for c in loads:
        c.wait()
    pl.semaphore_wait(barrier, len(peers))

    def spot(stream, way, owner):
        if stream < 2:
            return up.at[stream, pl.ds(owner * block + way * depth, depth)]
        return down.at[pl.ds(owner * block + way * depth + (stream - 2) * quarter, quarter)]

    def ring(stream, way, s, arriving):
        shift = s + 1 if arriving else s
        owner = place(lax.rem(pos + n - shift, n)) if way == 0 else place(lax.rem(pos + shift, n))
        ref = spot(stream, way, owner)
        return pltpu.make_async_remote_copy(
            src_ref=ref, dst_ref=ref,
            send_sem=ring_send.at[stream, way, s], recv_sem=ring_recv.at[stream, way, s],
            device_id=(ahead if way == 0 else behind, tp), device_id_type=MESH,
        )

    def begin(stream):
        for way in range(2):
            ring(stream, way, 0, False).start()

    def forward(stream, s, last=False):
        for way in range(2):
            ring(stream, way, s, True).wait_recv()
            if not last:
                ring(stream, way, s + 1, False).start()

    queue = []
    for s in range(n - 1):
        for stream in (0, 1):
            queue.append((stream, s))
    for s in range(n - 1):
        for stream in (2, 3):
            queue.append((stream, s))
    done = [0]

    def serve(count):
        for _ in range(count):
            if done[0] == len(queue):
                return
            stream, s = queue[done[0]]
            done[0] += 1
            forward(stream, s, last=s == n - 2)
            if stream < 2 and s == n - 2:
                begin(stream + 2)

    halo = []

    def remote(src, dst, send, recv, where):
        c = pltpu.make_async_remote_copy(
            src_ref=src, dst_ref=dst, send_sem=send, recv_sem=recv, device_id=where, device_id_type=MESH
        )
        c.start()
        return c

    ends = pl.ds(rows - WINDOW, WINDOW)
    starts = pl.ds(0, WINDOW)
    low, high = pl.ds(0, WINDOW), pl.ds(rows + WINDOW, WINDOW)
    for i, (src, dst) in enumerate(((k_ref, kx), (v_ref, vx))):
        halo.append(remote(src.at[ends], dst.at[low], halo_send.at[i, 0], halo_recv.at[i, 0], (right, tp)))
        halo.append(remote(src.at[starts], dst.at[high], halo_send.at[i, 1], halo_recv.at[i, 1], (left, tp)))
    halo.append(remote(lab_row_ref.at[:, ends], lx.at[:, low], halo_send.at[2, 0], halo_recv.at[2, 0], (right, tp)))
    halo.append(remote(lab_row_ref.at[:, starts], lx.at[:, high], halo_send.at[2, 1], halo_recv.at[2, 1], (left, tp)))
    begin(0)
    begin(1)
    inner = pl.ds(WINDOW, rows)
    kx[inner, :] = k_ref[...]
    vx[inner, :] = v_ref[...]
    lx[:, inner] = lab_row_ref[...]
    for c in halo:
        c.wait()
    lx[:, low] = jnp.where(me == 0, -1, lx[:, low])
    lx[:, high] = jnp.where(me == n - 1, -1, lx[:, high])
    for i in range(rows // WINDOW + 2):
        chunk = slice(i * WINDOW, (i + 1) * WINDOW)
        square = jnp.broadcast_to(lx[0:1, chunk].astype(F32), (WINDOW, WINDOW))
        lc[chunk, :] = jnp.transpose(square)

    kv_local = k_ref.shape[1] // HEAD_DIM
    per_kv = q_ref.shape[1] // k_ref.shape[1]
    blocks = rows // WINDOW
    model = wout_ref.shape[1]

    def attend(b, carry):
        here = pl.ds(pl.multiple_of(b * WINDOW, WINDOW), WINDOW)
        wide = pl.ds(pl.multiple_of(b * WINDOW, WINDOW), 3 * WINDOW)
        q = q_ref[here, :]
        kw = kx[wide, :]
        vw = vx[wide, :]
        lab_k = lx[0:1, wide].astype(F32)
        lab_q = lc[pl.ds(pl.multiple_of(b * WINDOW + WINDOW, WINDOW), WINDOW), 0:1]
        key = lax.broadcasted_iota(jnp.int32, (WINDOW, 3 * WINDOW), 1) - WINDOW
        query = lax.broadcasted_iota(jnp.int32, (WINDOW, 3 * WINDOW), 0)
        allowed = (jnp.abs(key - query) <= WINDOW) & (lab_q == lab_k)
        results = []
        for g in range(kv_local):
            k = kw[:, g * HEAD_DIM:(g + 1) * HEAD_DIM]
            v = vw[:, g * HEAD_DIM:(g + 1) * HEAD_DIM]
            for j in range(per_kv):
                h = g * per_kv + j
                qh = q[:, h * HEAD_DIM:(h + 1) * HEAD_DIM]
                score = lax.dot_general(
                    qh, k, (((1,), (1,)), ((), ())), preferred_element_type=F32
                ) * HEAD_DIM ** (-0.5)
                score = jnp.where(allowed, score, NEG)
                sink = sink_ref[h]
                highest = jnp.maximum(jnp.max(score, axis=1, keepdims=True), sink)
                raw = jnp.where(allowed, jnp.exp(score - highest), 0.0)
                total = jnp.sum(raw, axis=1, keepdims=True) + jnp.exp(sink - highest)
                probs = (raw / total).astype(BF16)
                results.append(jnp.dot(probs, v, preferred_element_type=F32).astype(BF16))
        attended = jnp.concatenate(results, axis=1)
        part[here, :] = jnp.dot(attended, wout_ref[...], preferred_element_type=F32).astype(BF16)
        return carry

    split = blocks // 3
    for t in range(3):
        lax.fori_loop(t * split, (t + 1) * split if t < 2 else blocks, attend, 0)
        serve(2 if t == 1 else 1)

    tile = 32
    other_half = pl.ds((1 - core) * half, half)
    swap = remote(part.at[other_half], first, core_send, core_recv, (me, partner))
    swap.wait()

    def add_first(i, carry):
        r = pl.ds(pl.multiple_of(i * tile, tile), tile)
        o = pl.ds(pl.multiple_of(core * half + i * tile, tile), tile)
        first[r, :] = (part[o, :].astype(F32) + first[r, :].astype(F32)).astype(BF16)
        return carry

    lax.fori_loop(0, half // tile, add_first, 0)
    copies = []
    for j in range(1, ny):
        to = lax.rem(y + j, ny)
        copies.append(remote(
            first.at[pl.ds(to * piece, piece)], second.at[j - 1], y_send.at[j - 1], y_recv.at[j - 1], (me, to * 2 + core)
        ))
    serve(2)
    for c in copies:
        c.wait()

    def add_second(i, carry):
        r = pl.ds(pl.multiple_of(i * tile, tile), tile)
        s = first[pl.ds(pl.multiple_of(y * piece + i * tile, tile), tile), :].astype(F32)
        for j in range(ny - 1):
            s = s + second[j, r, :].astype(F32)
        o = pl.ds(pl.multiple_of(core * half + y * piece + i * tile, tile), tile)
        mixed[o, :] = (res[r, :].astype(F32) + s).astype(BF16)
        return carry

    lax.fori_loop(0, piece // tile, add_second, 0)
    mine = mixed.at[pl.ds(core * half + y * piece, piece)]
    copies = []
    for j in range(1, ny):
        to = lax.rem(y + j, ny)
        copies.append(remote(mine, mine, back_send.at[j - 1], back_recv.at[j - 1], (me, to * 2 + core)))
    serve(2)
    for j, c in enumerate(copies):
        c.wait_send()
        frm = lax.rem(y + ny - (j + 1), ny)
        theirs = mixed.at[pl.ds(core * half + frm * piece, piece)]
        pltpu.make_async_remote_copy(
            src_ref=theirs, dst_ref=theirs, send_sem=back_send.at[j], recv_sem=back_recv.at[j],
            device_id=(me, partner), device_id_type=MESH,
        ).wait_recv()
    own_half = mixed.at[pl.ds(core * half, half)]
    swap = remote(own_half, own_half, pair_send, pair_recv, (me, partner))
    swap.wait_send()
    their_half = mixed.at[other_half]
    pltpu.make_async_remote_copy(
        src_ref=their_half, dst_ref=their_half, send_sem=pair_send, recv_sem=pair_recv,
        device_id=(me, partner), device_id_type=MESH,
    ).wait_recv()

    def normalise(i, carry):
        r = pl.ds(pl.multiple_of(i * tile, tile), tile)
        m = mixed[r, :].astype(F32)
        mean_sq = jnp.mean(m * m, axis=1, keepdims=True)
        normed[r, :] = (m * lax.rsqrt(mean_sq + EPS) * gain_ref[...]).astype(BF16)
        return carry

    lax.fori_loop(0, rows // tile, normalise, 0)

    serve(2 * (n - 1) - done[0])
    big = rows // 3

    def project(t, which, dst):
        r = slice(t * big, (t + 1) * big)
        dst[r, :] = jnp.dot(normed[r, :], up[which], preferred_element_type=F32).astype(BF16)

    for t in range(3):
        project(t, 0, value)
        serve(1)
    tail = remote(value.at[pl.ds(rows - RIM, RIM)], rim.at[0], rim_send.at[0], rim_recv.at[0], (right, tp))
    head = remote(value.at[pl.ds(0, RIM)], rim.at[1], rim_send.at[1], rim_recv.at[1], (left, tp))
    for t in range(3):
        project(t, 1, gate)
        serve(1)
    tail.wait()
    head.wait()

    taps = taps_ref[...].astype(F32)
    step = 64
    before = rim[0, RIM - 1:RIM, :].astype(F32)

    def label(i, shift):
        return lc[WINDOW + i * step + shift:WINDOW + (i + 1) * step + shift, 0:1]

    for i in range(rows // step):
        r = slice(i * step, (i + 1) * step)
        x = value[r, :].astype(F32)
        after = (value[(i + 1) * step:(i + 1) * step + RIM, :] if (i + 1) * step < rows else rim[1, :, :])[0:1].astype(F32)
        prev = jnp.concatenate([before, x[:-1]], axis=0)
        nxt = jnp.concatenate([x[1:], after], axis=0)
        conv = (
            taps[0:1] * jnp.where(label(i, -1) == label(i, 0), prev, 0.0)
            + taps[1:2] * x
            + taps[2:3] * jnp.where(label(i, 1) == label(i, 0), nxt, 0.0)
        )
        gate[r, :] = (conv * jax.nn.sigmoid(conv) * gate[r, :].astype(F32)).astype(BF16)
        before = x[step - 1:step]
        if i % 3 == 2:
            serve(1)

    per_tp = n // ntp
    mine_rows = pl.ds(core * half, half)
    partner_rows = pl.ds((1 - core) * half, half)
    units = []
    for d in range(n):
        if d in (1, n - 1) and n > 2:
            units.append((2 * (n - 1) + 2 * (n - d), d, 0, 1))
            units.append((2 * (n - 1) + 2 * d, d, 1, 1))
        else:
            units.append((2 * (n - 1) + (2 * max(d, n - d) if d else 0), d, 0, 2))
    units.sort()

    def target(owner):
        to = owner // per_tp
        local = lax.rem(owner, per_tp)
        slot = lax.rem(tp - to + ntp, ntp) - 1
        return to, local, slot

    def lower(u):
        _, d, way, count = units[u]
        owner = place(lax.rem(pos + d, n))
        w = down[pl.ds(pl.multiple_of(owner * block + way * depth, depth), count * depth), :]

        def body(i, carry):
            r = pl.ds(pl.multiple_of(i * big, big), big)
            product = lax.dot_general(
                gate[r, :], w, (((1,), (1,)), ((), ())), preferred_element_type=F32
            ).astype(BF16)
            for j in range(count):
                pd[owner, way + j, r, :] = product[:, j * depth:(j + 1) * depth]
            return carry

        lax.fori_loop(0, 3, body, 0)
        return remote(
            pd.at[owner, pl.ds(way, count), partner_rows], box.at[owner, pl.ds(way, count)],
            down_send.at[u], down_recv.at[u], (me, partner),
        )

    def reduce(u, c):
        _, d, way, count = units[u]
        owner = place(lax.rem(pos + d, n))
        c.wait()

        def merge(i, carry):
            r = pl.ds(pl.multiple_of(i * tile, tile), tile)
            o = pl.ds(pl.multiple_of(core * half + i * tile, tile), tile)
            for j in range(way, way + count):
                pd[owner, j, o, :] = (pd[owner, j, o, :].astype(F32) + box[owner, j, r, :].astype(F32)).astype(BF16)
            return carry

        lax.fori_loop(0, half // tile, merge, 0, unroll=2)
        to, local, slot = target(owner)

        @pl.when(to != tp)
        def _():
            remote(
                pd.at[owner, pl.ds(way, count), mine_rows], inbox.at[local, slot, pl.ds(way, count)],
                out_send.at[u], out_recv.at[local, slot], (me, to),
            )

    waiting = None
    for u in range(len(units)):
        serve(units[u][0] - done[0])
        c = lower(u)
        if waiting is not None:
            reduce(*waiting)
        waiting = (u, c)
    reduce(*waiting)
    serve(len(queue))

    span = per_tp * block
    for local in range(per_tp):
        owner = tp * per_tp + local
        for slot in range(ntp - 1):
            ref = inbox.at[local, slot]
            pltpu.make_async_remote_copy(
                src_ref=ref, dst_ref=ref, send_sem=out_send.at[0], recv_sem=out_recv.at[local, slot],
                device_id=(me, partner), device_id_type=MESH,
            ).wait_recv()
        for same in range(2):
            base = (core if same else 1 - core) * half
            slots = range(1, ntp - 1, 2) if same else range(0, ntp - 1, 2)

            def finish(i, carry):
                r = pl.ds(pl.multiple_of(i * tile, tile), tile)
                o = pl.ds(pl.multiple_of(base + i * tile, tile), tile)
                kept = mixed[o, pl.ds(pl.multiple_of(tp * span, span), span)]
                for j in range(2):
                    s = sum(inbox[local, slot, j, r, :].astype(F32) for slot in slots)
                    if same:
                        s = s + pd[owner, j, o, :].astype(F32)
                    cols = slice(local * block + j * depth, local * block + (j + 1) * depth)
                    out_ref[o, cols] = (kept[:, cols].astype(F32) + s).astype(BF16)
                return carry

            lax.fori_loop(0, half // tile, finish, 0)
    for u, (_, d, way, count) in enumerate(units):
        owner = place(lax.rem(pos + d, n))
        to, local, slot = target(owner)

        @pl.when(to != tp)
        def _():
            ref = pd.at[owner, pl.ds(way, count), mine_rows]
            pltpu.make_async_remote_copy(
                src_ref=ref, dst_ref=ref, send_sem=out_send.at[u], recv_sem=out_recv.at[0, 0],
                device_id=(me, to), device_id_type=MESH,
            ).wait_send()
    for stream in range(4):
        for way in range(2):
            for s in range(n - 1):
                ring(stream, way, s, False).wait_send()


def paired_kernel(
    n, ntp,
    q_hbm, k_ref, v_ref, sink_ref, lab_row_ref,
    res_hbm, wout_hbm, gain_ref, wv_hbm, wg_hbm, taps_ref, wd_hbm,
    out_hbm,
    w3, other, passing, kx, vx, lx, lp, lc, same, part, first, second, mixed, normed, value, gate,
    pd, box, yin1, zin1, zin2, yin2, res, q_ref, wout_ref, kept, result,
    loc_sem, halo_send, halo_recv, lab_send, lab_recv, zs, zr, xs, xr,
    core_send, core_recv, y_send, y_recv, ag_send, ag_recv, rim_send, rim_recv,
    box_send, box_recv, yo1_send, yo1_recv, zo1_send, zo1_recv, zo2_send, zo2_recv, yo2_send, yo2_recv, out_sem,
):
    me = lax.axis_index("sp")
    tp = lax.axis_index("tp")
    core = lax.rem(tp, 2)
    y = tp // 2
    z = me // 2
    x = lax.rem(me, 2)
    zh = z // 2
    own = lax.rem(z, 2)
    pair = 1 - own
    zp = 2 * zh + pair
    far_mid = 2 - zh
    far_end = 3 - 3 * zh
    partner = y * 2 + 1 - core
    across = (1 - y) * 2 + core
    beside = (zp * 2 + x, tp)
    sibling = (z * 2 + 1 - x, tp)
    rows, cols = q_hbm.shape
    half = rows // 2
    piece = half // 2
    block, hidden = wv_hbm.shape
    wide = w3.shape[2]
    narrow = hidden - wide
    model = wout_hbm.shape[1]
    span = out_hbm.shape[1]
    is_mid = (z == 1) | (z == 2)
    is_end = (z == 0) | (z == 3)
    is_wide = is_mid
    is_narrow = is_end
    roles = ((is_narrow, narrow, wide, 0, narrow), (is_wide, wide, narrow, narrow, 0))
    sides = (is_end, is_mid)

    def copy(src, dst, send, recv, where):
        return pltpu.make_async_remote_copy(
            src_ref=src, dst_ref=dst, send_sem=send, recv_sem=recv, device_id=where, device_id_type=MESH
        )

    def arrive(ref, recv):
        copy(ref, ref, core_send.at[0], recv, (me, partner)).wait_recv()

    def left(ref, send):
        copy(ref, ref, send, core_recv.at[0], (me, partner)).wait_send()

    def spot(s, zo, xo, width):
        return w3.at[s, pl.ds(pl.multiple_of((zo * 2 + xo) * block, block), block), pl.ds(0, width)]

    sources = (wv_hbm, wg_hbm, wd_hbm)

    def loads(s):
        for cond, width, rest, at, rest_at in roles:
            def pair_of():
                a = pltpu.make_async_copy(sources[s].at[:, pl.ds(at, width)], spot(s, z, x, width), loc_sem.at[s, 0])
                b = pltpu.make_async_copy(
                    sources[s].at[:, pl.ds(rest_at, rest)], other.at[s, :, pl.ds(0, rest)], loc_sem.at[s, 1]
                )
                return a, b
            yield cond, pair_of

    for s in range(3):
        for cond, pair_of in loads(s):
            @pl.when(cond)
            def _():
                for c in pair_of():
                    c.start()
    my_piece = core * half + y * piece
    res_load = pltpu.make_async_copy(res_hbm.at[pl.ds(pl.multiple_of(my_piece, piece), piece)], res, loc_sem.at[3, 0])
    res_load.start()
    late_loads = (
        pltpu.make_async_copy(q_hbm, q_ref, loc_sem.at[4, 0]),
        pltpu.make_async_copy(wout_hbm, wout_ref, loc_sem.at[4, 1]),
    )
    for c in late_loads:
        c.start()

    barrier = pltpu.get_barrier_semaphore()
    peers = [(lax.rem(me + j, n), tp) for j in range(1, n)] + [(me, lax.rem(tp + j, ntp)) for j in range(1, ntp)]
    for peer in peers:
        pl.semaphore_signal(barrier, inc=1, device_id=peer, device_id_type=MESH)

    def loaded(s):
        for cond, pair_of in loads(s):
            @pl.when(cond)
            def _():
                for c in pair_of():
                    c.wait()

    loaded(0)
    pl.semaphore_wait(barrier, len(peers))

    def begin_end(s):
        for cond, width, rest, _, _ in roles:
            @pl.when(is_end & cond)
            def _():
                b = other.at[s, :, pl.ds(0, rest)]
                copy(b, spot(s, z, x, rest), zs.at[s, 0], zr.at[s, 0], beside).start()

    def far_end_sends(s):
        for cond, width, rest, _, _ in roles:
            @pl.when(is_end & cond)
            def _():
                a = spot(s, z, x, width)
                copy(a, a, zs.at[s, 1], zr.at[s, 2], ((3 - z) * 2 + x, tp)).start()

    def far_mid_sends(s):
        for cond, width, rest, _, _ in roles:
            @pl.when(is_mid & cond)
            def _():
                b = other.at[s, :, pl.ds(0, rest)]
                copy(b, spot(s, z, x, rest), zs.at[s, 2], zr.at[s, 1], ((3 - zp) * 2 + x, tp)).start()

    def begin_mid(s):
        for cond, width, rest, _, _ in roles:
            @pl.when(is_mid & cond)
            def _():
                a = spot(s, z, x, width)
                copy(a, a, zs.at[s, 1], zr.at[s, 1], ((3 - z) * 2 + x, tp)).start()

    def begin_out(s):
        for cond, width, rest, _, _ in roles:
            @pl.when(is_mid & cond)
            def _():
                b = other.at[s, :, pl.ds(0, rest)]
                copy(b, spot(s, z, x, rest), zs.at[s, 0], zr.at[s, 0], beside).start()

    def begin_x(s, who=(0, 1)):
        for (cond, width, _, _, _), side in ((r, sides[w]) for r in roles for w in who):
            @pl.when(cond & side)
            def _():
                a = spot(s, z, x, width)
                copy(a, a, xs.at[s, 0], xr.at[s, 0], sibling).start()

    def pass_on(first):
        for cond, width, rest, _, _ in roles:
            @pl.when(is_end & cond)
            def _():
                b = other.at[2, :, pl.ds(0, rest)]
                held = passing.at[:, pl.ds(0, rest)]
                if first:
                    copy(b, held, xs.at[2, 4], xr.at[2, 4], sibling).start()
                else:
                    arrive(held, xr.at[2, 4])
                    copy(held, spot(2, z, 1 - x, rest), zs.at[2, 4], zr.at[2, 3], beside).start()

    owners = (zp, far_mid, far_end)

    def event(s, j, who=(0, 1)):
        for side in who:
            for cond, width, _, _, _ in roles:
                @pl.when(sides[side] & cond)
                def _():
                    a = spot(s, owners[j], x, width)
                    arrive(a, zr.at[s, j])
                    if side == 1 and j == 0:
                        copy(a, a, zs.at[s, 3], zr.at[s, 2], ((3 - z) * 2 + x, tp)).start()
                    if (s, j, side) != (2, 0, 1):
                        copy(a, a, xs.at[s, j + 1], xr.at[s, j + 1], sibling).start()

    def xwait(s, j):
        for side in range(2):
            for cond, width, _, _, _ in roles:
                @pl.when(sides[side] & cond)
                def _():
                    where = spot(s, ((z,) + owners)[j], 1 - x, width)
                    arrive(where, zr.at[2, 3] if (s, j, side) == (2, 1, 1) else xr.at[s, j])

    def finish_stream(s):
        for cond, width, rest, _, _ in roles:
            @pl.when(cond)
            def _():
                left(spot(s, z, x, rest), zs.at[s, 0])
                left(spot(s, z, x, width), zs.at[s, 1])
                for j in range(4):
                    if (s, j) != (2, 1):
                        left(spot(s, z, x, width), xs.at[s, j])

            if s == 2:
                @pl.when(is_end & cond)
                def _():
                    left(spot(s, z, x, width), xs.at[2, 1])
                    left(spot(s, z, x, rest), xs.at[2, 4])
                    left(spot(s, z, x, rest), zs.at[2, 4])

            @pl.when(is_mid & cond)
            def _():
                left(spot(s, z, x, rest), zs.at[s, 2])
                left(spot(s, z, x, width), zs.at[s, 3])

    right, before = lax.rem(me + 1, n), lax.rem(me + n - 1, n)
    ends = pl.ds(rows - WINDOW, WINDOW)
    starts = pl.ds(0, WINDOW)
    low, high = pl.ds(0, WINDOW), pl.ds(rows + WINDOW, WINDOW)
    halo = []
    for i, (src, dst) in enumerate(((k_ref, kx), (v_ref, vx))):
        halo.append(copy(src.at[ends], dst.at[low], halo_send.at[i, 0], halo_recv.at[i, 0], (right, tp)))
        halo.append(copy(src.at[starts], dst.at[high], halo_send.at[i, 1], halo_recv.at[i, 1], (before, tp)))
    halo.append(copy(lab_row_ref.at[:, ends], lx.at[:, low], halo_send.at[2, 0], halo_recv.at[2, 0], (right, tp)))
    halo.append(copy(lab_row_ref.at[:, starts], lx.at[:, high], halo_send.at[2, 1], halo_recv.at[2, 1], (before, tp)))
    for c in halo:
        c.start()
    begin_end(0)
    begin_mid(0)
    begin_out(0)
    far_end_sends(0)
    far_mid_sends(0)
    begin_x(0)
    loaded(1)
    begin_end(1)
    begin_x(1)
    loaded(2)
    begin_x(2, (0,))
    pass_on(True)

    @pl.when(is_narrow)
    def _():
        if narrow < wide:
            w3[:, :, narrow:wide] = jnp.zeros((3, n * block, wide - narrow), BF16)

    inner = pl.ds(WINDOW, rows)
    kx[inner, :] = k_ref[...]
    vx[inner, :] = v_ref[...]
    lx[:, inner] = lab_row_ref[...]
    lab_copy = copy(lx, lp, lab_send, lab_recv, beside)
    chunks = rows // WINDOW

    def columns(row_ref, which):
        for i in which:
            chunk = slice(i * WINDOW, (i + 1) * WINDOW)
            square = jnp.broadcast_to(row_ref[0:1, chunk].astype(F32), (WINDOW, WINDOW))
            lc[chunk, :] = jnp.transpose(square)

    def neighbours(slot):
        for i in range(chunks):
            here = lc[WINDOW * (i + 1):WINDOW * (i + 2), :]
            for side, shift in ((0, -1), (1, 1)):
                there = lc[WINDOW * (i + 1) + shift:WINDOW * (i + 2) + shift, :]
                same[slot, side, i * WINDOW:(i + 1) * WINDOW, :] = jnp.where(here == there, 1.0, 0.0)

    columns(lx, range(1, chunks + 1))

    def edges():
        for c in halo:
            c.wait()
        lx[:, low] = jnp.where(me == 0, -1, lx[:, low])
        lx[:, high] = jnp.where(me == n - 1, -1, lx[:, high])
        lab_copy.start()
        columns(lx, (0, chunks + 1))
        neighbours(own)

    kv_local = k_ref.shape[1] // HEAD_DIM
    per_kv = cols // k_ref.shape[1]
    per_half = chunks // 2
    tile = 32

    def attend(i, carry):
        own_half = i // per_half
        j = lax.rem(i, per_half)
        flip = (1 - own_half) * core + own_half * (1 - y)
        turn = flip * (per_half - 1 - j) + (1 - flip) * j
        b = ((1 - own_half) * (1 - core) + own_half * core) * per_half + turn
        here = pl.ds(pl.multiple_of(b * WINDOW, WINDOW), WINDOW)
        wide_keys = pl.ds(pl.multiple_of(b * WINDOW, WINDOW), 3 * WINDOW)
        q = q_ref[here, :] * jnp.asarray(HEAD_DIM ** (-0.5), BF16)
        kw = kx[wide_keys, :]
        vw = vx[wide_keys, :]
        lab_k = lx[0:1, wide_keys].astype(F32)
        lab_q = lc[pl.ds(pl.multiple_of(b * WINDOW + WINDOW, WINDOW), WINDOW), 0:1]
        key = lax.broadcasted_iota(jnp.int32, (WINDOW, 3 * WINDOW), 1) - WINDOW
        query = lax.broadcasted_iota(jnp.int32, (WINDOW, 3 * WINDOW), 0)
        allowed = (jnp.abs(key - query) <= WINDOW) & (lab_q == lab_k)
        results = []
        for g in range(kv_local):
            k = kw[:, g * HEAD_DIM:(g + 1) * HEAD_DIM]
            v = vw[:, g * HEAD_DIM:(g + 1) * HEAD_DIM]
            heads = range(g * per_kv, (g + 1) * per_kv)
            stacked = jnp.concatenate([q[:, h * HEAD_DIM:(h + 1) * HEAD_DIM] for h in heads], axis=0)
            scores = lax.dot_general(stacked, k, (((1,), (1,)), ((), ())), preferred_element_type=F32)
            raws, scales = [], []
            for u, h in enumerate(heads):
                score = jnp.where(allowed, scores[u * WINDOW:(u + 1) * WINDOW], NEG)
                sink = sink_ref[h]
                highest = jnp.maximum(jnp.max(score, axis=1, keepdims=True), sink)
                raw = jnp.exp(score - highest)
                scales.append(1.0 / (jnp.sum(raw, axis=1, keepdims=True) + jnp.exp(sink - highest)))
                raws.append(raw.astype(BF16))
            summed = jnp.dot(jnp.concatenate(raws, axis=0), v, preferred_element_type=F32)
            for u in range(per_kv):
                results.append((summed[u * WINDOW:(u + 1) * WINDOW] * scales[u]).astype(BF16))
        attended = jnp.concatenate(results, axis=1)
        part[here, :] = jnp.dot(attended, wout_ref[...], preferred_element_type=F32).astype(BF16)
        mine = first.at[pl.ds(pl.multiple_of(turn * WINDOW, WINDOW), WINDOW)]

        @pl.when(own_half == 0)
        def _():
            copy(part.at[here], mine, core_send.at[turn], core_recv.at[turn], (me, partner)).start()

        @pl.when(own_half == 1)
        def _():
            arrive(mine, core_recv.at[turn])

            def add(t, carry):
                r = pl.ds(pl.multiple_of(turn * WINDOW + t * tile, tile), tile)
                o = pl.ds(pl.multiple_of(b * WINDOW + t * tile, tile), tile)
                first[r, :] = (part[o, :].astype(F32) + first[r, :].astype(F32)).astype(BF16)
                return carry

            lax.fori_loop(0, WINDOW // tile, add, 0)

        @pl.when(i == per_half)
        def _():
            y_copy(0, y).start()

        @pl.when(i == per_half + 1)
        def _():
            y_copy(1, y).start()

        @pl.when(i == 1)
        def _():
            edges()

        @pl.when(i == 3)
        def _():
            event(0, 0, (1,))
            begin_mid(1)
            begin_out(1)
            far_mid_sends(1)

        @pl.when(i == 4)
        def _():
            event(0, 1, (1,))

        return carry

    def y_copy(k, yy):
        if k == 0:
            count, src, dst = 2 * piece // 3, (1 - yy) * (half - 2 * piece // 3), (1 - yy) * (piece // 3)
        else:
            count, src, dst = piece // 3, 2 * piece // 3 + (1 - yy) * (piece // 3), yy * (2 * piece // 3)
        return copy(
            first.at[pl.ds(pl.multiple_of(src, 64), count)], second.at[pl.ds(pl.multiple_of(dst, 64), count)],
            y_send.at[k], y_recv.at[k], (me, across),
        )

    res_load.wait()
    for c in late_loads:
        c.wait()
    lax.fori_loop(0, 2 * per_half, attend, 0)
    for k in range(2):
        y_copy(k, 1 - y).wait_recv()

    def norm(slot, start, count):
        def body(i, carry):
            r = pl.ds(pl.multiple_of(start + i * tile, tile), tile)
            m = mixed[r, :].astype(F32)
            mean_sq = jnp.mean(m * m, axis=1, keepdims=True)
            normed[slot, r, :] = (m * lax.rsqrt(mean_sq + EPS) * gain_ref[...]).astype(BF16)
            return carry

        lax.fori_loop(0, count // tile, body, 0, unroll=3)

    def add_second(i, carry):
        r = pl.ds(pl.multiple_of(i * tile, tile), tile)
        f = pl.ds(pl.multiple_of(y * piece + i * tile, tile), tile)
        o = pl.ds(pl.multiple_of(my_piece + i * tile, tile), tile)
        s = first[f, :].astype(F32) + second[r, :].astype(F32)
        mixed[o, :] = (res[r, :].astype(F32) + s).astype(BF16)
        return carry

    lax.fori_loop(0, piece // tile, add_second, 0)

    def part_of(c, yy):
        return c * half + yy * piece

    def mixed_at(c, yy):
        return mixed.at[pl.ds(pl.multiple_of(part_of(c, yy), piece), piece)]

    bit = piece // 2

    def normed_at(slot, c, yy, b):
        return normed.at[slot, pl.ds(pl.multiple_of(part_of(c, yy) + b * bit, bit), bit)]

    def share(k, ref, where):
        copy(ref, ref, ag_send.at[k], ag_recv.at[k], where).start()

    share(0, mixed_at(core, y), (me, across))
    share(1, mixed_at(core, y), (me, partner))
    for b in range(2):
        norm(own, my_piece + b * bit, bit)
        share(4 + b, normed_at(own, core, y, b), beside)
    event(0, 0, (0,))
    event(1, 0, (1,))
    event(0, 1, (0,))
    arrive(mixed_at(1 - core, y), ag_recv.at[1])
    norm(own, part_of(1 - core, y), piece)
    event(0, 2, (1,))
    arrive(mixed_at(core, 1 - y), ag_recv.at[0])
    share(2, mixed_at(core, 1 - y), (me, partner))
    norm(own, part_of(core, 1 - y), piece)
    event(0, 2, (0,))

    def serve_spread(b):
        arrive(normed_at(pair, core, y, b), ag_recv.at[4 + b])
        share(6 + b, normed_at(pair, core, y, b), (me, across))
        share(8 + b, normed_at(pair, core, y, b), (me, partner))

    event(1, 0, (0,))
    event(1, 1, (0,))
    serve_spread(0)
    far_end_sends(1)
    serve_spread(1)
    event(1, 1, (1,))
    begin_end(2)
    pass_on(False)
    arrive(mixed_at(1 - core, 1 - y), ag_recv.at[2])
    norm(own, part_of(1 - core, 1 - y), piece)

    big = rows // 2

    def project(which, slot):
        def body(t, carry):
            r = pl.ds(pl.multiple_of(t * big, big), big)
            product = jnp.dot(normed[slot, r, :], w3[which], preferred_element_type=F32).astype(BF16)
            if which == 0:
                value[slot, pl.ds(pl.multiple_of(RIM + t * big, RIM), big), :] = product
            else:
                gate[slot, r, :] = product
            return carry

        lax.fori_loop(0, 2, body, 0)

    inside = pl.ds(RIM, RIM)
    last = pl.ds(rows, RIM)
    fronts, backs = pl.ds(0, RIM), pl.ds(RIM + rows, RIM)
    facing = ((3 - z) * 2 + 1 - x, tp)
    near_rims = (
        (x == 0, ((0, last, 0, 0), (1, inside, 0, 1), (1, last, 1, 0))),
        (x == 1, ((0, inside, 0, 1), (0, last, 1, 0), (1, inside, 1, 1))),
    )
    far_rims = (((x == 0) & (zh == 1), (0, inside, 1, 1)), ((x == 1) & (zh == 0), (1, last, 0, 0)))

    def rim_copy(frm, source, to, side, where):
        target = value.at[to, (fronts, backs)[side]]
        pad = 2 * to + side
        copy(value.at[frm, source], target, rim_send.at[pad], rim_recv.at[pad], where).start()

    def send_far_rims(side):
        for cond, spec in far_rims:
            @pl.when(cond & side)
            def _():
                rim_copy(*spec, facing)

    mine = mixed.at[:, pl.ds(pl.multiple_of(tp * span, span), span)]
    kept_copy = pltpu.make_async_copy(mine, kept, loc_sem.at[3, 1])
    kept_copy.start()

    def serve_x(s):
        for j in range(4):
            xwait(s, j)

    serve_x(0)
    project(0, own)
    send_far_rims(is_mid)
    begin_mid(2)
    begin_out(2)
    far_mid_sends(2)
    event(1, 2)

    def serve_diagonal(b):
        arrive(normed_at(pair, core, 1 - y, b), ag_recv.at[6 + b])
        share(10 + b, normed_at(pair, core, 1 - y, b), (me, partner))

    def serve_rest(b):
        arrive(normed_at(pair, 1 - core, y, b), ag_recv.at[8 + b])
        arrive(normed_at(pair, 1 - core, 1 - y, b), ag_recv.at[10 + b])

    serve_diagonal(0)
    serve_diagonal(1)
    serve_rest(0)
    serve_rest(1)
    project(0, pair)

    send_far_rims(is_end)
    for cond, specs in near_rims:
        @pl.when(cond)
        def _():
            for spec in specs:
                rim_copy(*spec, sibling)

    far_end_sends(2)
    begin_x(2, (1,))
    event(2, 0, (0,))
    serve_x(1)
    project(1, own)
    event(2, 0, (1,))
    project(1, pair)
    event(2, 1, (1,))
    lab_copy.wait()
    columns(lp, range(chunks + 2))
    neighbours(pair)

    def serve_rims(slot):
        for side, rd in enumerate((fronts, backs)):
            if slot == side:
                @pl.when((x != side) | (zh != side))
                def _():
                    arrive(value.at[slot, rd], rim_recv.at[2 * slot + side])

                @pl.when((x == side) & (zh == side))
                def _():
                    value[slot, rd, :] = jnp.zeros((RIM, wide), BF16)
            else:
                arrive(value.at[slot, rd], rim_recv.at[2 * slot + side])

    serve_rims(0)
    serve_rims(1)

    taps_all = taps_ref[...].astype(F32)
    taps = jnp.where(is_wide, taps_all[:, narrow:], taps_all[:, :wide])
    step = 64
    lanes = wide // WINDOW

    for slot in range(2):
        def gated(i, carry):
            base = i * step
            r = pl.ds(pl.multiple_of(base, step), step)
            x_rows = value[slot, pl.ds(pl.multiple_of(RIM + base, RIM), step), :].astype(F32)
            above = value[slot, pl.ds(pl.multiple_of(base, RIM), RIM), :].astype(F32)[RIM - 1:RIM]
            below = value[slot, pl.ds(pl.multiple_of(RIM + base + step, RIM), RIM), :].astype(F32)[0:1]
            prev = jnp.concatenate([above, x_rows[:-1]], axis=0)
            nxt = jnp.concatenate([x_rows[1:], below], axis=0)
            with_prev = jnp.concatenate([same[slot, 0, r, :]] * lanes, axis=1) > 0.5
            with_next = jnp.concatenate([same[slot, 1, r, :]] * lanes, axis=1) > 0.5
            conv = (
                taps[0:1] * jnp.where(with_prev, prev, 0.0)
                + taps[1:2] * x_rows
                + taps[2:3] * jnp.where(with_next, nxt, 0.0)
            )
            gate[slot, r, :] = (conv * jax.nn.sigmoid(conv) * gate[slot, r, :].astype(F32)).astype(BF16)
            return carry

        lax.fori_loop(0, rows // step, gated, 0)

    order = (z, zp, far_mid, far_end)
    quarter = rows // 2

    def boxed(u, k):
        slot = (pair, own)[k]
        return copy(pd.at[u, slot], box.at[u // 2, slot], box_send.at[u, k], box_recv.at[u // 2, k], (me, partner))

    def lower(u):
        t = order[u]
        w = w3[2, pl.ds(pl.multiple_of(t * span, span), span), :]
        for k, slot in enumerate((pair, own)):
            def body(i, carry):
                r = pl.ds(pl.multiple_of(i * rows, rows), rows)
                pd[u, slot, r, :] = lax.dot_general(
                    gate[slot, r, :], w, (((1,), (1,)), ((), ())), preferred_element_type=F32
                ).astype(BF16)
                return carry

            lax.fori_loop(0, 1, body, 0)

            @pl.when(core != lax.rem(t, 2))
            def _():
                boxed(u, k).start()

    cuts = (rows // 6 * 3, rows // 6 * 3, rows // 6 * 3, rows // 6 * 2)

    def segment(u, g):
        count = (rows - cuts[u]) // 2
        return cuts[u] + g * count, count

    slab = rows // 12

    def accumulate(ref, slot, at, count, other_ref, base):
        def body(i, carry):
            r = pl.ds(pl.multiple_of(at + i * slab, slab), slab)
            o = pl.ds(pl.multiple_of(base + i * slab, slab), slab)
            ref[slot, r, :] = (ref[slot, r, :].astype(F32) + other_ref[o, :].astype(F32)).astype(BF16)
            return carry

        lax.fori_loop(0, count // slab, body, 0)

    def z_first(u, g):
        at, count = segment(u, g)
        return copy(
            pd.at[u, pair, pl.ds(at, count)], zin1.at[u // 2, g, pl.ds(0, count)],
            zo1_send.at[u // 2, g], zo1_recv.at[u // 2, g], beside,
        )

    def then_y(u, g):
        at, count = segment(u, g)
        return copy(
            pd.at[u, own, pl.ds(at, count)], yin2.at[g, pl.ds(0, count)], yo2_send.at[g], yo2_recv.at[g], (me, across)
        )

    def y_first(u, slot, k):
        top = pl.ds(0, cuts[u])
        return copy(pd.at[u, slot, top], yin1.at[slot, top], yo1_send.at[k], yo1_recv.at[k], (me, across))

    def then_z(u):
        top = pl.ds(0, cuts[u])
        return copy(pd.at[u, pair, top], zin2.at[top], zo2_send, zo2_recv, beside)

    def stage_one(u):
        t = order[u]

        @pl.when(core == lax.rem(t, 2))
        def _():

            def add(slot, at, count):
                accumulate(pd.at[u], slot, at, count, box.at[u // 2, slot], at)

            arrive(box.at[u // 2, pair], box_recv.at[u // 2, 0])
            if u < 3:
                add(pair, 0, cuts[u])

                @pl.when(y != t // 2)
                def _():
                    y_first(u, pair, 0).start()

            for g in range(2):
                add(pair, *segment(u, g))
                z_first(u, g).start()
            if u == 3:
                add(pair, 0, cuts[u])

                @pl.when(y != t // 2)
                def _():
                    y_first(u, pair, 0).start()

            arrive(box.at[u // 2, own], box_recv.at[u // 2, 1])
            add(own, 0, cuts[u])

            @pl.when(y != t // 2)
            def _():
                y_first(u, own, 1).start()

            for g in range(2):
                add(own, *segment(u, g))

    def stage_y(u):
        t = order[u]

        @pl.when(tp == t)
        def _():
            top = pl.ds(0, cuts[u])
            arrive(yin1.at[pair, top], yo1_recv.at[0])
            accumulate(pd.at[u], pair, 0, cuts[u], yin1.at[pair], 0)
            then_z(u).start()
            arrive(yin1.at[own, top], yo1_recv.at[1])
            accumulate(pd.at[u], own, 0, cuts[u], yin1.at[own], 0)

    def stage_z(u):
        t = order[u]

        @pl.when(core == lax.rem(t, 2))
        def _():
            for g in range(2):
                at, count = segment(u, g)
                arrive(zin1.at[u // 2, g, pl.ds(0, count)], zo1_recv.at[u // 2, g])
                accumulate(pd.at[u], own, at, count, zin1.at[u // 2, g], 0)

                @pl.when(y != t // 2)
                def _():
                    then_y(u, g).start()

    def put(at, count, k):
        r = pl.ds(at, count)
        return pltpu.make_async_copy(result.at[r], out_hbm.at[r], out_sem.at[k])

    def stage_three(u):
        t = order[u]

        @pl.when(tp == t)
        def _():
            def close(at, count, extra, k):
                def body(i, carry):
                    r = pl.ds(pl.multiple_of(i * slab, slab), slab)
                    o = pl.ds(pl.multiple_of(at + i * slab, slab), slab)
                    s = pd[u, own, o, :].astype(F32) + extra[r, :].astype(F32)
                    result[o, :] = (kept[o, :].astype(F32) + s).astype(BF16)
                    return carry

                lax.fori_loop(0, count // slab, body, 0)
                put(at, count, k).start()

            arrive(zin2.at[pl.ds(0, cuts[u])], zo2_recv)
            close(0, cuts[u], zin2, 0)
            for g in range(2):
                at, count = segment(u, g)
                arrive(yin2.at[g, pl.ds(0, count)], yo2_recv.at[g])
                close(at, count, yin2.at[g], 1 + g)
            put(0, cuts[u], 0).wait()
            for g in range(2):
                put(*segment(u, g), 1 + g).wait()

    def drain(u):
        t = order[u]

        @pl.when(core != lax.rem(t, 2))
        def _():
            for k in range(2):
                boxed(u, k).wait_send()

        @pl.when(core == lax.rem(t, 2))
        def _():
            for g in range(2):
                z_first(u, g).wait_send()

            @pl.when(y != t // 2)
            def _():
                for k, slot in enumerate((pair, own)):
                    y_first(u, slot, k).wait_send()
                for g in range(2):
                    then_y(u, g).wait_send()

            @pl.when(y == t // 2)
            def _():
                then_z(u).wait_send()

    xwait(2, 0)
    lower(0)
    event(2, 1, (0,))
    stage_one(0)
    xwait(2, 1)
    lower(1)
    stage_one(1)
    event(2, 2)
    xwait(2, 2)
    lower(2)
    stage_one(2)
    xwait(2, 3)
    lower(3)
    stage_one(3)
    stage_z(0)
    stage_z(1)
    stage_y(0)
    stage_y(1)
    stage_z(2)
    stage_z(3)
    stage_y(2)
    stage_y(3)
    kept_copy.wait()
    stage_three(0)
    stage_three(1)
    stage_three(2)
    stage_three(3)

    for s in range(3):
        finish_stream(s)
    for j in range(per_half):
        left(first.at[pl.ds(0, WINDOW)], core_send.at[j])
    for k in range(2):
        y_copy(k, y).wait_send()
    for k in range(3):
        left(mixed_at(core, y), ag_send.at[k])
    for k in range(4, 12):
        left(normed_at(own, core, y, 0), ag_send.at[k])
    for pad in range(4):
        sends = (x == pad // 3) | (zh == pad // 3) if pad in (0, 3) else x >= 0

        @pl.when(sends)
        def _():
            left(value.at[0, fronts], rim_send.at[pad])
    for u in range(4):
        drain(u)


def solution(mesh):
    n, ntp = mesh.shape["sp"], mesh.shape["tp"]

    def by_ring(q, k, v, sink, doc, res, wout, gain, wv, wg, taps, wd):
        rows, model = res.shape
        hidden = wv.shape[1]
        block = wv.shape[0]
        ny = ntp // 2
        labels = doc + 1
        lab_row = labels[None, :]
        vm = pl.BlockSpec(memory_space=pltpu.VMEM)
        hbm = pl.BlockSpec(memory_space=pl.ANY)
        smem = pl.BlockSpec(memory_space=pltpu.SMEM)
        dma = pltpu.SemaphoreType.DMA
        kvc = k.shape[1]
        span = model // ntp
        scratch = [
            pltpu.VMEM((2, n * block, hidden), BF16),
            pltpu.VMEM((n * block, hidden), BF16),
            pltpu.VMEM((rows + 2 * WINDOW, kvc), BF16),
            pltpu.VMEM((rows + 2 * WINDOW, kvc), BF16),
            pltpu.VMEM((1, rows + 2 * WINDOW), jnp.int32),
            pltpu.VMEM((rows + 2 * WINDOW, WINDOW), F32),
            pltpu.VMEM((rows, model), BF16),
            pltpu.VMEM((rows // 2, model), BF16),
            pltpu.VMEM((max(ny - 1, 1), rows // 2 // ny, model), BF16),
            pltpu.VMEM((rows, model), BF16),
            pltpu.VMEM((rows, model), BF16),
            pltpu.VMEM((rows, hidden), BF16),
            pltpu.VMEM((rows, hidden), BF16),
            pltpu.VMEM((2, RIM, hidden), BF16),
            pltpu.VMEM((n, 2, rows, block // 2), BF16),
            pltpu.VMEM((n, 2, rows // 2, block // 2), BF16),
            pltpu.VMEM((n // ntp, ntp - 1, 2, rows // 2, block // 2), BF16),
            pltpu.VMEM((rows // 2 // ny, model), BF16),
            dma((4,)),
            dma((4, 2, n - 1)), dma((4, 2, n - 1)),
            dma((3, 2)), dma((3, 2)),
            dma((2,)), dma((2,)),
            dma, dma,
            dma((ny,)), dma((ny,)),
            dma((ny,)), dma((ny,)),
            dma, dma,
            dma((n + 2,)), dma((n + 2,)),
            dma((n + 2,)), dma((n // ntp, ntp - 1)),
        ]
        return pl.pallas_call(
            functools.partial(ring_kernel, n, ntp),
            out_shape=jax.ShapeDtypeStruct((rows, span), BF16),
            in_specs=[vm, vm, vm, smem, vm, hbm, vm, vm, hbm, hbm, vm, hbm],
            out_specs=vm,
            scratch_shapes=scratch,
            compiler_params=pltpu.CompilerParams(
                collective_id=0, has_side_effects=True, vmem_limit_bytes=67043328
            ),
            name="layer",
        )(q, k, v, sink, lab_row, res, wout, gain[None, :], wv, wg, taps, wd)


    def by_pairs(q, k, v, sink, doc, res, wout, gain, wv, wg, taps, wd):
        rows, model = res.shape
        block, hidden = wv.shape
        half = rows // 2
        piece = half // 2
        span = model // ntp
        kvc = k.shape[1]
        third = rows // 12 * 5
        wide = (hidden // LANES + 1) // 2 * LANES
        lab_row = doc[None, :]
        vm = pl.BlockSpec(memory_space=pltpu.VMEM)
        hbm = pl.BlockSpec(memory_space=pl.ANY)
        smem = pl.BlockSpec(memory_space=pltpu.SMEM)
        dma = pltpu.SemaphoreType.DMA
        scratch = [
            pltpu.VMEM((3, n * block, wide), BF16),
            pltpu.VMEM((3, block, wide), BF16),
            pltpu.VMEM((block, wide), BF16),
            pltpu.VMEM((rows + 2 * WINDOW, kvc), BF16),
            pltpu.VMEM((rows + 2 * WINDOW, kvc), BF16),
            pltpu.VMEM((1, rows + 2 * WINDOW), jnp.int32),
            pltpu.VMEM((1, rows + 2 * WINDOW), jnp.int32),
            pltpu.VMEM((rows + 2 * WINDOW, WINDOW), F32),
            pltpu.VMEM((2, 2, rows, WINDOW), F32),
            pltpu.VMEM((rows, model), BF16),
            pltpu.VMEM((half, model), BF16),
            pltpu.VMEM((piece, model), BF16),
            pltpu.VMEM((rows, model), BF16),
            pltpu.VMEM((2, rows, model), BF16),
            pltpu.VMEM((2, rows + 2 * RIM, wide), BF16),
            pltpu.VMEM((2, rows, wide), BF16),
            pltpu.VMEM((4, 2, rows, span), BF16),
            pltpu.VMEM((2, 2, rows, span), BF16),
            pltpu.VMEM((2, half, span), BF16),
            pltpu.VMEM((2, 2, third, span), BF16),
            pltpu.VMEM((half, span), BF16),
            pltpu.VMEM((2, third, span), BF16),
            pltpu.VMEM((piece, model), BF16),
            pltpu.VMEM(q.shape, BF16),
            pltpu.VMEM(wout.shape, BF16),
            pltpu.VMEM((rows, span), BF16),
            pltpu.VMEM((rows, span), BF16),
            dma((5, 2)),
            dma((3, 2)), dma((3, 2)),
            dma, dma,
            dma((3, 5)), dma((3, 4)),
            dma((3, 5)), dma((3, 5)),
            dma((rows // WINDOW // 2,)), dma((rows // WINDOW // 2,)),
            dma((2,)), dma((2,)),
            dma((12,)), dma((12,)),
            dma((4,)), dma((4,)),
            dma((4, 2)), dma((2, 2)),
            dma((2,)), dma((2,)),
            dma((2, 2)), dma((2, 2)),
            dma, dma,
            dma((2,)), dma((2,)),
            dma((3,)),
        ]
        return pl.pallas_call(
            functools.partial(paired_kernel, n, ntp),
            out_shape=jax.ShapeDtypeStruct((rows, span), BF16),
            in_specs=[hbm, vm, vm, smem, vm, hbm, hbm, vm, hbm, hbm, vm, hbm],
            out_specs=hbm,
            scratch_shapes=scratch,
            compiler_params=pltpu.CompilerParams(
                collective_id=0, has_side_effects=True, vmem_limit_bytes=67043328
            ),
            name="layer",
        )(q, k, v, sink, lab_row, res, wout, gain[None, :], wv, wg, taps, wd)

    placed = (
        P("sp", "tp"), P("sp", "tp"), P("sp", "tp"), P("tp"), P("sp"), P("sp", None),
        P("tp", None), P(), P("sp", "tp"), P("sp", "tp"), P(None, "tp"), P("sp", "tp"),
    )
    return jax.shard_map(
        by_pairs if (n, ntp) == (8, 4) else by_ring, mesh=mesh, in_specs=placed, out_specs=P("sp", "tp"), check_vma=False
    )
```
